256 devices in a mesh: fs: 32 (over z, x), rep: 4 (over y), tp: 2 (over core).
Axes of the slice: x: 4, y: 4, z: 8, core: 2. Of those that a mesh axis runs over, the one named last changes fastest.
Arguments:
- inputs: bfloat16 [16384, 2048], P(('fs', 'rep')), may hold values from -24 to 24
- query_cot: bfloat16 [16384, 1024], P(('fs', 'rep'), 'tp'), may hold values from -0.046875 to 0.046875
- attended: bfloat16 [16384, 1024], P(('fs', 'rep')), may hold values from -24 to 24
- output_cot: bfloat16 [16384, 2048], P(('fs', 'rep'), 'tp'), may hold values from -0.046875 to 0.046875
- proj_query: bfloat16 [2048, 256], P('fs'), may hold values from -0.125 to 0.125
- proj_output: bfloat16 [1024, 256], P('fs'), may hold values from -0.1875 to 0.1875
- weight_query: float32 [2048, 1024], P('fs', 'tp'), may hold values from -0.125 to 0.125
- weight_output: float32 [1024, 2048], P('fs', 'tp'), may hold values from -0.1875 to 0.1875
- first_query: float32 [256, 1024], P('fs', 'tp'), may hold values from -6 to 6
- second_query: float32 [256, 1024], P('fs', 'tp'), may hold values from 0.0002 to 2
- first_output: float32 [256, 2048], P('fs', 'tp'), may hold values from -6 to 6
- second_output: float32 [256, 2048], P('fs', 'tp'), may hold values from 0.0002 to 2
Outputs:
- new_weight_query: float32 [2048, 1024], P('fs', 'tp')
- new_weight_output: float32 [1024, 2048], P('fs', 'tp')
- step_query: float32 [2048, 1024], P('fs', 'tp')
- step_output: float32 [1024, 2048], P('fs', 'tp')
- new_first_query: float32 [256, 1024], P('fs', 'tp')
- new_second_query: float32 [256, 1024], P('fs', 'tp')
- new_first_output: float32 [256, 2048], P('fs', 'tp')
- new_second_output: float32 [256, 2048], P('fs', 'tp')
- copy_query: bfloat16 [2048, 1024], P(None, 'tp')
- copy_output: bfloat16 [1024, 2048], P(None, 'tp')
The draws below stay inside these ranges and needn't reach their ends.
All inputs are finite; a program needn't handle non-finite values.
Results may differ from the reference program's by a relative error of at most 0.0031.
Values may be sent and summed in bfloat16 or wider, within the bound.
A program may use at most 64 MiB of HBM per device.

```python
import jax
import jax.numpy as jnp
from jax import lax

D = 2048
DA = 1024
RANK = 256
TOKENS = 16384


def variance_table(key, height, breadth):
    base = jnp.exp(jax.random.uniform(key, (height, breadth), jnp.float32, jnp.log(0.02), jnp.log(1.0)))
    row_place = jnp.arange(height, dtype=jnp.float32) / height
    col_place = jnp.arange(breadth, dtype=jnp.float32) / breadth
    return base * jnp.exp(-jnp.log(10.0) * row_place)[:, None] * jnp.exp(-jnp.log(10.0) * col_place)[None, :]


def draw_second_query(key, part):
    return variance_table(jax.random.fold_in(key, 11), RANK, DA)


def draw_second_output(key, part):
    return variance_table(jax.random.fold_in(key, 12), RANK, D)


def with_spikes(drawn, stream_key, source, target, parts, factor):
    owner, partner = [(jnp.arange(drawn.shape[axis_at]) // (drawn.shape[axis_at] // parts)).reshape([-1 if axis == axis_at else 1 for axis in range(drawn.ndim)]) for axis_at in (source, target)]
    chosen = jax.random.permutation(stream_key, parts)[partner]
    strong = (owner == chosen) | (owner == (partner + parts // 2) % parts)
    return jnp.where(strong, factor * drawn, drawn)


def block_scale(own_key, extent, cuts, least, top_value):
    factor_of = 1.0
    for axis_at, shards_of in cuts:
        draws = jax.random.uniform(jax.random.fold_in(jax.random.fold_in(own_key, 6), axis_at), (shards_of,), jnp.float32, least / len(cuts), top_value / len(cuts))
        factor_of = factor_of * jnp.repeat(jnp.exp(draws), extent[axis_at] // shards_of).reshape((-1,) + (1,) * (len(extent) - 1 - axis_at))
    return factor_of


def scatter_about(rng, extent, scale, most, pieces=(), kind=jnp.bfloat16):
    values = scale * jax.random.normal(rng, extent, jnp.float32)
    if pieces:
        values = values * block_scale(rng, extent, pieces, -0.22, 0.18)
    return jnp.clip(values, -most, most).astype(kind)


def bell_draw_with(key, shape, scale, reach, pieces, heavy, kind=jnp.bfloat16):
    values = scale * jax.random.normal(key, shape, jnp.float32)
    if pieces:
        values = values * block_scale(key, shape, pieces, -0.22, 0.18)
    return jnp.clip(with_spikes(values, jax.random.fold_in(key, 3), *heavy), -reach, reach).astype(kind)


def setup_inputs(seed: int = 0) -> dict:
    keys = jax.random.split(jax.random.key(seed), 13)
    inputs = bell_draw_with(keys[0], (TOKENS, D), 1.0, 24.0, ((0, 128),), (0, 1, 128, 5.5))
    query_cot = scatter_about(keys[1], (TOKENS, DA), TOKENS ** -0.5, 0.046875, ((0, 128), (1, 2)))
    attended = bell_draw_with(keys[2], (TOKENS, DA), 1.0, 24.0, ((0, 128),), (0, 1, 128, 5.5))
    output_cot = scatter_about(keys[3], (TOKENS, D), TOKENS ** -0.5, 0.046875, ((0, 128), (1, 2)))
    proj_query = scatter_about(keys[4], (D, RANK), D ** -0.5, 0.125, ((0, 32),))
    proj_output = scatter_about(keys[5], (DA, RANK), DA ** -0.5, 0.1875, ((0, 32),))
    weight_query = scatter_about(keys[6], (D, DA), D ** -0.5, 0.125, ((0, 32), (1, 2)), jnp.float32)
    weight_output = scatter_about(keys[7], (DA, D), DA ** -0.5, 0.1875, ((0, 32), (1, 2)), jnp.float32)
    first_query = scatter_about(keys[8], (RANK, DA), 1.0, 6.0, ((0, 32), (1, 2)), jnp.float32)
    second_query = draw_second_query(jax.random.fold_in(keys[12], 71), 0)
    first_output = scatter_about(keys[10], (RANK, D), 1.0, 6.0, ((0, 32), (1, 2)), jnp.float32)
    second_output = draw_second_output(jax.random.fold_in(keys[12], 71), 0)
    return dict(inputs=inputs, query_cot=query_cot, attended=attended, output_cot=output_cot, proj_query=proj_query, proj_output=proj_output, weight_query=weight_query, weight_output=weight_output, first_query=first_query, second_query=second_query, first_output=first_output, second_output=second_output)


beta_first = 0.9
beta_second = 0.95
adam_eps = 1e-08
mean_eps = 1e-06
learn_rate = 0.02

def contract_rows(left, right, high):
    if high:
        return lax.dot_general(left, right, (((0,), (0,)), ((), ())), precision=lax.Precision.HIGHEST, preferred_element_type=jnp.float32)
    return lax.dot_general(left, right, (((0,), (0,)), ((), ())), preferred_element_type=jnp.float32)

def moment_update(low_sum, first, second):
    first_new = beta_first * first + (1.0 - beta_first) * low_sum
    second_new = beta_second * second + (1.0 - beta_second) * low_sum * low_sum
    normed = first_new / (jnp.sqrt(second_new) + adam_eps)
    return (first_new, second_new, normed)

def reference(inputs, query_cot, attended, output_cot, proj_query, proj_output, weight_query, weight_output, first_query, second_query, first_output, second_output):
    grad_query = contract_rows(inputs, query_cot, False)
    grad_output = contract_rows(attended, output_cot, False)
    low_query = contract_rows(proj_query.astype(jnp.float32), grad_query, True)
    low_output = contract_rows(proj_output.astype(jnp.float32), grad_output, True)
    first_q, second_q, normed_q = moment_update(low_query, first_query, second_query)
    first_o, second_o, normed_o = moment_update(low_output, first_output, second_output)
    entries = RANK * (DA + D)
    total = jnp.sum(normed_q * normed_q) + jnp.sum(normed_o * normed_o)
    scale = lax.rsqrt(total / entries + mean_eps)
    half_q = normed_q.astype(jnp.bfloat16)
    half_o = normed_o.astype(jnp.bfloat16)
    step_q = scale * jnp.dot(proj_query, half_q, preferred_element_type=jnp.float32)
    step_o = scale * jnp.dot(proj_output, half_o, preferred_element_type=jnp.float32)
    new_q = weight_query - learn_rate * step_q
    new_o = weight_output - learn_rate * step_o
    return (new_q, new_o, step_q, step_o, first_q, second_q, first_o, second_o, new_q.astype(jnp.bfloat16), new_o.astype(jnp.bfloat16))
```

```python
import functools

import jax
import jax.numpy as jnp
from jax import lax
from jax.experimental import pallas as pl
from jax.experimental.pallas import tpu as pltpu
from jax.sharding import PartitionSpec as P

D = 2048
DA = 1024
RANK = 256
NZ, NX, NY = 8, 4, 4

beta_first = 0.9
beta_second = 0.95
adam_eps = 1e-08
mean_eps = 1e-06
learn_rate = 0.02
HALF = 768

MESH = pl.DeviceIdType.MESH
NEAR_FIRST = (1, 7, 2, 6, 3, 5, 4)


def moment_update(low_sum, first, second):
    first_new = beta_first * first + (1.0 - beta_first) * low_sum
    second_new = beta_second * second + (1.0 - beta_second) * low_sum * low_sum
    normed = first_new / (jnp.sqrt(second_new) + adam_eps)
    return (first_new, second_new, normed)


def coded(v):
    square = v * v
    fourth = square * square
    return jnp.where(v < 0, -fourth, fourth).astype(jnp.bfloat16)


def decoded(c):
    c = c.astype(jnp.float32)
    root = lax.rsqrt(lax.rsqrt(jnp.maximum(jnp.abs(c), 1e-37)))
    return jnp.where(c < 0, -root, root)


def comm_kernel(
    inputs, query_cot, attended, output_cot, proj_q, proj_o, w_q, w_o,
    first_q, second_q, first_o, second_o,
    pq, po, half, low, scale, wg_q, wg_o,
    x_in, c_q, x_at, c_o, fst, snd, old_q, old_o, code_q, code_o,
    lb, cb, by, bx, sz, bz, ty, by2, qc, qz, qx, qy,
    loc, a_zs, a_zr, a_xs, a_xr, a_cs, a_cr,
    w_xs, w_xr, w_zs, w_zr, w_ys, w_yr,
    b_ys, b_yr, b_xs, b_xr, b_zs, b_zr, b_2s, b_2r, b_ls, b_lr,
    e_zs, e_zr, e_xs, e_xr, e_ys, e_yr,
    q_cs, q_cr, q_zs, q_zr, q_xs, q_xr, q_ys, q_yr,
):
    f = lax.axis_index("fs")
    y = lax.axis_index("rep")
    t = lax.axis_index("tp")
    z = f // NX
    x = f % NX
    p = y % 2
    o = 1 - p

    def at_z(d):
        return {"fs": ((z + d) % NZ) * NX + x}

    def at_x(e):
        return {"fs": z * NX + (x + e) % NX}

    def at_y(s):
        return {"rep": (y + s) % NY}

    other_core = {"tp": 1 - t}
    sends = []

    def remote(src, dst, ssem, rsem, dev):
        return pltpu.make_async_remote_copy(
            src_ref=src, dst_ref=dst, send_sem=ssem, recv_sem=rsem,
            device_id=dev, device_id_type=MESH,
        )

    def send(src, dst, ssem, rsem, dev):
        c = remote(src, dst, ssem, rsem, dev)
        c.start()
        sends.append(c)

    def arrived(dst, rsem):
        remote(dst, dst, rsem, rsem, other_core).wait_recv()

    loads = [
        pltpu.make_async_copy(proj_q.at[t], pq.at[f, t], loc.at[0]),
        pltpu.make_async_copy(proj_o.at[t], po.at[f, t], loc.at[1]),
        pltpu.make_async_copy(inputs, x_in, loc.at[2]),
        pltpu.make_async_copy(attended, x_at, loc.at[3]),
        pltpu.make_async_copy(query_cot, c_q, loc.at[4]),
        pltpu.make_async_copy(output_cot, c_o, loc.at[5]),
        pltpu.make_async_copy(first_q, fst.at[0, :, pl.ds(0, 512)], loc.at[6]),
        pltpu.make_async_copy(first_o.at[:, pl.ds(0, 256)], fst.at[0, :, pl.ds(512, 256)], loc.at[7]),
        pltpu.make_async_copy(first_o.at[:, pl.ds(256, 768)], fst.at[1], loc.at[8]),
        pltpu.make_async_copy(second_q, snd.at[0, :, pl.ds(0, 512)], loc.at[9]),
        pltpu.make_async_copy(second_o.at[:, pl.ds(0, 256)], snd.at[0, :, pl.ds(512, 256)], loc.at[10]),
        pltpu.make_async_copy(second_o.at[:, pl.ds(256, 768)], snd.at[1], loc.at[11]),
        pltpu.make_async_copy(w_q.at[p], old_q, loc.at[12]),
        pltpu.make_async_copy(w_o.at[p], old_o, loc.at[13]),
    ]
    for c in loads:
        c.start()

    barrier = pltpu.get_barrier_semaphore()
    peers = [at_z(d) for d in range(1, NZ)] + [at_x(e) for e in range(1, NX)]
    peers += [at_y(s) for s in range(1, NY)] + [other_core]
    for dev in peers:
        pl.semaphore_signal(barrier, inc=1, device_id=dev, device_id_type=MESH)
    pl.semaphore_wait(barrier, len(peers))

    loads[0].wait()
    loads[1].wait()
    for d in NEAR_FIRST:
        send(pq.at[f, t], pq.at[f, t], a_zs.at[0, d], a_zr.at[0, d], at_z(d))
        send(po.at[f, t], po.at[f, t], a_zs.at[1, d], a_zr.at[1, d], at_z(d))
    for d in (0,) + NEAR_FIRST:
        g = ((z + NZ - d) % NZ) * NX + x
        if d:
            arrived(pq.at[g, t], a_zr.at[0, d])
            arrived(po.at[g, t], a_zr.at[1, d])
        for e in range(1, NX):
            send(pq.at[g, t], pq.at[g, t], a_xs.at[0, d, e], a_xr.at[0, d, e], at_x(e))
            send(po.at[g, t], po.at[g, t], a_xs.at[1, d, e], a_xr.at[1, d, e], at_x(e))

    for c in loads[12:14]:
        c.wait()
    code_q[...] = coded(old_q[...])
    code_o[...] = coded(old_o[...])
    out_q = pltpu.make_async_copy(code_q, wg_q.at[f, p], loc.at[12])
    out_o = pltpu.make_async_copy(code_o, wg_o.at[f, p], loc.at[13])
    out_q.start()
    out_o.start()
    for e in range(1, NX):
        send(code_q, wg_q.at[f, p], w_xs.at[0, e], w_xr.at[0, e], at_x(e))
        send(code_o, wg_o.at[f, p], w_xs.at[1, e], w_xr.at[1, e], at_x(e))

    for d in (0,) + NEAR_FIRST:
        row = ((z + NZ - d) % NZ) * NX
        for e in range(1, NX):
            g = row + (x + NX - e) % NX
            arrived(pq.at[g, t], a_xr.at[0, d, e])
            arrived(po.at[g, t], a_xr.at[1, d, e])
        for k, ref in enumerate((pq, po)):
            part = ref.at[pl.ds(row, NX), t]
            send(part, part, a_cs.at[k, d], a_cr.at[k, d], other_core)
    for d in (0,) + NEAR_FIRST:
        row = ((z + NZ - d) % NZ) * NX
        for k, ref in enumerate((pq, po)):
            arrived(ref.at[pl.ds(row, NX), 1 - t], a_cr.at[k, d])

    for c in loads[2:6]:
        c.wait()

    def partial_low(tokens, whole, cot, depth):
        reduced = jnp.dot(
            tokens[...], whole[...].reshape(depth, RANK), preferred_element_type=jnp.float32
        )
        high = reduced.astype(jnp.bfloat16)
        rest = (reduced - high.astype(jnp.float32)).astype(jnp.bfloat16)
        both = jnp.concatenate([high, rest], axis=0)
        return lax.dot_general(
            both, jnp.concatenate([cot, cot], axis=0),
            (((0,), (0,)), ((), ())), preferred_element_type=jnp.float32,
        )

    def put(par, lo, block):
        for zz in range(NZ):
            for xx in range(NX):
                r = (zz * NX + xx) * 8
                lb[par, xx, zz, :, lo : lo + block.shape[1]] = block[r : r + 8, :]

    low_o = partial_low(x_at, po, c_o[...], DA)
    put(0, 512, low_o[:, :256])
    put(1, 0, low_o[:, 256:])
    put(0, 0, partial_low(x_in, pq, c_q[...], D))

    for j in range(NX):
        cb[j] = coded(lb[o, j])
        send(cb.at[j], by.at[j], b_ys.at[j], b_yr.at[j], at_y(1 if j < 2 else -1 + NY))

    def weights(s):
        if s == 0:
            out_q.wait()
            out_o.wait()
            for e in range(1, NX):
                g = z * NX + (x + NX - e) % NX
                arrived(wg_q.at[g, p], w_xr.at[0, e])
                arrived(wg_o.at[g, p], w_xr.at[1, e])
        groups = []
        for way, sign in ((0, 1), (1, -1)):
            row = ((z - sign * s + NZ) % NZ) * NX
            for k, ref in enumerate((wg_q, wg_o)):
                if s == 4 and way != k:
                    continue
                part = ref.at[pl.ds(row, NX), p]
                if s:
                    arrived(part, w_zr.at[way, k, s])
                if s < 3 or (s == 3 and way == k):
                    send(part, part, w_zs.at[way, k, s + 1], w_zr.at[way, k, s + 1], at_z(sign % NZ))
                if s or way == 0:
                    groups.append((way, k, ref, row))
        for way, k, ref, row in groups:
            for side in range(2):
                two = ref.at[pl.ds(row + 2 * side, 2), p]
                send(two, two, w_ys.at[way, k, s, side], w_yr.at[way, k, s, side],
                     at_y(1 if side == 0 else NY - 1))

    def weights_y(s):
        for way, sign in ((0, 1), (1, -1)):
            row = ((z - sign * s + NZ) % NZ) * NX
            for k, ref in enumerate((wg_q, wg_o)):
                if (s == 4 and way != k) or (s == 0 and way):
                    continue
                for side in range(2):
                    arrived(ref.at[pl.ds(row + 2 * side, 2), o], w_yr.at[way, k, s, side])

    weights(0)

    for e in (1, 2, 3, 0):
        j = (x + e) % NX
        arrived(by.at[j], b_yr.at[j])
        lb[p, j] = lb[p, j] + decoded(by[j])
        if e:
            cb[NX + e - 1] = coded(lb[p, j])
            send(cb.at[NX + e - 1], bx.at[e - 1], b_xs.at[e - 1], b_xr.at[e - 1], at_x(e))
    weights(1)
    for e in range(3):
        arrived(bx.at[e], b_xr.at[e])
    mine = (lb[p, x] + decoded(bx[0])) + (decoded(bx[1]) + decoded(bx[2]))
    lb[o, 0] = mine
    sz[...] = coded(mine)
    for d in NEAR_FIRST:
        send(sz.at[(z + d) % NZ], bz.at[d - 1], b_zs.at[d - 1], b_zr.at[d - 1], at_z(d))
    weights(2)
    for d in NEAR_FIRST:
        arrived(bz.at[d - 1], b_zr.at[d - 1])
    mine = lb[o, 0, z]
    for d in range(7):
        mine = mine + decoded(bz[d])
    ty[...] = mine
    send(ty, by2, b_2s.at[0], b_2r.at[0], at_y(2))
    for c in loads[6:12]:
        c.wait()
    arrived(by2, b_2r.at[0])

    low_sum = mine + by2[...]
    low[p] = low_sum
    _, _, normed = moment_update(low_sum, fst[p], snd[p])
    half[f, :, pl.ds(pl.multiple_of(p * HALF, 256), HALF)] = normed.astype(jnp.bfloat16)
    square = normed * normed
    total = square[:, 0:128]
    for k in range(1, 6):
        total = total + square[:, k * 128 : (k + 1) * 128]
    qc[0] = total

    def piece(g, n, par):
        return half.at[pl.ds(g, n), :, pl.ds(pl.multiple_of(par * HALF, 256), HALF)]

    send(qc.at[0], qc.at[1], q_cs.at[0], q_cr.at[0], other_core)
    for d in NEAR_FIRST:
        send(piece(f, 1, p), piece(f, 1, p), e_zs.at[d], e_zr.at[d], at_z(d))
    send(low.at[p], low.at[p], b_ls.at[0], b_lr.at[0], at_y(1))
    arrived(qc.at[1], q_cr.at[0])
    qz[z] = total + qc[1]
    for d in NEAR_FIRST:
        send(qz.at[z], qz.at[z], q_zs.at[d], q_zr.at[d], at_z(d))
    for d in (0,) + NEAR_FIRST:
        g = ((z + NZ - d) % NZ) * NX + x
        if d:
            arrived(piece(g, 1, p), e_zr.at[d])
        for e in range(1, NX):
            send(piece(g, 1, p), piece(g, 1, p), e_xs.at[d, e], e_xr.at[d, e], at_x(e))
    for d in NEAR_FIRST:
        arrived(qz.at[(z + NZ - d) % NZ], q_zr.at[d])
    total = qz[0]
    for k in range(1, NZ):
        total = total + qz[k]
    qx[x] = total
    for e in range(1, NX):
        send(qx.at[x], qx.at[x], q_xs.at[e], q_xr.at[e], at_x(e))
    for d in (0,) + NEAR_FIRST:
        row = ((z + NZ - d) % NZ) * NX
        for e in range(1, NX):
            arrived(piece(row + (x + NX - e) % NX, 1, p), e_xr.at[d, e])
        for side in range(2):
            two = piece(row + 2 * side, 2, p)
            send(two, two, e_ys.at[d, side], e_yr.at[d, side], at_y(1 if side == 0 else NY - 1))
    for e in range(1, NX):
        arrived(qx.at[(x + NX - e) % NX], q_xr.at[e])
    qy[p] = (qx[0] + qx[1]) + (qx[2] + qx[3])
    send(qy.at[p], qy.at[p], q_ys.at[0], q_yr.at[0], at_y(1))
    weights(3)
    arrived(low.at[o], b_lr.at[0])
    arrived(qy.at[o], q_yr.at[0])
    total = jnp.sum(qy[0] + qy[1])
    scale[...] = lax.rsqrt(jnp.full((8, 128), total) / (RANK * (DA + D)) + mean_eps)
    for d in (0,) + NEAR_FIRST:
        row = ((z + NZ - d) % NZ) * NX
        for side in range(2):
            arrived(piece(row + 2 * side, 2, o), e_yr.at[d, side])
    weights(4)
    for s in range(5):
        weights_y(s)
    for c in sends:
        c.wait_send()


def gathered(inputs, query_cot, attended, output_cot, proj_q, proj_o, w_q, w_o,
             first_q, second_q, first_o, second_o):
    f32, bf16 = jnp.float32, jnp.bfloat16
    vmem = pl.BlockSpec(memory_space=pltpu.VMEM)
    anywhere = pl.BlockSpec(memory_space=pl.ANY)
    dma = pltpu.SemaphoreType.DMA
    return pl.pallas_call(
        comm_kernel,
        out_shape=(
            jax.ShapeDtypeStruct((32, 2, 32, RANK), bf16),
            jax.ShapeDtypeStruct((32, 2, 16, RANK), bf16),
            jax.ShapeDtypeStruct((32, 8, 2 * HALF), bf16),
            jax.ShapeDtypeStruct((2, 8, HALF), f32),
            jax.ShapeDtypeStruct((8, 128), f32),
            jax.ShapeDtypeStruct((32, 2, 32, 512), bf16),
            jax.ShapeDtypeStruct((32, 2, 16, 1024), bf16),
        ),
        in_specs=[anywhere] * 12,
        out_specs=(vmem, vmem, vmem, vmem, vmem, anywhere, anywhere),
        scratch_shapes=[
            pltpu.VMEM((128, D), bf16),
            pltpu.VMEM((128, 512), bf16),
            pltpu.VMEM((128, DA), bf16),
            pltpu.VMEM((128, 1024), bf16),
            pltpu.VMEM((2, 8, HALF), f32),
            pltpu.VMEM((2, 8, HALF), f32),
            pltpu.VMEM((32, 512), f32),
            pltpu.VMEM((16, 1024), f32),
            pltpu.VMEM((32, 512), bf16),
            pltpu.VMEM((16, 1024), bf16),
            pltpu.VMEM((2, NX, NZ, 8, HALF), f32),
            pltpu.VMEM((7, NZ, 8, HALF), bf16),
            pltpu.VMEM((NX, NZ, 8, HALF), bf16),
            pltpu.VMEM((3, NZ, 8, HALF), bf16),
            pltpu.VMEM((NZ, 8, HALF), bf16),
            pltpu.VMEM((7, 8, HALF), bf16),
            pltpu.VMEM((8, HALF), f32),
            pltpu.VMEM((8, HALF), f32),
            pltpu.VMEM((2, 8, 128), f32),
            pltpu.VMEM((NZ, 8, 128), f32),
            pltpu.VMEM((NX, 8, 128), f32),
            pltpu.VMEM((2, 8, 128), f32),
            dma((14,)),
            dma((2, 8)), dma((2, 8)), dma((2, 8, 4)), dma((2, 8, 4)), dma((2, 8)), dma((2, 8)),
            dma((2, 4)), dma((2, 4)), dma((2, 2, 5)), dma((2, 2, 5)), dma((2, 2, 5, 2)), dma((2, 2, 5, 2)),
            dma((4,)), dma((4,)), dma((3,)), dma((3,)), dma((7,)), dma((7,)),
            dma((1,)), dma((1,)), dma((1,)), dma((1,)),
            dma((8,)), dma((8,)), dma((8, 4)), dma((8, 4)), dma((8, 2)), dma((8, 2)),
            dma((1,)), dma((1,)), dma((8,)), dma((8,)), dma((4,)), dma((4,)), dma((1,)), dma((1,)),
        ],
        compiler_params=pltpu.CompilerParams(collective_id=0, has_side_effects=True),
    )(
        inputs, query_cot, attended, output_cot,
        proj_q.reshape(2, 32, RANK), proj_o.reshape(2, 16, RANK),
        w_q, w_o, first_q, second_q, first_o, second_o,
    )


def local(
    inputs, query_cot, attended, output_cot, proj_query, proj_output,
    weight_query, weight_output, first_query, second_query, first_output, second_output,
):
    pq, po, half, low, scale_tile, wg_q, wg_o = gathered(
        inputs, query_cot, attended, output_cot, proj_query, proj_output,
        weight_query.reshape(2, 32, 512), weight_output.reshape(2, 16, 1024),
        first_query, second_query, first_output, second_output,
    )
    whole_q, whole_o = pq.reshape(D, RANK), po.reshape(DA, RANK)
    half = half.reshape(RANK, 2 * HALF)
    half_q, half_o = half[:, :512], half[:, 512:]
    scale = scale_tile[0, 0]
    low_q = low[0, :, :512]
    low_o = jnp.concatenate([low[0, :, 512:], low[1]], axis=1)
    first_q, second_q, _ = moment_update(low_q, first_query, second_query)
    first_o, second_o, _ = moment_update(low_o, first_output, second_output)
    step_q = scale * jnp.dot(proj_query, half_q, preferred_element_type=jnp.float32)
    step_o = scale * jnp.dot(proj_output, half_o, preferred_element_type=jnp.float32)
    new_q = weight_query - learn_rate * step_q
    new_o = weight_output - learn_rate * step_o
    all_q = scale * jnp.dot(whole_q, half_q, preferred_element_type=jnp.float32)
    all_o = scale * jnp.dot(whole_o, half_o, preferred_element_type=jnp.float32)
    old_q = decoded(wg_q.reshape(D, 512))
    old_o = decoded(wg_o.reshape(DA, 1024))
    copy_q = (old_q - learn_rate * all_q).astype(jnp.bfloat16)
    copy_o = (old_o - learn_rate * all_o).astype(jnp.bfloat16)
    return (new_q, new_o, step_q, step_o, first_q, second_q, first_o, second_o, copy_q, copy_o)


def solution(mesh):
    return jax.shard_map(
        local,
        mesh=mesh,
        in_specs=(
            P(("fs", "rep"), None),
            P(("fs", "rep"), "tp"),
            P(("fs", "rep"), None),
            P(("fs", "rep"), "tp"),
            P("fs", None),
            P("fs", None),
            P("fs", "tp"),
            P("fs", "tp"),
            P("fs", "tp"),
            P("fs", "tp"),
            P("fs", "tp"),
            P("fs", "tp"),
        ),
        out_specs=(
            P("fs", "tp"),
            P("fs", "tp"),
            P("fs", "tp"),
            P("fs", "tp"),
            P("fs", "tp"),
            P("fs", "tp"),
            P("fs", "tp"),
            P("fs", "tp"),
            P(None, "tp"),
            P(None, "tp"),
        ),
        check_vma=False,
    )
```

```python
import functools

import jax
import jax.numpy as jnp
from jax import lax
from jax.experimental import pallas as pl
from jax.experimental.pallas import tpu as pltpu
from jax.sharding import PartitionSpec as P

D = 2048
DA = 1024
RANK = 256
NZ, NX, NY = 8, 4, 4

beta_first = 0.9
beta_second = 0.95
adam_eps = 1e-08
mean_eps = 1e-06
learn_rate = 0.02
HALF = 768

MESH = pl.DeviceIdType.MESH
NEAR_FIRST = (1, 7, 2, 6, 3, 5, 4)


def moment_update(low_sum, first, second):
    first_new = beta_first * first + (1.0 - beta_first) * low_sum
    second_new = beta_second * second + (1.0 - beta_second) * low_sum * low_sum
    normed = first_new / (jnp.sqrt(second_new) + adam_eps)
    return (first_new, second_new, normed)


def coded(v):
    square = v * v
    fourth = jnp.maximum(square * square, 1e-36)
    return jnp.where(v < 0, -fourth, fourth).astype(jnp.bfloat16)


def decoded(c):
    c = c.astype(jnp.float32)
    root = c * lax.rsqrt(jnp.abs(c))
    return root * lax.rsqrt(jnp.abs(root))


def comm_kernel(
    inputs, query_cot, attended, output_cot, proj_q, proj_o, w_q, w_o,
    first_q, second_q, first_o, second_o,
    pq_out, po_out, half_out, low_out, total_out, wg_q, wg_o,
    pq, po, half, low,
    x_in, c_q, x_at, c_o, fst, snd, old_q, old_o, code_q, code_o,
    lb, cb, by, bx, sz, bz, ty, by2, qz, qx, qy, qt,
    loc, a_zs, a_zr, a_xs, a_xr, a_cs, a_cr,
    w_xs, w_xr, w_zs, w_zr, w_ys, w_yr,
    b_ys, b_yr, b_xs, b_xr, b_zs, b_zr, b_2s, b_2r, b_ls, b_lr,
    e_zs, e_zr, e_xs, e_xr, e_ys, e_yr,
    q_zs, q_zr, q_xs, q_xr, q_ys, q_yr,
):
    f = lax.axis_index("fs")
    y = lax.axis_index("rep")
    t = lax.axis_index("tp")
    z = f // NX
    x = f % NX
    p = y % 2
    o = 1 - p

    def at_z(d):
        return {"fs": ((z + d) % NZ) * NX + x}

    def at_zt(d):
        return {"fs": ((z + d) % NZ) * NX + x, "tp": 1 - t}

    def at_x(e):
        return {"fs": z * NX + (x + e) % NX}

    def at_y(s):
        return {"rep": (y + s) % NY}

    other_core = {"tp": 1 - t}
    sends = []

    def remote(src, dst, ssem, rsem, dev):
        return pltpu.make_async_remote_copy(
            src_ref=src, dst_ref=dst, send_sem=ssem, recv_sem=rsem,
            device_id=dev, device_id_type=MESH,
        )

    def send(src, dst, ssem, rsem, dev):
        c = remote(src, dst, ssem, rsem, dev)
        c.start()
        sends.append(c)

    def arrived(dst, rsem):
        remote(dst, dst, rsem, rsem, other_core).wait_recv()

    loads = [
        pltpu.make_async_copy(proj_q.at[t], pq.at[f, t], loc.at[0]),
        pltpu.make_async_copy(proj_o.at[t], po.at[f, t], loc.at[1]),
        pltpu.make_async_copy(w_q.at[p], old_q, loc.at[12]),
        pltpu.make_async_copy(w_o.at[p], old_o, loc.at[13]),
        pltpu.make_async_copy(inputs, x_in, loc.at[2]),
        pltpu.make_async_copy(attended, x_at, loc.at[3]),
        pltpu.make_async_copy(query_cot, c_q, loc.at[4]),
        pltpu.make_async_copy(output_cot, c_o, loc.at[5]),
        pltpu.make_async_copy(first_q, fst.at[0, :, pl.ds(0, 512)], loc.at[6]),
        pltpu.make_async_copy(first_o.at[:, pl.ds(0, 256)], fst.at[0, :, pl.ds(512, 256)], loc.at[7]),
        pltpu.make_async_copy(first_o.at[:, pl.ds(256, 768)], fst.at[1], loc.at[8]),
        pltpu.make_async_copy(second_q, snd.at[0, :, pl.ds(0, 512)], loc.at[9]),
        pltpu.make_async_copy(second_o.at[:, pl.ds(0, 256)], snd.at[0, :, pl.ds(512, 256)], loc.at[10]),
        pltpu.make_async_copy(second_o.at[:, pl.ds(256, 768)], snd.at[1], loc.at[11]),
    ]
    for c in loads:
        c.start()

    barrier = pltpu.get_barrier_semaphore()
    peers = [at_z(d) for d in range(1, NZ)] + [at_zt(d) for d in range(1, NZ)]
    peers += [at_x(e) for e in range(1, NX)]
    peers += [at_y(s) for s in range(1, NY)] + [other_core]
    for dev in peers:
        pl.semaphore_signal(barrier, inc=1, device_id=dev, device_id_type=MESH)
    for c in loads[:4]:
        c.wait()
    code_q[...] = coded(old_q[...])
    code_o[...] = coded(old_o[...])
    own_q = pltpu.make_async_copy(code_q, wg_q.at[f, p], loc.at[12])
    own_o = pltpu.make_async_copy(code_o, wg_o.at[f, p], loc.at[13])
    own_q.start()
    own_o.start()
    pl.semaphore_wait(barrier, len(peers))

    for d in NEAR_FIRST:
        send(pq.at[f, t], pq.at[f, t], a_zs.at[0, d], a_zr.at[0, d], at_z(d))
        send(po.at[f, t], po.at[f, t], a_zs.at[1, d], a_zr.at[1, d], at_z(d))

    def factors_x(d):
        g = ((z + NZ - d) % NZ) * NX + x
        if d:
            arrived(pq.at[g, t], a_zr.at[0, d])
            arrived(po.at[g, t], a_zr.at[1, d])
        for e in (2, 1, 3):
            send(pq.at[g, t], pq.at[g, t], a_xs.at[0, d, e], a_xr.at[0, d, e], at_x(e))
            send(po.at[g, t], po.at[g, t], a_xs.at[1, d, e], a_xr.at[1, d, e], at_x(e))

    factors_x(0)
    for e in range(1, NX):
        send(code_q, wg_q.at[f, p], w_xs.at[0, e], w_xr.at[0, e], at_x(e))
        send(code_o, wg_o.at[f, p], w_xs.at[1, e], w_xr.at[1, e], at_x(e))
    for d in NEAR_FIRST:
        factors_x(d)

    def weight_rows(s):
        for way, sign in ((0, 1), (1, -1)):
            row = ((z - sign * s + NZ) % NZ) * NX
            for k, ref in enumerate((wg_q, wg_o)):
                if (s == 4 and way != k) or (s == 0 and way):
                    continue
                yield way, k, ref, row

    def weights_z(s):
        if s == 0:
            own_q.wait()
            own_o.wait()
            for e in range(1, NX):
                g = z * NX + (x + NX - e) % NX
                arrived(wg_q.at[g, p], w_xr.at[0, e])
                arrived(wg_o.at[g, p], w_xr.at[1, e])
        for way, k, ref, row in weight_rows(s):
            part = ref.at[pl.ds(row, NX), p]
            if s:
                arrived(part, w_zr.at[way, k, s])
            for w, sign in ((0, 1), (1, -1)):
                if (s == 0 or w == way) and (s < 3 or (s == 3 and way == k)):
                    send(part, part, w_zs.at[w, k, s + 1], w_zr.at[w, k, s + 1], at_z(sign % NZ))

    def weights_y(s):
        for way, k, ref, row in weight_rows(s):
            for side in range(2):
                two = ref.at[pl.ds(row + 2 * side, 2), p]
                send(two, two, w_ys.at[way, k, s, side], w_yr.at[way, k, s, side],
                     at_y(1 if side == 0 else NY - 1))

    def weights_done(s):
        for way, k, ref, row in weight_rows(s):
            for side in range(2):
                arrived(ref.at[pl.ds(row + 2 * side, 2), o], w_yr.at[way, k, s, side])

    weights_z(0)
    weights_y(0)

    for d in (0,) + NEAR_FIRST:
        row = ((z + NZ - d) % NZ) * NX
        for e in range(1, NX):
            g = row + (x + NX - e) % NX
            arrived(pq.at[g, t], a_xr.at[0, d, e])
            arrived(po.at[g, t], a_xr.at[1, d, e])
        for k, ref in enumerate((pq, po)):
            part = ref.at[pl.ds(row, NX), t]
            send(part, part, a_cs.at[k, d], a_cr.at[k, d], other_core)
    for d in (0,) + NEAR_FIRST:
        row = ((z + NZ - d) % NZ) * NX
        for k, ref in enumerate((pq, po)):
            arrived(ref.at[pl.ds(row, NX), 1 - t], a_cr.at[k, d])
    outs = [
        pltpu.make_async_copy(pq, pq_out, loc.at[0]),
        pltpu.make_async_copy(po, po_out, loc.at[1]),
    ]
    for c in outs:
        c.start()

    for c in loads[4:8]:
        c.wait()

    def partial_low(tokens, whole, cot, depth):
        reduced = jnp.dot(
            tokens[...], whole[...].reshape(depth, RANK), preferred_element_type=jnp.float32
        )
        high = reduced.astype(jnp.bfloat16)
        rest = (reduced - high.astype(jnp.float32)).astype(jnp.bfloat16)
        both = jnp.concatenate([high, rest], axis=0)
        return lax.dot_general(
            both, jnp.concatenate([cot, cot], axis=0),
            (((0,), (0,)), ((), ())), preferred_element_type=jnp.float32,
        )

    def put(par, lo, block):
        for zz in range(NZ):
            for xx in range(NX):
                r = (zz * NX + xx) * 8
                lb[par, xx, zz, :, lo : lo + block.shape[1]] = block[r : r + 8, :]

    low_o = partial_low(x_at, po, c_o[...], DA)
    put(0, 512, low_o[:, :256])
    put(1, 0, low_o[:, 256:])
    put(0, 0, partial_low(x_in, pq, c_q[...], D))

    chunks = (
        (2, 0, 8, 1), (3, 0, 8, NY - 1), (1, 0, 4, 1), (1, 4, 4, NY - 1), (0, 0, 4, 1), (0, 4, 4, NY - 1),
    )
    for n, (e, lo, rows, step) in enumerate(chunks):
        part = (x + e) % NX, pl.ds(lo, rows)
        cb[part] = coded(lb[(o,) + part])
        send(cb.at[part], by.at[part], b_ys.at[n], b_yr.at[n], at_y(step))
    weights_z(1)
    weights_y(1)

    for n, (e, lo, rows, step) in enumerate(chunks):
        j = (x + e) % NX
        part = j, pl.ds(lo, rows)
        arrived(by.at[part], b_yr.at[n])
        lb[(p,) + part] = lb[(p,) + part] + decoded(by[part])
        if e and lo + rows == NZ:
            cb[NX + e - 1] = coded(lb[p, j])
            send(cb.at[NX + e - 1], bx.at[e - 1], b_xs.at[e - 1], b_xr.at[e - 1], at_x(e))
    weights_z(2)
    for e in (1, 2, 0):
        arrived(bx.at[e], b_xr.at[e])
    mine = (lb[p, x] + decoded(bx[0])) + (decoded(bx[1]) + decoded(bx[2]))
    lb[o, 0] = mine
    sz[...] = coded(mine)
    for d in (4, 3, 5, 2, 6, 1, 7):
        send(sz.at[(z + d) % NZ], bz.at[d - 1], b_zs.at[d - 1], b_zr.at[d - 1], at_z(d))
    weights_y(2)
    weights_z(3)
    for d in NEAR_FIRST:
        arrived(bz.at[d - 1], b_zr.at[d - 1])
    mine = lb[o, 0, z]
    for d in range(7):
        mine = mine + decoded(bz[d])
    ty[...] = mine
    send(ty, by2, b_2s.at[0], b_2r.at[0], at_y(2))
    for c in loads[8:14]:
        c.wait()
    arrived(by2, b_2r.at[0])

    low_sum = mine + by2[...]
    low[p] = low_sum
    _, _, normed = moment_update(low_sum, fst[p], snd[p])
    half[f, :, pl.ds(pl.multiple_of(p * HALF, 256), HALF)] = normed.astype(jnp.bfloat16)
    square = normed * normed
    total = square[:, 0:128]
    for k in range(1, 6):
        total = total + square[:, k * 128 : (k + 1) * 128]
    qz[z * 2 + t] = jnp.sum(total, axis=0, keepdims=True)

    def piece(g, n, par):
        return half.at[pl.ds(g, n), :, pl.ds(pl.multiple_of(par * HALF, 256), HALF)]

    def square_z(d, core):
        return ((z + NZ - d) % NZ) * 2 + (t if core == 0 else 1 - t)

    for d in NEAR_FIRST:
        send(piece(f, 1, p), piece(f, 1, p), e_zs.at[d], e_zr.at[d], at_z(d))
    for d in range(NZ):
        for core, dev in ((0, at_z(d)), (1, at_zt(d) if d else other_core)):
            if d or core:
                row = qz.at[z * 2 + t]
                send(row, row, q_zs.at[d, core], q_zr.at[d, core], dev)
    send(low.at[p], low.at[p], b_ls.at[0], b_lr.at[0], at_y(1))
    for d in (0,) + NEAR_FIRST:
        g = ((z + NZ - d) % NZ) * NX + x
        if d:
            arrived(piece(g, 1, p), e_zr.at[d])
        for e in (2, 1, 3):
            send(piece(g, 1, p), piece(g, 1, p), e_xs.at[d, e], e_xr.at[d, e], at_x(e))
    for d in range(NZ):
        for core in range(2):
            if d or core:
                arrived(qz.at[square_z(d, core)], q_zr.at[d, core])
    total = qz[0]
    for k in range(1, 2 * NZ):
        total = total + qz[k]
    qx[x] = total
    for e in (2, 1, 3):
        send(qx.at[x], qx.at[x], q_xs.at[e], q_xr.at[e], at_x(e))
    for d in (0,) + NEAR_FIRST:
        row = ((z + NZ - d) % NZ) * NX
        for e in range(1, NX):
            arrived(piece(row + (x + NX - e) % NX, 1, p), e_xr.at[d, e])
        for side in range(2):
            two = piece(row + 2 * side, 2, p)
            send(two, two, e_ys.at[d, side], e_yr.at[d, side], at_y(1 if side == 0 else NY - 1))
    for e in range(1, NX):
        arrived(qx.at[(x + NX - e) % NX], q_xr.at[e])
    qy[p] = (qx[0] + qx[1]) + (qx[2] + qx[3])
    send(qy.at[p], qy.at[p], q_ys.at[0], q_yr.at[0], at_y(1))
    weights_y(3)
    weights_z(4)
    weights_y(4)
    arrived(low.at[o], b_lr.at[0])
    for d in (0,) + NEAR_FIRST:
        row = ((z + NZ - d) % NZ) * NX
        for side in range(2):
            arrived(piece(row + 2 * side, 2, o), e_yr.at[d, side])
    arrived(qy.at[o], q_yr.at[0])
    qt[...] = qy[0] + qy[1]
    outs += [
        pltpu.make_async_copy(half, half_out, loc.at[2]),
        pltpu.make_async_copy(low, low_out, loc.at[3]),
        pltpu.make_async_copy(qt, total_out, loc.at[4]),
    ]
    for c in outs[2:]:
        c.start()
    for s in range(5):
        weights_done(s)
    for c in outs:
        c.wait()
    for c in sends:
        c.wait_send()


def gathered(inputs, query_cot, attended, output_cot, proj_q, proj_o, w_q, w_o,
             first_q, second_q, first_o, second_o):
    f32, bf16 = jnp.float32, jnp.bfloat16
    anywhere = pl.BlockSpec(memory_space=pl.ANY)
    dma = pltpu.SemaphoreType.DMA
    shared = (
        ((32, 2, 32, RANK), bf16),
        ((32, 2, 16, RANK), bf16),
        ((32, 8, 2 * HALF), bf16),
        ((2, 8, HALF), f32),
    )
    return pl.pallas_call(
        comm_kernel,
        out_shape=tuple(jax.ShapeDtypeStruct(*s) for s in shared) + (
            jax.ShapeDtypeStruct((1, 128), f32),
            jax.ShapeDtypeStruct((32, 2, 32, 512), bf16),
            jax.ShapeDtypeStruct((32, 2, 16, 1024), bf16),
        ),
        in_specs=[anywhere] * 12,
        out_specs=(anywhere,) * 7,
        scratch_shapes=[pltpu.VMEM(*s) for s in shared] + [
            pltpu.VMEM((128, D), bf16),
            pltpu.VMEM((128, 512), bf16),
            pltpu.VMEM((128, DA), bf16),
            pltpu.VMEM((128, 1024), bf16),
            pltpu.VMEM((2, 8, HALF), f32),
            pltpu.VMEM((2, 8, HALF), f32),
            pltpu.VMEM((32, 512), f32),
            pltpu.VMEM((16, 1024), f32),
            pltpu.VMEM((32, 512), bf16),
            pltpu.VMEM((16, 1024), bf16),
            pltpu.VMEM((2, NX, NZ, 8, HALF), f32),
            pltpu.VMEM((7, NZ, 8, HALF), bf16),
            pltpu.VMEM((NX, NZ, 8, HALF), bf16),
            pltpu.VMEM((3, NZ, 8, HALF), bf16),
            pltpu.VMEM((NZ, 8, HALF), bf16),
            pltpu.VMEM((7, 8, HALF), bf16),
            pltpu.VMEM((8, HALF), f32),
            pltpu.VMEM((8, HALF), f32),
            pltpu.VMEM((2 * NZ, 1, 128), f32),
            pltpu.VMEM((NX, 1, 128), f32),
            pltpu.VMEM((2, 1, 128), f32),
            pltpu.VMEM((1, 128), f32),
            dma((14,)),
            dma((2, 8)), dma((2, 8)), dma((2, 8, 4)), dma((2, 8, 4)), dma((2, 8)), dma((2, 8)),
            dma((2, 4)), dma((2, 4)), dma((2, 2, 5)), dma((2, 2, 5)), dma((2, 2, 5, 2)), dma((2, 2, 5, 2)),
            dma((6,)), dma((6,)), dma((3,)), dma((3,)), dma((7,)), dma((7,)),
            dma((1,)), dma((1,)), dma((1,)), dma((1,)),
            dma((8,)), dma((8,)), dma((8, 4)), dma((8, 4)), dma((8, 2)), dma((8, 2)),
            dma((8, 2)), dma((8, 2)), dma((4,)), dma((4,)), dma((1,)), dma((1,)),
        ],
        compiler_params=pltpu.CompilerParams(collective_id=0, has_side_effects=True),
    )(
        inputs, query_cot, attended, output_cot,
        proj_q.reshape(2, 32, RANK), proj_o.reshape(2, 16, RANK),
        w_q.reshape(2, 32, 512), w_o.reshape(2, 16, 1024),
        first_q, second_q, first_o, second_o,
    )


def final_kernel(
    pq, po, wq, wo, half, low, total, proj_q, proj_o, weight_q, weight_o,
    first_q, second_q, first_o, second_o,
    new_q, new_o, step_q, step_o, nf_q, ns_q, nf_o, ns_o, copy_q, copy_o,
):
    mean = jnp.sum(total[...], axis=1, keepdims=True) / (RANK * (DA + D))
    scale = lax.rsqrt(mean + mean_eps)

    def step(factor, lo, width):
        rows = half[:, :, lo : lo + width].reshape(RANK, width)
        return scale * jnp.dot(factor, rows, preferred_element_type=jnp.float32)

    rows_q, rows_o = copy_q.shape[0], copy_o.shape[0]
    all_q = step(pq[...].reshape(rows_q, RANK), 0, 512)
    copy_q[...] = (decoded(wq[...].reshape(rows_q, 512)) - learn_rate * all_q).astype(jnp.bfloat16)
    all_o = step(po[...].reshape(rows_o, RANK), 512, 1024)
    copy_o[...] = (decoded(wo[...].reshape(rows_o, 1024)) - learn_rate * all_o).astype(jnp.bfloat16)

    @pl.when(pl.program_id(0) == 0)
    def _():
        mine_q = step(proj_q[...], 0, 512)
        step_q[...] = mine_q
        new_q[...] = weight_q[...] - learn_rate * mine_q
        mine_o = step(proj_o[...], 512, 1024)
        step_o[...] = mine_o
        new_o[...] = weight_o[...] - learn_rate * mine_o
        nf_q[...], ns_q[...], _ = moment_update(low[0, :, :512], first_q[...], second_q[...])
        nf_o[:, :256], ns_o[:, :256], _ = moment_update(
            low[0, :, 512:], first_o[:, :256], second_o[:, :256]
        )
        nf_o[:, 256:], ns_o[:, 256:], _ = moment_update(low[1], first_o[:, 256:], second_o[:, 256:])


STEPS = 8


def finished(pq, po, wq, wo, half, low, total, proj_q, proj_o, weight_q, weight_o,
             first_q, second_q, first_o, second_o):
    f32, bf16 = jnp.float32, jnp.bfloat16

    def blocks(shape):
        rest = (0,) * (len(shape) - 1)
        return pl.BlockSpec((shape[0] // STEPS,) + tuple(shape[1:]), lambda i: (i,) + rest)

    def whole(shape):
        return pl.BlockSpec(tuple(shape), lambda i: (0,) * len(shape))

    small = (half, low, total, proj_q, proj_o, weight_q, weight_o, first_q, second_q, first_o, second_o)
    outs = (
        ((64, 512), f32), ((32, 1024), f32), ((64, 512), f32), ((32, 1024), f32),
        ((8, 512), f32), ((8, 512), f32), ((8, 1024), f32), ((8, 1024), f32),
        ((D, 512), bf16), ((DA, 1024), bf16),
    )
    return pl.pallas_call(
        final_kernel,
        grid=(STEPS,),
        out_shape=tuple(jax.ShapeDtypeStruct(*s) for s in outs),
        in_specs=[blocks(a.shape) for a in (pq, po, wq, wo)] + [whole(a.shape) for a in small],
        out_specs=tuple(whole(s) for s, _ in outs[:8]) + tuple(blocks(s) for s, _ in outs[8:]),
        cost_estimate=pl.CostEstimate(flops=2_200_000_000, bytes_accessed=12_000_000, transcendentals=0),
    )(pq, po, wq, wo, *small)


def local(
    inputs, query_cot, attended, output_cot, proj_query, proj_output,
    weight_query, weight_output, first_query, second_query, first_output, second_output,
):
    pq, po, half, low, total, wg_q, wg_o = gathered(
        inputs, query_cot, attended, output_cot, proj_query, proj_output,
        weight_query, weight_output, first_query, second_query, first_output, second_output,
    )
    return finished(
        pq, po, wg_q, wg_o, half, low, total, proj_query, proj_output, weight_query, weight_output,
        first_query, second_query, first_output, second_output,
    )


def solution(mesh):
    return jax.shard_map(
        local,
        mesh=mesh,
        in_specs=(
            P(("fs", "rep"), None),
            P(("fs", "rep"), "tp"),
            P(("fs", "rep"), None),
            P(("fs", "rep"), "tp"),
            P("fs", None),
            P("fs", None),
            P("fs", "tp"),
            P("fs", "tp"),
            P("fs", "tp"),
            P("fs", "tp"),
            P("fs", "tp"),
            P("fs", "tp"),
        ),
        out_specs=(
            P("fs", "tp"),
            P("fs", "tp"),
            P("fs", "tp"),
            P("fs", "tp"),
            P("fs", "tp"),
            P("fs", "tp"),
            P("fs", "tp"),
            P("fs", "tp"),
            P(None, "tp"),
            P(None, "tp"),
        ),
        check_vma=False,
    )
```

```python
import functools

import jax
import jax.numpy as jnp
from jax import lax
from jax.experimental import pallas as pl
from jax.experimental.pallas import tpu as pltpu
from jax.sharding import PartitionSpec as P

D = 2048
DA = 1024
RANK = 256
NZ, NX, NY = 8, 4, 4

beta_first = 0.9
beta_second = 0.95
adam_eps = 1e-08
mean_eps = 1e-06
learn_rate = 0.02
HALF = 768

MESH = pl.DeviceIdType.MESH
NEAR_FIRST = (1, 7, 2, 6, 3, 5, 4)


def moment_update(low_sum, first, second):
    first_new = beta_first * first + (1.0 - beta_first) * low_sum
    second_new = beta_second * second + (1.0 - beta_second) * low_sum * low_sum
    normed = first_new / (jnp.sqrt(second_new) + adam_eps)
    return (first_new, second_new, normed)


def coded(v):
    square = v * v
    fourth = jnp.maximum(square * square, 1e-36)
    return jnp.where(v < 0, -fourth, fourth).astype(jnp.bfloat16)


def decoded(c):
    c = c.astype(jnp.float32)
    root = c * lax.rsqrt(jnp.abs(c))
    return root * lax.rsqrt(jnp.abs(root))


def comm_kernel(
    inputs, query_cot, attended, output_cot, proj_q, proj_o, w_q, w_o,
    first_q, second_q, first_o, second_o,
    pf_out, half_out, low_out, total_out, wg_q, wg_o,
    pf, half, low,
    x_in, c_q, x_at, c_o, fst, snd, old_q, old_o, code_q, code_o,
    lb, cb, by, bx, sz, bz, ty, by2, qz, qx, qy, qt,
    loc, sent, a_z, a_x, a_c, w_x, w_z, w_d, w_y, b_y, b_x, b_z, b_2, b_l,
    e_z, e_x, e_y, q_z, q_x, q_y,
):
    f = lax.axis_index("fs")
    y = lax.axis_index("rep")
    t = lax.axis_index("tp")
    z = f // NX
    x = f % NX
    p = y % 2
    o = 1 - p

    def at_z(d):
        return {"fs": ((z + d) % NZ) * NX + x}

    def at_zt(d):
        return {"fs": ((z + d) % NZ) * NX + x, "tp": 1 - t}

    def at_x(e):
        return {"fs": z * NX + (x + e) % NX}

    def at_y(s):
        return {"rep": (y + s) % NY}

    other_core = {"tp": 1 - t}

    def remote(src, dst, ssem, rsem, dev):
        return pltpu.make_async_remote_copy(
            src_ref=src, dst_ref=dst, send_sem=ssem, recv_sem=rsem,
            device_id=dev, device_id_type=MESH,
        )

    def send(src, dst, kind, rsem, dev):
        remote(src, dst, sent.at[kind], rsem, dev).start()

    def arrived(dst, rsem):
        remote(dst, dst, rsem, rsem, other_core).wait_recv()

    loads = [
        pltpu.make_async_copy(proj_q.at[t], pf.at[f, t, pl.ds(0, 32)], loc.at[0]),
        pltpu.make_async_copy(proj_o.at[t], pf.at[f, t, pl.ds(32, 16)], loc.at[1]),
        pltpu.make_async_copy(w_q.at[p], old_q, loc.at[12]),
        pltpu.make_async_copy(w_o.at[p], old_o, loc.at[13]),
        pltpu.make_async_copy(inputs, x_in, loc.at[2]),
        pltpu.make_async_copy(attended, x_at, loc.at[3]),
        pltpu.make_async_copy(query_cot, c_q, loc.at[4]),
        pltpu.make_async_copy(output_cot, c_o, loc.at[5]),
        pltpu.make_async_copy(first_q, fst.at[0, :, pl.ds(0, 512)], loc.at[6]),
        pltpu.make_async_copy(first_o.at[:, pl.ds(0, 256)], fst.at[0, :, pl.ds(512, 256)], loc.at[7]),
        pltpu.make_async_copy(first_o.at[:, pl.ds(256, 768)], fst.at[1], loc.at[8]),
        pltpu.make_async_copy(second_q, snd.at[0, :, pl.ds(0, 512)], loc.at[9]),
        pltpu.make_async_copy(second_o.at[:, pl.ds(0, 256)], snd.at[0, :, pl.ds(512, 256)], loc.at[10]),
        pltpu.make_async_copy(second_o.at[:, pl.ds(256, 768)], snd.at[1], loc.at[11]),
    ]
    for c in loads:
        c.start()

    barrier = pltpu.get_barrier_semaphore()
    peers = [at_z(d) for d in range(1, NZ)] + [at_zt(d) for d in range(1, NZ)]
    peers += [at_x(e) for e in range(1, NX)]
    peers += [at_y(s) for s in range(1, NY)] + [other_core]
    for dev in peers:
        pl.semaphore_signal(barrier, inc=1, device_id=dev, device_id_type=MESH)
    for c in loads[:4]:
        c.wait()
    code_q[...] = coded(old_q[...])
    code_o[...] = coded(old_o[...])
    own_q = pltpu.make_async_copy(code_q, wg_q.at[f, p], loc.at[12])
    own_o = pltpu.make_async_copy(code_o, wg_o.at[f, p], loc.at[13])
    own_q.start()
    own_o.start()
    pl.semaphore_wait(barrier, len(peers))

    for d in NEAR_FIRST:
        send(pf.at[f, t], pf.at[f, t], 0, a_z.at[d], at_z(d))

    def factors_x(d):
        g = ((z + NZ - d) % NZ) * NX + x
        if d:
            arrived(pf.at[g, t], a_z.at[d])
        for e in (2, 1, 3):
            send(pf.at[g, t], pf.at[g, t], 0, a_x.at[d], at_x(e))

    def rows_at(d):
        return ((z + NZ - d) % NZ) * NX

    def output_x(d):
        g = rows_at(d) + x
        if d:
            arrived(wg_o.at[g, p], w_d.at[d])
        src = wg_o.at[g, p] if d else code_o
        for e in (2, 1, 3):
            send(src, wg_o.at[g, p], 4, w_x.at[1 + d], at_x(e))

    def weights_y(k, d):
        ref = (wg_q, wg_o)[k]
        for side in range(2):
            two = ref.at[pl.ds(rows_at(d) + 2 * side, 2), p]
            send(two, two, 3 + 2 * k, w_y.at[k], at_y(1 if side == 0 else NY - 1))

    def output_y(d):
        arrived(wg_o.at[pl.ds(0, 3), p], w_x.at[1 + d])
        weights_y(1, d)

    def query_z(s):
        if s == 0:
            arrived(wg_q.at[pl.ds(0, 3), p], w_x.at[0])
            part = wg_q.at[pl.ds(rows_at(0), NX), p]
            send(part, part, 2, w_z.at[1, 0], at_z(1))
            send(part, part, 2, w_z.at[1, 1], at_z(NZ - 1))
            weights_y(0, 0)
            return
        if s == NZ // 2:
            for way in range(2):
                arrived(wg_q.at[pl.ds(rows_at(s) + 2 * way, 2), p], w_z.at[s, way])
            weights_y(0, s)
            return
        for way, sign in ((0, 1), (1, -1)):
            part = wg_q.at[pl.ds(rows_at(sign * s), NX), p]
            arrived(part, w_z.at[s, way])
            if s == NZ // 2 - 1:
                part = wg_q.at[pl.ds(rows_at(sign * s) + 2 * way, 2), p]
            send(part, part, 2, w_z.at[s + 1, way], at_z(sign % NZ))
        for sign in (1, -1):
            weights_y(0, sign * s)

    for d in NEAR_FIRST:
        send(code_o, wg_o.at[f, p], 4, w_d.at[d], at_z(d))
    factors_x(0)
    for e in (2, 1, 3):
        send(code_q, wg_q.at[f, p], 2, w_x.at[0], at_x(e))
    output_x(0)
    for d in NEAR_FIRST:
        factors_x(d)

    own_q.wait()
    own_o.wait()
    query_z(0)
    output_y(0)

    for d in (0,) + NEAR_FIRST:
        arrived(pf.at[pl.ds(0, 3), t], a_x.at[d])
        part = pf.at[pl.ds(rows_at(d), NX), t]
        send(part, part, 1, a_c.at[0], other_core)
    arrived(pf.at[:, 1 - t], a_c.at[0])
    outs = [pltpu.make_async_copy(pf, pf_out, loc.at[0])]
    outs[0].start()

    for c in loads[4:8]:
        c.wait()

    def partial_low(tokens, whole, cot, depth):
        reduced = jnp.dot(
            tokens[...], whole.reshape(depth, RANK), preferred_element_type=jnp.float32
        )
        high = reduced.astype(jnp.bfloat16)
        rest = (reduced - high.astype(jnp.float32)).astype(jnp.bfloat16)
        both = jnp.concatenate([high, rest], axis=0)
        return lax.dot_general(
            both, jnp.concatenate([cot, cot], axis=0),
            (((0,), (0,)), ((), ())), preferred_element_type=jnp.float32,
        )

    def put(par, lo, block):
        for zz in range(NZ):
            for xx in range(NX):
                r = (zz * NX + xx) * 8
                lb[par, xx, zz, :, lo : lo + block.shape[1]] = block[r : r + 8, :]

    low_o = partial_low(x_at, pf[:, :, 32:, :], c_o[...], DA)
    put(0, 512, low_o[:, :256])
    put(1, 0, low_o[:, 256:])
    put(0, 0, partial_low(x_in, pf[:, :, :32, :], c_q[...], D))

    chunks = (
        (2, 0, 8, 1), (3, 0, 8, NY - 1), (1, 0, 4, 1), (1, 4, 4, NY - 1), (0, 0, 4, 1), (0, 4, 4, NY - 1),
    )
    for n, (e, lo, rows, step) in enumerate(chunks):
        part = (x + e) % NX, pl.ds(lo, rows)
        cb[part] = coded(lb[(o,) + part])
        send(cb.at[part], by.at[part], 6, b_y.at[n], at_y(step))
    query_z(1)
    for d in (1, 7, 2):
        output_x(d)

    for n, (e, lo, rows, step) in enumerate(chunks):
        j = (x + e) % NX
        part = j, pl.ds(lo, rows)
        arrived(by.at[part], b_y.at[n])
        lb[(p,) + part] = lb[(p,) + part] + decoded(by[part])
        if e and lo + rows == NZ:
            cb[NX + e - 1] = coded(lb[p, j])
            send(cb.at[NX + e - 1], bx.at[e - 1], 7, b_x.at[0], at_x(e))
    query_z(2)
    for d in (6, 3, 5, 4):
        output_x(d)
    arrived(bx, b_x.at[0])
    mine = (lb[p, x] + decoded(bx[0])) + (decoded(bx[1]) + decoded(bx[2]))
    lb[o, 0] = mine
    sz[...] = coded(mine)
    for d in (4, 3, 5, 2, 6, 1, 7):
        send(sz.at[(z + d) % NZ], bz.at[d - 1], 8, b_z.at[0], at_z(d))
    query_z(3)
    arrived(bz, b_z.at[0])
    mine = lb[o, 0, z]
    for d in range(7):
        mine = mine + decoded(bz[d])
    ty[...] = mine
    send(ty, by2, 9, b_2.at[0], at_y(2))
    for d in (1, 7, 2):
        output_y(d)
    for c in loads[8:14]:
        c.wait()
    arrived(by2, b_2.at[0])

    low_sum = mine + by2[...]
    low[p] = low_sum
    _, _, normed = moment_update(low_sum, fst[p], snd[p])
    half[f, :, pl.ds(pl.multiple_of(p * HALF, 256), HALF)] = normed.astype(jnp.bfloat16)
    square = normed * normed
    total = square[:, 0:128]
    for k in range(1, 6):
        total = total + square[:, k * 128 : (k + 1) * 128]
    qz[z * 2 + t] = jnp.sum(total, axis=0, keepdims=True)

    def piece(g, n, par):
        return half.at[pl.ds(g, n), :, pl.ds(pl.multiple_of(par * HALF, 256), HALF)]

    for d in NEAR_FIRST:
        send(piece(f, 1, p), piece(f, 1, p), 11, e_z.at[d], at_z(d))
    for d in range(NZ):
        for core, dev in ((0, at_z(d)), (1, at_zt(d) if d else other_core)):
            if d or core:
                row = qz.at[z * 2 + t]
                send(row, row, 13, q_z.at[0], dev)
    send(low.at[p], low.at[p], 10, b_l.at[0], at_y(1))
    query_z(4)
    for d in (6, 3, 5, 4):
        output_y(d)
    for d in (0,) + NEAR_FIRST:
        g = ((z + NZ - d) % NZ) * NX + x
        if d:
            arrived(piece(g, 1, p), e_z.at[d])
        for e in (2, 1, 3):
            send(piece(g, 1, p), piece(g, 1, p), 11, e_x.at[d], at_x(e))
    arrived(qz.at[pl.ds(0, 2 * NZ - 1)], q_z.at[0])
    total = qz[0]
    for k in range(1, 2 * NZ):
        total = total + qz[k]
    qx[x] = total
    for e in (2, 1, 3):
        send(qx.at[x], qx.at[x], 14, q_x.at[0], at_x(e))
    for d in (0,) + NEAR_FIRST:
        row = rows_at(d)
        arrived(piece(0, 3, p), e_x.at[d])
        for side in range(2):
            two = piece(row + 2 * side, 2, p)
            send(two, two, 12, e_y.at[0], at_y(1 if side == 0 else NY - 1))
    arrived(qx.at[pl.ds(0, 3)], q_x.at[0])
    qy[p] = (qx[0] + qx[1]) + (qx[2] + qx[3])
    send(qy.at[p], qy.at[p], 15, q_y.at[0], at_y(1))
    arrived(low.at[o], b_l.at[0])
    arrived(piece(0, 32, o), e_y.at[0])
    arrived(qy.at[o], q_y.at[0])
    qt[...] = qy[0] + qy[1]
    outs += [
        pltpu.make_async_copy(half, half_out, loc.at[2]),
        pltpu.make_async_copy(low, low_out, loc.at[3]),
        pltpu.make_async_copy(qt, total_out, loc.at[4]),
    ]
    for c in outs[1:]:
        c.start()
    arrived(wg_q.at[:, o], w_y.at[0])
    arrived(wg_o.at[:, o], w_y.at[1])
    for c in outs:
        c.wait()
    for kind, ref in enumerate((
        pf.at[pl.ds(0, 31), 0], pf.at[:, 0],
        wg_q.at[pl.ds(0, 31), 0], wg_q.at[:, 0], wg_o.at[pl.ds(0, 31), 0], wg_o.at[:, 0],
        by, bx, bz, by2, low.at[0], piece(0, 31, 0), piece(0, 32, 0),
        qz.at[pl.ds(0, 2 * NZ - 1)], qx.at[pl.ds(0, 3)], qy.at[0],
    )):
        remote(ref, ref, sent.at[kind], sent.at[kind], other_core).wait_send()


def gathered(inputs, query_cot, attended, output_cot, proj_q, proj_o, w_q, w_o,
             first_q, second_q, first_o, second_o):
    f32, bf16 = jnp.float32, jnp.bfloat16
    anywhere = pl.BlockSpec(memory_space=pl.ANY)
    dma = pltpu.SemaphoreType.DMA
    shared = (
        ((32, 2, 48, RANK), bf16),
        ((32, 8, 2 * HALF), bf16),
        ((2, 8, HALF), f32),
    )
    return pl.pallas_call(
        comm_kernel,
        out_shape=tuple(jax.ShapeDtypeStruct(*s) for s in shared) + (
            jax.ShapeDtypeStruct((1, 128), f32),
            jax.ShapeDtypeStruct((32, 2, 32, 512), bf16),
            jax.ShapeDtypeStruct((32, 2, 16, 1024), bf16),
        ),
        in_specs=[anywhere] * 12,
        out_specs=(anywhere,) * 6,
        scratch_shapes=[pltpu.VMEM(*s) for s in shared] + [
            pltpu.VMEM((128, D), bf16),
            pltpu.VMEM((128, 512), bf16),
            pltpu.VMEM((128, DA), bf16),
            pltpu.VMEM((128, 1024), bf16),
            pltpu.VMEM((2, 8, HALF), f32),
            pltpu.VMEM((2, 8, HALF), f32),
            pltpu.VMEM((32, 512), f32),
            pltpu.VMEM((16, 1024), f32),
            pltpu.VMEM((32, 512), bf16),
            pltpu.VMEM((16, 1024), bf16),
            pltpu.VMEM((2, NX, NZ, 8, HALF), f32),
            pltpu.VMEM((7, NZ, 8, HALF), bf16),
            pltpu.VMEM((NX, NZ, 8, HALF), bf16),
            pltpu.VMEM((3, NZ, 8, HALF), bf16),
            pltpu.VMEM((NZ, 8, HALF), bf16),
            pltpu.VMEM((7, 8, HALF), bf16),
            pltpu.VMEM((8, HALF), f32),
            pltpu.VMEM((8, HALF), f32),
            pltpu.VMEM((2 * NZ, 1, 128), f32),
            pltpu.VMEM((NX, 1, 128), f32),
            pltpu.VMEM((2, 1, 128), f32),
            pltpu.VMEM((1, 128), f32),
            dma((14,)), dma((16,)), dma((8,)), dma((8,)), dma((1,)), dma((9,)), dma((5, 2)), dma((8,)), dma((2,)),
            dma((6,)), dma((1,)), dma((1,)), dma((1,)), dma((1,)),
            dma((8,)), dma((8,)), dma((1,)), dma((1,)), dma((1,)), dma((1,)),
        ],
        compiler_params=pltpu.CompilerParams(collective_id=0, has_side_effects=True),
    )(
        inputs, query_cot, attended, output_cot,
        proj_q.reshape(2, 32, RANK), proj_o.reshape(2, 16, RANK),
        w_q.reshape(2, 32, 512), w_o.reshape(2, 16, 1024),
        first_q, second_q, first_o, second_o,
    )


def final_kernel(
    pf, wq, wo, half, low, total, proj_q, proj_o, weight_q, weight_o,
    first_q, second_q, first_o, second_o,
    new_q, new_o, step_q, step_o, nf_q, ns_q, nf_o, ns_o, copy_q, copy_o,
):
    mean = jnp.sum(total[...], axis=1, keepdims=True) / (RANK * (DA + D))
    scale = lax.rsqrt(mean + mean_eps)

    def step(factor, lo, width):
        rows = half[:, :, lo : lo + width].reshape(RANK, width)
        return scale * jnp.dot(factor, rows, preferred_element_type=jnp.float32)

    rows_q, rows_o = copy_q.shape[0], copy_o.shape[0]
    all_q = step(pf[:, :, :32, :].reshape(rows_q, RANK), 0, 512)
    copy_q[...] = (decoded(wq[...].reshape(rows_q, 512)) - learn_rate * all_q).astype(jnp.bfloat16)
    all_o = step(pf[:, :, 32:, :].reshape(rows_o, RANK), 512, 1024)
    copy_o[...] = (decoded(wo[...].reshape(rows_o, 1024)) - learn_rate * all_o).astype(jnp.bfloat16)

    @pl.when(pl.program_id(0) == 0)
    def _():
        mine_q = step(proj_q[...], 0, 512)
        step_q[...] = mine_q
        new_q[...] = weight_q[...] - learn_rate * mine_q
        mine_o = step(proj_o[...], 512, 1024)
        step_o[...] = mine_o
        new_o[...] = weight_o[...] - learn_rate * mine_o
        nf_q[...], ns_q[...], _ = moment_update(low[0, :, :512], first_q[...], second_q[...])
        nf_o[:, :256], ns_o[:, :256], _ = moment_update(
            low[0, :, 512:], first_o[:, :256], second_o[:, :256]
        )
        nf_o[:, 256:], ns_o[:, 256:], _ = moment_update(low[1], first_o[:, 256:], second_o[:, 256:])


STEPS = 8


def finished(pf, wq, wo, half, low, total, proj_q, proj_o, weight_q, weight_o,
             first_q, second_q, first_o, second_o):
    f32, bf16 = jnp.float32, jnp.bfloat16

    def blocks(shape):
        rest = (0,) * (len(shape) - 1)
        return pl.BlockSpec((shape[0] // STEPS,) + tuple(shape[1:]), lambda i: (i,) + rest)

    def whole(shape):
        return pl.BlockSpec(tuple(shape), lambda i: (0,) * len(shape))

    small = (half, low, total, proj_q, proj_o, weight_q, weight_o, first_q, second_q, first_o, second_o)
    outs = (
        ((64, 512), f32), ((32, 1024), f32), ((64, 512), f32), ((32, 1024), f32),
        ((8, 512), f32), ((8, 512), f32), ((8, 1024), f32), ((8, 1024), f32),
        ((D, 512), bf16), ((DA, 1024), bf16),
    )
    return pl.pallas_call(
        final_kernel,
        grid=(STEPS,),
        out_shape=tuple(jax.ShapeDtypeStruct(*s) for s in outs),
        in_specs=[blocks(a.shape) for a in (pf, wq, wo)] + [whole(a.shape) for a in small],
        out_specs=tuple(whole(s) for s, _ in outs[:8]) + tuple(blocks(s) for s, _ in outs[8:]),
        cost_estimate=pl.CostEstimate(flops=2_200_000_000, bytes_accessed=12_000_000, transcendentals=0),
    )(pf, wq, wo, *small)


def local(
    inputs, query_cot, attended, output_cot, proj_query, proj_output,
    weight_query, weight_output, first_query, second_query, first_output, second_output,
):
    pf, half, low, total, wg_q, wg_o = gathered(
        inputs, query_cot, attended, output_cot, proj_query, proj_output,
        weight_query, weight_output, first_query, second_query, first_output, second_output,
    )
    return finished(
        pf, wg_q, wg_o, half, low, total, proj_query, proj_output, weight_query, weight_output,
        first_query, second_query, first_output, second_output,
    )


def solution(mesh):
    return jax.shard_map(
        local,
        mesh=mesh,
        in_specs=(
            P(("fs", "rep"), None),
            P(("fs", "rep"), "tp"),
            P(("fs", "rep"), None),
            P(("fs", "rep"), "tp"),
            P("fs", None),
            P("fs", None),
            P("fs", "tp"),
            P("fs", "tp"),
            P("fs", "tp"),
            P("fs", "tp"),
            P("fs", "tp"),
            P("fs", "tp"),
        ),
        out_specs=(
            P("fs", "tp"),
            P("fs", "tp"),
            P("fs", "tp"),
            P("fs", "tp"),
            P("fs", "tp"),
            P("fs", "tp"),
            P("fs", "tp"),
            P("fs", "tp"),
            P(None, "tp"),
            P(None, "tp"),
        ),
        check_vma=False,
    )
```

```python
import functools

import jax
import jax.numpy as jnp
from jax import lax
from jax.experimental import pallas as pl
from jax.experimental.pallas import tpu as pltpu
from jax.sharding import PartitionSpec as P

D = 2048
DA = 1024
RANK = 256
NZ, NX, NY = 8, 4, 4

beta_first = 0.9
beta_second = 0.95
adam_eps = 1e-08
mean_eps = 1e-06
learn_rate = 0.02
HALF = 768

MESH = pl.DeviceIdType.MESH
NEAR_FIRST = (1, 7, 2, 6, 3, 5, 4)


def moment_update(low_sum, first, second):
    first_new = beta_first * first + (1.0 - beta_first) * low_sum
    second_new = beta_second * second + (1.0 - beta_second) * low_sum * low_sum
    normed = first_new / (jnp.sqrt(second_new) + adam_eps)
    return (first_new, second_new, normed)


def coded(v):
    square = v * v
    fourth = jnp.maximum(square * square, 1e-36)
    return jnp.where(v < 0, -fourth, fourth).astype(jnp.bfloat16)


def decoded(c):
    c = c.astype(jnp.float32)
    root = c * lax.rsqrt(jnp.abs(c))
    return root * lax.rsqrt(jnp.abs(root))


def comm_kernel(
    inputs, query_cot, attended, output_cot, proj_q, proj_o, w_q, w_o,
    first_q, second_q, first_o, second_o,
    pf_out, half_out, low_out, total_out, wg_q, wg_o,
    pf, half, low,
    x_in, c_q, x_at, c_o, fst, snd, old_q, old_o, code_q, code_o,
    lb, cb, by, bx, sz, bz, ty, by2, qz, qx, qy, qt,
    loc, sent, a_z, a_x, a_c, w_x, w_z, w_d, w_y, b_y, b_x, b_z, b_2, b_l,
    e_z, e_x, e_y, q_z, q_x, q_y,
):
    f = lax.axis_index("fs")
    y = lax.axis_index("rep")
    t = lax.axis_index("tp")
    z = f // NX
    x = f % NX
    p = y % 2
    o = 1 - p

    def at_z(d):
        return {"fs": ((z + d) % NZ) * NX + x}

    def at_zt(d):
        return {"fs": ((z + d) % NZ) * NX + x, "tp": 1 - t}

    def at_x(e):
        return {"fs": z * NX + (x + e) % NX}

    def at_y(s):
        return {"rep": (y + s) % NY}

    other_core = {"tp": 1 - t}

    def remote(src, dst, ssem, rsem, dev):
        return pltpu.make_async_remote_copy(
            src_ref=src, dst_ref=dst, send_sem=ssem, recv_sem=rsem,
            device_id=dev, device_id_type=MESH,
        )

    def send(src, dst, kind, rsem, dev):
        remote(src, dst, sent.at[kind], rsem, dev).start()

    def arrived(dst, rsem):
        remote(dst, dst, rsem, rsem, other_core).wait_recv()

    loads = [
        pltpu.make_async_copy(proj_q.at[t], pf.at[f, t, pl.ds(0, 32)], loc.at[0]),
        pltpu.make_async_copy(proj_o.at[t], pf.at[f, t, pl.ds(32, 16)], loc.at[1]),
        pltpu.make_async_copy(w_q.at[p], old_q, loc.at[12]),
        pltpu.make_async_copy(w_o.at[p], old_o, loc.at[13]),
        pltpu.make_async_copy(inputs, x_in, loc.at[2]),
        pltpu.make_async_copy(attended, x_at, loc.at[3]),
        pltpu.make_async_copy(query_cot, c_q, loc.at[4]),
        pltpu.make_async_copy(output_cot, c_o, loc.at[5]),
        pltpu.make_async_copy(first_q, fst.at[0, :, pl.ds(0, 512)], loc.at[6]),
        pltpu.make_async_copy(first_o.at[:, pl.ds(0, 256)], fst.at[0, :, pl.ds(512, 256)], loc.at[7]),
        pltpu.make_async_copy(first_o.at[:, pl.ds(256, 768)], fst.at[1], loc.at[8]),
        pltpu.make_async_copy(second_q, snd.at[0, :, pl.ds(0, 512)], loc.at[9]),
        pltpu.make_async_copy(second_o.at[:, pl.ds(0, 256)], snd.at[0, :, pl.ds(512, 256)], loc.at[10]),
        pltpu.make_async_copy(second_o.at[:, pl.ds(256, 768)], snd.at[1], loc.at[11]),
    ]
    for c in loads:
        c.start()

    barrier = pltpu.get_barrier_semaphore()
    peers = [at_z(d) for d in range(1, NZ)] + [at_zt(d) for d in range(1, NZ)]
    peers += [at_x(e) for e in range(1, NX)]
    peers += [at_y(s) for s in range(1, NY)] + [other_core]
    for dev in peers:
        pl.semaphore_signal(barrier, inc=1, device_id=dev, device_id_type=MESH)
    for c in loads[:4]:
        c.wait()
    code_q[...] = coded(old_q[...])
    code_o[...] = coded(old_o[...])
    own_q = pltpu.make_async_copy(code_q, wg_q.at[f, p], loc.at[12])
    own_o = pltpu.make_async_copy(code_o, wg_o.at[f, p], loc.at[13])
    own_q.start()
    own_o.start()
    pl.semaphore_wait(barrier, len(peers))

    for d in NEAR_FIRST:
        send(pf.at[f, t], pf.at[f, t], 0, a_z.at[d], at_z(d))

    def factors_x(d):
        g = ((z + NZ - d) % NZ) * NX + x
        if d:
            arrived(pf.at[g, t], a_z.at[d])
        for e in (2, 1, 3):
            send(pf.at[g, t], pf.at[g, t], 0, a_x.at[d], at_x(e))

    def rows_at(d):
        return ((z + NZ - d) % NZ) * NX

    def output_x(d):
        g = rows_at(d) + x
        if d:
            arrived(wg_o.at[g, p], w_d.at[d])
        src = wg_o.at[g, p] if d else code_o
        for e in (2, 1, 3):
            send(src, wg_o.at[g, p], 4, w_x.at[1 + d], at_x(e))

    def weights_y(k, d):
        ref = (wg_q, wg_o)[k]
        for side in range(2):
            two = ref.at[pl.ds(rows_at(d) + 2 * side, 2), p]
            send(two, two, 3 + 2 * k, w_y.at[k], at_y(1 if side == 0 else NY - 1))

    def output_y(d):
        arrived(wg_o.at[pl.ds(0, 3), p], w_x.at[1 + d])
        weights_y(1, d)

    def query_z(s):
        if s == 0:
            arrived(wg_q.at[pl.ds(0, 3), p], w_x.at[0])
            part = wg_q.at[pl.ds(rows_at(0), NX), p]
            send(part, part, 2, w_z.at[1, 0], at_z(1))
            send(part, part, 2, w_z.at[1, 1], at_z(NZ - 1))
            weights_y(0, 0)
            return
        if s == NZ // 2:
            for way in range(2):
                arrived(wg_q.at[pl.ds(rows_at(s) + 2 * way, 2), p], w_z.at[s, way])
            weights_y(0, s)
            return
        for way, sign in ((0, 1), (1, -1)):
            part = wg_q.at[pl.ds(rows_at(sign * s), NX), p]
            arrived(part, w_z.at[s, way])
            if s == NZ // 2 - 1:
                part = wg_q.at[pl.ds(rows_at(sign * s) + 2 * way, 2), p]
            send(part, part, 2, w_z.at[s + 1, way], at_z(sign % NZ))
        for sign in (1, -1):
            weights_y(0, sign * s)

    for d in NEAR_FIRST:
        send(code_o, wg_o.at[f, p], 4, w_d.at[d], at_z(d))
    factors_x(0)
    for e in (2, 1, 3):
        send(code_q, wg_q.at[f, p], 2, w_x.at[0], at_x(e))
    output_x(0)
    for d in NEAR_FIRST:
        factors_x(d)

    own_q.wait()
    own_o.wait()
    query_z(0)
    output_y(0)

    for d in (0,) + NEAR_FIRST:
        arrived(pf.at[pl.ds(0, 3), t], a_x.at[d])
        part = pf.at[pl.ds(rows_at(d), NX), t]
        send(part, part, 1, a_c.at[0], other_core)
    arrived(pf.at[:, 1 - t], a_c.at[0])
    outs = [pltpu.make_async_copy(pf, pf_out, loc.at[0])]
    outs[0].start()

    for c in loads[4:8]:
        c.wait()

    def partial_low(tokens, whole, cot, depth):
        reduced = jnp.dot(
            tokens[...], whole.reshape(depth, RANK), preferred_element_type=jnp.float32
        )
        high = reduced.astype(jnp.bfloat16)
        rest = (reduced - high.astype(jnp.float32)).astype(jnp.bfloat16)
        both = jnp.concatenate([high, rest], axis=0)
        return lax.dot_general(
            both, jnp.concatenate([cot, cot], axis=0),
            (((0,), (0,)), ((), ())), preferred_element_type=jnp.float32,
        )

    def put(par, lo, block):
        for zz in range(NZ):
            for xx in range(NX):
                r = (zz * NX + xx) * 8
                lb[par, xx, zz, :, lo : lo + block.shape[1]] = block[r : r + 8, :]

    low_o = partial_low(x_at, pf[:, :, 32:, :], c_o[...], DA)
    put(0, 512, low_o[:, :256])
    put(1, 0, low_o[:, 256:])
    put(0, 0, partial_low(x_in, pf[:, :, :32, :], c_q[...], D))

    chunks = (
        (2, 0, 8, 1), (3, 0, 8, NY - 1), (1, 0, 4, 1), (1, 4, 4, NY - 1), (0, 0, 4, 1), (0, 4, 4, NY - 1),
    )
    for n, (e, lo, rows, step) in enumerate(chunks):
        part = (x + e) % NX, pl.ds(lo, rows)
        cb[part] = coded(lb[(o,) + part])
        send(cb.at[part], by.at[part], 6, b_y.at[n], at_y(step))
    query_z(1)
    for d in (1, 7, 2):
        output_x(d)

    for n, (e, lo, rows, step) in enumerate(chunks):
        j = (x + e) % NX
        part = j, pl.ds(lo, rows)
        arrived(by.at[part], b_y.at[n])
        lb[(p,) + part] = lb[(p,) + part] + decoded(by[part])
        if e and lo + rows == NZ:
            cb[NX + e - 1] = coded(lb[p, j])
            send(cb.at[NX + e - 1], bx.at[e - 1], 7, b_x.at[0], at_x(e))
    query_z(2)
    for d in (6, 3, 5, 4):
        output_x(d)
    for d in (1, 7, 2):
        output_y(d)
    arrived(bx, b_x.at[0])
    mine = (lb[p, x] + decoded(bx[0])) + (decoded(bx[1]) + decoded(bx[2]))
    lb[o, 0] = mine
    sz[...] = coded(mine)
    for d in (4, 3, 5, 2, 6, 1, 7):
        send(sz.at[(z + d) % NZ], bz.at[d - 1], 8, b_z.at[0], at_z(d))
    query_z(3)
    arrived(bz, b_z.at[0])
    mine = lb[o, 0, z]
    for d in range(7):
        mine = mine + decoded(bz[d])
    ty[...] = mine
    send(ty, by2, 9, b_2.at[0], at_y(2))
    query_z(4)
    for d in (6, 3, 5, 4):
        output_y(d)
    for c in loads[8:14]:
        c.wait()
    arrived(by2, b_2.at[0])

    low_sum = mine + by2[...]
    low[p] = low_sum
    _, _, normed = moment_update(low_sum, fst[p], snd[p])
    half[f, :, pl.ds(pl.multiple_of(p * HALF, 256), HALF)] = normed.astype(jnp.bfloat16)
    square = normed * normed
    total = square[:, 0:128]
    for k in range(1, 6):
        total = total + square[:, k * 128 : (k + 1) * 128]
    qz[z * 2 + t] = jnp.sum(total, axis=0, keepdims=True)

    def piece(g, n, par):
        return half.at[pl.ds(g, n), :, pl.ds(pl.multiple_of(par * HALF, 256), HALF)]

    for d in NEAR_FIRST:
        send(piece(f, 1, p), piece(f, 1, p), 11, e_z.at[d], at_z(d))
    for d in range(NZ):
        for core, dev in ((0, at_z(d)), (1, at_zt(d) if d else other_core)):
            if d or core:
                row = qz.at[z * 2 + t]
                send(row, row, 13, q_z.at[0], dev)
    send(low.at[p], low.at[p], 10, b_l.at[0], at_y(1))
    for d in (0,) + NEAR_FIRST:
        g = ((z + NZ - d) % NZ) * NX + x
        if d:
            arrived(piece(g, 1, p), e_z.at[d])
        for e in (2, 1, 3):
            send(piece(g, 1, p), piece(g, 1, p), 11, e_x.at[d], at_x(e))
    arrived(qz.at[pl.ds(0, 2 * NZ - 1)], q_z.at[0])
    total = qz[0]
    for k in range(1, 2 * NZ):
        total = total + qz[k]
    qx[x] = total
    for e in (2, 1, 3):
        send(qx.at[x], qx.at[x], 14, q_x.at[0], at_x(e))
    for d in (0,) + NEAR_FIRST:
        row = rows_at(d)
        arrived(piece(0, 3, p), e_x.at[d])
        for side in range(2):
            two = piece(row + 2 * side, 2, p)
            send(two, two, 12, e_y.at[0], at_y(1 if side == 0 else NY - 1))
    arrived(qx.at[pl.ds(0, 3)], q_x.at[0])
    qy[p] = (qx[0] + qx[1]) + (qx[2] + qx[3])
    send(qy.at[p], qy.at[p], 15, q_y.at[0], at_y(1))
    arrived(low.at[o], b_l.at[0])
    arrived(piece(0, 32, o), e_y.at[0])
    arrived(qy.at[o], q_y.at[0])
    qt[...] = qy[0] + qy[1]
    outs += [
        pltpu.make_async_copy(half, half_out, loc.at[2]),
        pltpu.make_async_copy(low, low_out, loc.at[3]),
        pltpu.make_async_copy(qt, total_out, loc.at[4]),
    ]
    for c in outs[1:]:
        c.start()
    arrived(wg_q.at[:, o], w_y.at[0])
    arrived(wg_o.at[:, o], w_y.at[1])
    for c in outs:
        c.wait()
    for kind, ref in enumerate((
        pf.at[pl.ds(0, 31), 0], pf.at[:, 0],
        wg_q.at[pl.ds(0, 31), 0], wg_q.at[:, 0], wg_o.at[pl.ds(0, 31), 0], wg_o.at[:, 0],
        by, bx, bz, by2, low.at[0], piece(0, 31, 0), piece(0, 32, 0),
        qz.at[pl.ds(0, 2 * NZ - 1)], qx.at[pl.ds(0, 3)], qy.at[0],
    )):
        remote(ref, ref, sent.at[kind], sent.at[kind], other_core).wait_send()


def gathered(inputs, query_cot, attended, output_cot, proj_q, proj_o, w_q, w_o,
             first_q, second_q, first_o, second_o):
    f32, bf16 = jnp.float32, jnp.bfloat16
    anywhere = pl.BlockSpec(memory_space=pl.ANY)
    dma = pltpu.SemaphoreType.DMA
    shared = (
        ((32, 2, 48, RANK), bf16),
        ((32, 8, 2 * HALF), bf16),
        ((2, 8, HALF), f32),
    )
    return pl.pallas_call(
        comm_kernel,
        out_shape=tuple(jax.ShapeDtypeStruct(*s) for s in shared) + (
            jax.ShapeDtypeStruct((1, 128), f32),
            jax.ShapeDtypeStruct((32, 2, 32, 512), bf16),
            jax.ShapeDtypeStruct((32, 2, 16, 1024), bf16),
        ),
        in_specs=[anywhere] * 12,
        out_specs=(anywhere,) * 6,
        scratch_shapes=[pltpu.VMEM(*s) for s in shared] + [
            pltpu.VMEM((128, D), bf16),
            pltpu.VMEM((128, 512), bf16),
            pltpu.VMEM((128, DA), bf16),
            pltpu.VMEM((128, 1024), bf16),
            pltpu.VMEM((2, 8, HALF), f32),
            pltpu.VMEM((2, 8, HALF), f32),
            pltpu.VMEM((32, 512), f32),
            pltpu.VMEM((16, 1024), f32),
            pltpu.VMEM((32, 512), bf16),
            pltpu.VMEM((16, 1024), bf16),
            pltpu.VMEM((2, NX, NZ, 8, HALF), f32),
            pltpu.VMEM((7, NZ, 8, HALF), bf16),
            pltpu.VMEM((NX, NZ, 8, HALF), bf16),
            pltpu.VMEM((3, NZ, 8, HALF), bf16),
            pltpu.VMEM((NZ, 8, HALF), bf16),
            pltpu.VMEM((7, 8, HALF), bf16),
            pltpu.VMEM((8, HALF), f32),
            pltpu.VMEM((8, HALF), f32),
            pltpu.VMEM((2 * NZ, 1, 128), f32),
            pltpu.VMEM((NX, 1, 128), f32),
            pltpu.VMEM((2, 1, 128), f32),
            pltpu.VMEM((1, 128), f32),
            dma((14,)), dma((16,)), dma((8,)), dma((8,)), dma((1,)), dma((9,)), dma((5, 2)), dma((8,)), dma((2,)),
            dma((6,)), dma((1,)), dma((1,)), dma((1,)), dma((1,)),
            dma((8,)), dma((8,)), dma((1,)), dma((1,)), dma((1,)), dma((1,)),
        ],
        compiler_params=pltpu.CompilerParams(collective_id=0, has_side_effects=True),
    )(
        inputs, query_cot, attended, output_cot,
        proj_q.reshape(2, 32, RANK), proj_o.reshape(2, 16, RANK),
        w_q.reshape(2, 32, 512), w_o.reshape(2, 16, 1024),
        first_q, second_q, first_o, second_o,
    )


def final_kernel(
    pf, wq, wo, half, low, total, proj_q, proj_o, weight_q, weight_o,
    first_q, second_q, first_o, second_o,
    new_q, new_o, step_q, step_o, nf_q, ns_q, nf_o, ns_o, copy_q, copy_o,
):
    mean = jnp.sum(total[...], axis=1, keepdims=True) / (RANK * (DA + D))
    scale = lax.rsqrt(mean + mean_eps)

    def step(factor, lo, width):
        rows = half[:, :, lo : lo + width].reshape(RANK, width)
        return scale * jnp.dot(factor, rows, preferred_element_type=jnp.float32)

    rows_q, rows_o = copy_q.shape[0], copy_o.shape[0]
    all_q = step(pf[:, :, :32, :].reshape(rows_q, RANK), 0, 512)
    copy_q[...] = (decoded(wq[...].reshape(rows_q, 512)) - learn_rate * all_q).astype(jnp.bfloat16)
    all_o = step(pf[:, :, 32:, :].reshape(rows_o, RANK), 512, 1024)
    copy_o[...] = (decoded(wo[...].reshape(rows_o, 1024)) - learn_rate * all_o).astype(jnp.bfloat16)

    @pl.when(pl.program_id(0) == 0)
    def _():
        mine_q = step(proj_q[...], 0, 512)
        step_q[...] = mine_q
        new_q[...] = weight_q[...] - learn_rate * mine_q
        mine_o = step(proj_o[...], 512, 1024)
        step_o[...] = mine_o
        new_o[...] = weight_o[...] - learn_rate * mine_o
        nf_q[...], ns_q[...], _ = moment_update(low[0, :, :512], first_q[...], second_q[...])
        nf_o[:, :256], ns_o[:, :256], _ = moment_update(
            low[0, :, 512:], first_o[:, :256], second_o[:, :256]
        )
        nf_o[:, 256:], ns_o[:, 256:], _ = moment_update(low[1], first_o[:, 256:], second_o[:, 256:])


STEPS = 4


def finished(pf, wq, wo, half, low, total, proj_q, proj_o, weight_q, weight_o,
             first_q, second_q, first_o, second_o):
    f32, bf16 = jnp.float32, jnp.bfloat16

    def blocks(shape):
        rest = (0,) * (len(shape) - 1)
        return pl.BlockSpec((shape[0] // STEPS,) + tuple(shape[1:]), lambda i: (i,) + rest)

    def whole(shape):
        return pl.BlockSpec(tuple(shape), lambda i: (0,) * len(shape))

    small = (half, low, total, proj_q, proj_o, weight_q, weight_o, first_q, second_q, first_o, second_o)
    outs = (
        ((64, 512), f32), ((32, 1024), f32), ((64, 512), f32), ((32, 1024), f32),
        ((8, 512), f32), ((8, 512), f32), ((8, 1024), f32), ((8, 1024), f32),
        ((D, 512), bf16), ((DA, 1024), bf16),
    )
    return pl.pallas_call(
        final_kernel,
        grid=(STEPS,),
        out_shape=tuple(jax.ShapeDtypeStruct(*s) for s in outs),
        in_specs=[blocks(a.shape) for a in (pf, wq, wo)] + [whole(a.shape) for a in small],
        out_specs=tuple(whole(s) for s, _ in outs[:8]) + tuple(blocks(s) for s, _ in outs[8:]),
        cost_estimate=pl.CostEstimate(flops=2_200_000_000, bytes_accessed=12_000_000, transcendentals=0),
    )(pf, wq, wo, *small)


def local(
    inputs, query_cot, attended, output_cot, proj_query, proj_output,
    weight_query, weight_output, first_query, second_query, first_output, second_output,
):
    pf, half, low, total, wg_q, wg_o = gathered(
        inputs, query_cot, attended, output_cot, proj_query, proj_output,
        weight_query, weight_output, first_query, second_query, first_output, second_output,
    )
    return finished(
        pf, wg_q, wg_o, half, low, total, proj_query, proj_output, weight_query, weight_output,
        first_query, second_query, first_output, second_output,
    )


def solution(mesh):
    return jax.shard_map(
        local,
        mesh=mesh,
        in_specs=(
            P(("fs", "rep"), None),
            P(("fs", "rep"), "tp"),
            P(("fs", "rep"), None),
            P(("fs", "rep"), "tp"),
            P("fs", None),
            P("fs", None),
            P("fs", "tp"),
            P("fs", "tp"),
            P("fs", "tp"),
            P("fs", "tp"),
            P("fs", "tp"),
            P("fs", "tp"),
        ),
        out_specs=(
            P("fs", "tp"),
            P("fs", "tp"),
            P("fs", "tp"),
            P("fs", "tp"),
            P("fs", "tp"),
            P("fs", "tp"),
            P("fs", "tp"),
            P("fs", "tp"),
            P(None, "tp"),
            P(None, "tp"),
        ),
        check_vma=False,
    )
```

```python
import functools

import jax
import jax.numpy as jnp
from jax import lax
from jax.experimental import pallas as pl
from jax.experimental.pallas import tpu as pltpu
from jax.sharding import PartitionSpec as P

D = 2048
DA = 1024
RANK = 256
NZ, NX, NY = 8, 4, 4

beta_first = 0.9
beta_second = 0.95
adam_eps = 1e-08
mean_eps = 1e-06
learn_rate = 0.02
HALF = 768

MESH = pl.DeviceIdType.MESH
NEAR_FIRST = (1, 7, 2, 6, 3, 5, 4)


def moment_update(low_sum, first, second):
    first_new = beta_first * first + (1.0 - beta_first) * low_sum
    second_new = beta_second * second + (1.0 - beta_second) * low_sum * low_sum
    normed = first_new / (jnp.sqrt(second_new) + adam_eps)
    return (first_new, second_new, normed)


def coded(v):
    square = v * v
    fourth = jnp.maximum(square * square, 1e-36)
    return jnp.where(v < 0, -fourth, fourth).astype(jnp.bfloat16)


def decoded(c):
    c = c.astype(jnp.float32)
    root = c * lax.rsqrt(jnp.abs(c))
    return root * lax.rsqrt(jnp.abs(root))


def comm_kernel(
    inputs, query_cot, attended, output_cot, proj_q, proj_o, w_q, w_o,
    first_q, second_q, first_o, second_o,
    pf_out, half_out, low_out, total_out, wg_q, wg_o,
    pf, half, low,
    x_in, c_q, x_at, c_o, fst, snd, old_q, old_o, code_q, code_o,
    lb_o, lb_q, cb_o, cb_q, by_o, by_q, bx_o, bx_q, sz, bz, ty, by2, qz, qx, qy, qt,
    loc, sent, a_z, a_x, a_c, w_x, w_z, w_d, w_y, b_y, b_x, b_z, b_2, b_l,
    e_z, e_x, e_y, q_z, q_x, q_y,
):
    f = lax.axis_index("fs")
    y = lax.axis_index("rep")
    t = lax.axis_index("tp")
    z = f // NX
    x = f % NX
    p = y % 2
    o = 1 - p

    def at_z(d):
        return {"fs": ((z + d) % NZ) * NX + x}

    def at_zt(d):
        return {"fs": ((z + d) % NZ) * NX + x, "tp": 1 - t}

    def at_x(e):
        return {"fs": z * NX + (x + e) % NX}

    def at_y(s):
        return {"rep": (y + s) % NY}

    other_core = {"tp": 1 - t}

    def remote(src, dst, ssem, rsem, dev):
        return pltpu.make_async_remote_copy(
            src_ref=src, dst_ref=dst, send_sem=ssem, recv_sem=rsem,
            device_id=dev, device_id_type=MESH,
        )

    def send(src, dst, kind, rsem, dev):
        remote(src, dst, sent.at[kind], rsem, dev).start()

    def arrived(dst, rsem):
        remote(dst, dst, rsem, rsem, other_core).wait_recv()

    loads = [
        pltpu.make_async_copy(proj_q.at[t], pf.at[f, t, pl.ds(0, 32)], loc.at[0]),
        pltpu.make_async_copy(proj_o.at[t], pf.at[f, t, pl.ds(32, 16)], loc.at[1]),
        pltpu.make_async_copy(w_q.at[p], old_q, loc.at[12]),
        pltpu.make_async_copy(w_o.at[p], old_o, loc.at[13]),
        pltpu.make_async_copy(inputs, x_in, loc.at[2]),
        pltpu.make_async_copy(attended, x_at, loc.at[3]),
        pltpu.make_async_copy(query_cot, c_q, loc.at[4]),
        pltpu.make_async_copy(output_cot, c_o, loc.at[5]),
        pltpu.make_async_copy(first_o.at[:, pl.ds(0, 512)], fst.at[0, :, pl.ds(0, 512)], loc.at[6]),
        pltpu.make_async_copy(first_o.at[:, pl.ds(512, 512)], fst.at[1, :, pl.ds(0, 512)], loc.at[7]),
        pltpu.make_async_copy(first_q.at[:, pl.ds(0, 256)], fst.at[0, :, pl.ds(512, 256)], loc.at[8]),
        pltpu.make_async_copy(first_q.at[:, pl.ds(256, 256)], fst.at[1, :, pl.ds(512, 256)], loc.at[9]),
        pltpu.make_async_copy(second_o.at[:, pl.ds(0, 512)], snd.at[0, :, pl.ds(0, 512)], loc.at[10]),
        pltpu.make_async_copy(second_o.at[:, pl.ds(512, 512)], snd.at[1, :, pl.ds(0, 512)], loc.at[11]),
        pltpu.make_async_copy(second_q.at[:, pl.ds(0, 256)], snd.at[0, :, pl.ds(512, 256)], loc.at[14]),
        pltpu.make_async_copy(second_q.at[:, pl.ds(256, 256)], snd.at[1, :, pl.ds(512, 256)], loc.at[15]),
    ]
    for c in loads:
        c.start()

    barrier = pltpu.get_barrier_semaphore()
    peers = [at_z(d) for d in range(1, NZ)] + [at_zt(d) for d in range(1, NZ)]
    peers += [at_x(e) for e in range(1, NX)]
    peers += [at_y(s) for s in range(1, NY)] + [other_core]
    for dev in peers:
        pl.semaphore_signal(barrier, inc=1, device_id=dev, device_id_type=MESH)
    for c in loads[:4]:
        c.wait()
    code_q[...] = coded(old_q[...])
    code_o[...] = coded(old_o[...])
    own_q = pltpu.make_async_copy(code_q, wg_q.at[f, p], loc.at[12])
    own_o = pltpu.make_async_copy(code_o, wg_o.at[f, p], loc.at[13])
    own_q.start()
    own_o.start()
    pl.semaphore_wait(barrier, len(peers))

    factor_rows = (pl.ds(32, 16), pl.ds(0, 32))
    for k, rows in enumerate(factor_rows):
        for d in NEAR_FIRST:
            own = pf.at[f, t, rows]
            send(own, own, 0, a_z.at[k, d], at_z(d))

    def factors_x(k, d):
        part = pf.at[((z + NZ - d) % NZ) * NX + x, t, factor_rows[k]]
        if d:
            arrived(part, a_z.at[k, d])
        for e in (2, 1, 3):
            send(part, part, 0, a_x.at[k, d], at_x(e))

    def rows_at(d):
        return ((z + NZ - d) % NZ) * NX

    def output_x(d):
        g = rows_at(d) + x
        if d:
            arrived(wg_o.at[g, p], w_d.at[d])
        src = wg_o.at[g, p] if d else code_o
        for e in (2, 1, 3):
            send(src, wg_o.at[g, p], 4, w_x.at[1 + d], at_x(e))

    def weights_y(k, d):
        ref = (wg_q, wg_o)[k]
        for side in range(2):
            two = ref.at[pl.ds(rows_at(d) + 2 * side, 2), p]
            send(two, two, 3 + 2 * k, w_y.at[k], at_y(1 if side == 0 else NY - 1))

    def output_y(d):
        arrived(wg_o.at[pl.ds(0, 3), p], w_x.at[1 + d])
        weights_y(1, d)

    def query_z(s):
        if s == 0:
            arrived(wg_q.at[pl.ds(0, 3), p], w_x.at[0])
            part = wg_q.at[pl.ds(rows_at(0), NX), p]
            send(part, part, 2, w_z.at[1, 0], at_z(1))
            send(part, part, 2, w_z.at[1, 1], at_z(NZ - 1))
            return
        if s == NZ // 2:
            for way in range(2):
                arrived(wg_q.at[pl.ds(rows_at(s) + 2 * way, 2), p], w_z.at[s, way])
            return
        for way, sign in ((0, 1), (1, -1)):
            part = wg_q.at[pl.ds(rows_at(sign * s), NX), p]
            arrived(part, w_z.at[s, way])
            if s == NZ // 2 - 1:
                part = wg_q.at[pl.ds(rows_at(sign * s) + 2 * way, 2), p]
            send(part, part, 2, w_z.at[s + 1, way], at_z(sign % NZ))

    def query_y(s):
        for d in ((s, NZ - s) if s % (NZ // 2) else (s,)):
            weights_y(0, d)

    for d in NEAR_FIRST:
        send(code_o, wg_o.at[f, p], 4, w_d.at[d], at_z(d))
    factors_x(0, 0)
    factors_x(1, 0)
    for e in (2, 1, 3):
        send(code_q, wg_q.at[f, p], 2, w_x.at[0], at_x(e))
    output_x(0)
    for k in range(2):
        for d in NEAR_FIRST:
            factors_x(k, d)

    own_q.wait()
    own_o.wait()
    query_z(0)
    query_y(0)
    output_y(0)

    def factors_core(k):
        rows = factor_rows[k]
        for d in (0,) + NEAR_FIRST:
            arrived(pf.at[pl.ds(0, 3), t, rows], a_x.at[k, d])
            part = pf.at[pl.ds(rows_at(d), NX), t, rows]
            send(part, part, 1, a_c.at[k], other_core)
        arrived(pf.at[:, 1 - t, rows], a_c.at[k])

    def partial_low(tokens, whole, cot, depth):
        reduced = jnp.dot(
            tokens[...], whole.reshape(depth, RANK), preferred_element_type=jnp.float32
        )
        high = reduced.astype(jnp.bfloat16)
        rest = (reduced - high.astype(jnp.float32)).astype(jnp.bfloat16)
        both = jnp.concatenate([high, rest], axis=0)
        return lax.dot_general(
            both, jnp.concatenate([cot, cot], axis=0),
            (((0,), (0,)), ((), ())), preferred_element_type=jnp.float32,
        )

    def put(lb, block):
        width = block.shape[1] // 2
        for par in range(2):
            for zz in range(NZ):
                for xx in range(NX):
                    r = (zz * NX + xx) * 8
                    lb[par, xx, zz] = block[r : r + 8, par * width : (par + 1) * width]

    chunks = (
        (2, 0, 8, 1), (3, 0, 8, NY - 1), (1, 0, 4, 1), (1, 4, 4, NY - 1), (0, 0, 4, 1), (0, 4, 4, NY - 1),
    )

    def sums_y(k, lb, cb, by):
        for n, (e, lo, rows, step) in enumerate(chunks):
            part = (x + e) % NX, pl.ds(lo, rows)
            cb[part] = coded(lb[(o,) + part])
            send(cb.at[part], by.at[part], 6 + k, b_y.at[k, n], at_y(step))

    def sums_x(k, lb, cb, by, bx):
        for n, (e, lo, rows, step) in enumerate(chunks):
            j = (x + e) % NX
            part = j, pl.ds(lo, rows)
            arrived(by.at[part], b_y.at[k, n])
            lb[(p,) + part] = lb[(p,) + part] + decoded(by[part])
            if e and lo + rows == NZ:
                cb[NX + e - 1] = coded(lb[p, j])
                send(cb.at[NX + e - 1], bx.at[e - 1], 16 + k, b_x.at[k], at_x(e))

    factors_core(0)
    loads[5].wait()
    loads[7].wait()
    put(lb_o, partial_low(x_at, pf[:, :, 32:, :], c_o[...], DA))
    sums_y(0, lb_o, cb_o, by_o)
    output_x(1)
    output_x(7)
    factors_core(1)
    query_z(1)
    outs = [pltpu.make_async_copy(pf, pf_out, loc.at[0])]
    outs[0].start()
    loads[4].wait()
    loads[6].wait()
    put(lb_q, partial_low(x_in, pf[:, :, :32, :], c_q[...], D))
    sums_y(1, lb_q, cb_q, by_q)
    query_y(1)

    sums_x(0, lb_o, cb_o, by_o, bx_o)
    sums_x(1, lb_q, cb_q, by_q, bx_q)
    for d in (2, 6, 3, 5, 4):
        output_x(d)
    output_y(1)
    output_y(7)
    query_z(2)
    query_y(2)
    for k, (lb, bx) in enumerate(((lb_o, bx_o), (lb_q, bx_q))):
        arrived(bx, b_x.at[k])
        part = (lb[p, x] + decoded(bx[0])) + (decoded(bx[1]) + decoded(bx[2]))
        lb[o, 0] = part
        sz[:, :, pl.ds(512 * k, part.shape[2])] = coded(part)
    for d in (4, 3, 5, 2, 6, 1, 7):
        send(sz.at[(z + d) % NZ], bz.at[d - 1], 8, b_z.at[0], at_z(d))
    output_y(2)
    query_z(3)
    arrived(bz, b_z.at[0])
    mine = jnp.concatenate([lb_o[o, 0, z], lb_q[o, 0, z]], axis=1)
    for d in range(7):
        mine = mine + decoded(bz[d])
    ty[...] = mine
    send(ty, by2, 9, b_2.at[0], at_y(2))
    query_y(3)
    output_y(6)
    output_y(3)
    query_z(4)
    for c in loads[8:16]:
        c.wait()
    arrived(by2, b_2.at[0])

    low_sum = mine + by2[...]
    low[p] = low_sum
    _, _, normed = moment_update(low_sum, fst[p], snd[p])
    half[p, f] = normed.astype(jnp.bfloat16)
    square = normed * normed
    total = square[:, 0:128]
    for k in range(1, 6):
        total = total + square[:, k * 128 : (k + 1) * 128]
    qz[z * 2 + t] = jnp.sum(total, axis=0, keepdims=True)

    def piece(g, n, par):
        return half.at[par, pl.ds(g, n)]

    for d in NEAR_FIRST:
        send(piece(f, 1, p), piece(f, 1, p), 11, e_z.at[d], at_z(d))
    for d in range(NZ):
        for core, dev in ((0, at_z(d)), (1, at_zt(d) if d else other_core)):
            if d or core:
                row = qz.at[z * 2 + t]
                send(row, row, 13, q_z.at[0], dev)
    send(low.at[p], low.at[p], 10, b_l.at[0], at_y(1))
    query_y(4)
    output_y(5)
    output_y(4)
    for d in (0,) + NEAR_FIRST:
        g = ((z + NZ - d) % NZ) * NX + x
        if d:
            arrived(piece(g, 1, p), e_z.at[d])
        for e in (2, 1, 3):
            send(piece(g, 1, p), piece(g, 1, p), 11, e_x.at[d], at_x(e))
    arrived(qz.at[pl.ds(0, 2 * NZ - 1)], q_z.at[0])
    total = qz[0]
    for k in range(1, 2 * NZ):
        total = total + qz[k]
    qx[x] = total
    for e in (2, 1, 3):
        send(qx.at[x], qx.at[x], 14, q_x.at[0], at_x(e))
    for d in (0,) + NEAR_FIRST:
        row = rows_at(d)
        arrived(piece(0, 3, p), e_x.at[d])
        for side in range(2):
            two = piece(row + 2 * side, 2, p)
            send(two, two, 12, e_y.at[0], at_y(1 if side == 0 else NY - 1))
    arrived(qx.at[pl.ds(0, 3)], q_x.at[0])
    qy[p] = (qx[0] + qx[1]) + (qx[2] + qx[3])
    send(qy.at[p], qy.at[p], 15, q_y.at[0], at_y(1))
    arrived(low.at[o], b_l.at[0])
    arrived(piece(0, 32, o), e_y.at[0])
    arrived(qy.at[o], q_y.at[0])
    qt[...] = qy[0] + qy[1]
    outs += [
        pltpu.make_async_copy(half, half_out, loc.at[2]),
        pltpu.make_async_copy(low, low_out, loc.at[3]),
        pltpu.make_async_copy(qt, total_out, loc.at[4]),
    ]
    for c in outs[1:]:
        c.start()
    arrived(wg_q.at[:, o], w_y.at[0])
    arrived(wg_o.at[:, o], w_y.at[1])
    for c in outs:
        c.wait()
    for kind, ref in enumerate((
        pf.at[pl.ds(0, 31), 0], pf.at[:, 0],
        wg_q.at[pl.ds(0, 31), 0], wg_q.at[:, 0], wg_o.at[pl.ds(0, 31), 0], wg_o.at[:, 0],
        by_o, by_q, bz, by2, low.at[0], piece(0, 31, 0), piece(0, 32, 0),
        qz.at[pl.ds(0, 2 * NZ - 1)], qx.at[pl.ds(0, 3)], qy.at[0],
        bx_o, bx_q,
    )):
        remote(ref, ref, sent.at[kind], sent.at[kind], other_core).wait_send()


def gathered(inputs, query_cot, attended, output_cot, proj_q, proj_o, w_q, w_o,
             first_q, second_q, first_o, second_o):
    f32, bf16 = jnp.float32, jnp.bfloat16
    anywhere = pl.BlockSpec(memory_space=pl.ANY)
    dma = pltpu.SemaphoreType.DMA
    shared = (
        ((32, 2, 48, RANK), bf16),
        ((2, 32, 8, HALF), bf16),
        ((2, 8, HALF), f32),
    )
    return pl.pallas_call(
        comm_kernel,
        out_shape=tuple(jax.ShapeDtypeStruct(*s) for s in shared) + (
            jax.ShapeDtypeStruct((1, 128), f32),
            jax.ShapeDtypeStruct((32, 2, 32, 512), bf16),
            jax.ShapeDtypeStruct((32, 2, 16, 1024), bf16),
        ),
        in_specs=[anywhere] * 12,
        out_specs=(anywhere,) * 6,
        scratch_shapes=[pltpu.VMEM(*s) for s in shared] + [
            pltpu.VMEM((128, D), bf16),
            pltpu.VMEM((128, 512), bf16),
            pltpu.VMEM((128, DA), bf16),
            pltpu.VMEM((128, 1024), bf16),
            pltpu.VMEM((2, 8, HALF), f32),
            pltpu.VMEM((2, 8, HALF), f32),
            pltpu.VMEM((32, 512), f32),
            pltpu.VMEM((16, 1024), f32),
            pltpu.VMEM((32, 512), bf16),
            pltpu.VMEM((16, 1024), bf16),
            pltpu.VMEM((2, NX, NZ, 8, 512), f32),
            pltpu.VMEM((2, NX, NZ, 8, 256), f32),
            pltpu.VMEM((7, NZ, 8, 512), bf16),
            pltpu.VMEM((7, NZ, 8, 256), bf16),
            pltpu.VMEM((NX, NZ, 8, 512), bf16),
            pltpu.VMEM((NX, NZ, 8, 256), bf16),
            pltpu.VMEM((3, NZ, 8, 512), bf16),
            pltpu.VMEM((3, NZ, 8, 256), bf16),
            pltpu.VMEM((NZ, 8, HALF), bf16),
            pltpu.VMEM((7, 8, HALF), bf16),
            pltpu.VMEM((8, HALF), f32),
            pltpu.VMEM((8, HALF), f32),
            pltpu.VMEM((2 * NZ, 1, 128), f32),
            pltpu.VMEM((NX, 1, 128), f32),
            pltpu.VMEM((2, 1, 128), f32),
            pltpu.VMEM((1, 128), f32),
            dma((16,)), dma((18,)), dma((2, 8)), dma((2, 8)), dma((2,)), dma((9,)), dma((5, 2)), dma((8,)), dma((2,)),
            dma((2, 6)), dma((2,)), dma((1,)), dma((1,)), dma((1,)),
            dma((8,)), dma((8,)), dma((1,)), dma((1,)), dma((1,)), dma((1,)),
        ],
        compiler_params=pltpu.CompilerParams(collective_id=0, has_side_effects=True),
    )(
        inputs, query_cot, attended, output_cot,
        proj_q.reshape(2, 32, RANK), proj_o.reshape(2, 16, RANK),
        w_q.reshape(2, 32, 512), w_o.reshape(2, 16, 1024),
        first_q, second_q, first_o, second_o,
    )


def final_kernel(
    pf, wq, wo, half, low, total, proj_q, proj_o, weight_q, weight_o,
    first_q, second_q, first_o, second_o,
    new_q, new_o, step_q, step_o, nf_q, ns_q, nf_o, ns_o, copy_q, copy_o,
):
    mean = jnp.sum(total[...], axis=1, keepdims=True) / (RANK * (DA + D))
    scale = lax.rsqrt(mean + mean_eps)

    def step(factor, h, lo, width):
        rows = half[h, :, :, lo : lo + width].reshape(RANK, width)
        return scale * jnp.dot(factor, rows, preferred_element_type=jnp.float32)

    rows_q, rows_o = copy_q.shape[0], copy_o.shape[0]
    own = pl.program_id(0) == 0
    for h in range(2):
        at_o, at_q = pl.ds(512 * h, 512), pl.ds(256 * h, 256)
        all_o = step(pf[:, :, 32:, :].reshape(rows_o, RANK), h, 0, 512)
        old_o = decoded(wo[:, :, :, at_o].reshape(rows_o, 512))
        copy_o[:, at_o] = (old_o - learn_rate * all_o).astype(jnp.bfloat16)
        all_q = step(pf[:, :, :32, :].reshape(rows_q, RANK), h, 512, 256)
        old_q = decoded(wq[:, :, :, at_q].reshape(rows_q, 256))
        copy_q[:, at_q] = (old_q - learn_rate * all_q).astype(jnp.bfloat16)

    @pl.when(own)
    def _():
        for h in range(2):
            at_o, at_q = pl.ds(512 * h, 512), pl.ds(256 * h, 256)
            mine_o = step(proj_o[...], h, 0, 512)
            step_o[:, at_o] = mine_o
            new_o[:, at_o] = weight_o[:, at_o] - learn_rate * mine_o
            mine_q = step(proj_q[...], h, 512, 256)
            step_q[:, at_q] = mine_q
            new_q[:, at_q] = weight_q[:, at_q] - learn_rate * mine_q
            nf_o[:, at_o], ns_o[:, at_o], _ = moment_update(
                low[h, :, :512], first_o[:, at_o], second_o[:, at_o]
            )
            nf_q[:, at_q], ns_q[:, at_q], _ = moment_update(
                low[h, :, 512:], first_q[:, at_q], second_q[:, at_q]
            )


STEPS = 4


def finished(pf, wq, wo, half, low, total, proj_q, proj_o, weight_q, weight_o,
             first_q, second_q, first_o, second_o):
    f32, bf16 = jnp.float32, jnp.bfloat16

    def blocks(shape):
        rest = (0,) * (len(shape) - 1)
        return pl.BlockSpec((shape[0] // STEPS,) + tuple(shape[1:]), lambda i: (i,) + rest)

    def whole(shape):
        return pl.BlockSpec(tuple(shape), lambda i: (0,) * len(shape))

    small = (half, low, total, proj_q, proj_o, weight_q, weight_o, first_q, second_q, first_o, second_o)
    outs = (
        ((64, 512), f32), ((32, 1024), f32), ((64, 512), f32), ((32, 1024), f32),
        ((8, 512), f32), ((8, 512), f32), ((8, 1024), f32), ((8, 1024), f32),
        ((D, 512), bf16), ((DA, 1024), bf16),
    )
    return pl.pallas_call(
        final_kernel,
        grid=(STEPS,),
        out_shape=tuple(jax.ShapeDtypeStruct(*s) for s in outs),
        in_specs=[blocks(a.shape) for a in (pf, wq, wo)] + [whole(a.shape) for a in small],
        out_specs=tuple(whole(s) for s, _ in outs[:8]) + tuple(blocks(s) for s, _ in outs[8:]),
        cost_estimate=pl.CostEstimate(flops=2_200_000_000, bytes_accessed=12_000_000, transcendentals=0),
    )(pf, wq, wo, *small)


def local(
    inputs, query_cot, attended, output_cot, proj_query, proj_output,
    weight_query, weight_output, first_query, second_query, first_output, second_output,
):
    pf, half, low, total, wg_q, wg_o = gathered(
        inputs, query_cot, attended, output_cot, proj_query, proj_output,
        weight_query, weight_output, first_query, second_query, first_output, second_output,
    )
    return finished(
        pf, wg_q, wg_o, half, low, total, proj_query, proj_output, weight_query, weight_output,
        first_query, second_query, first_output, second_output,
    )


def solution(mesh):
    return jax.shard_map(
        local,
        mesh=mesh,
        in_specs=(
            P(("fs", "rep"), None),
            P(("fs", "rep"), "tp"),
            P(("fs", "rep"), None),
            P(("fs", "rep"), "tp"),
            P("fs", None),
            P("fs", None),
            P("fs", "tp"),
            P("fs", "tp"),
            P("fs", "tp"),
            P("fs", "tp"),
            P("fs", "tp"),
            P("fs", "tp"),
        ),
        out_specs=(
            P("fs", "tp"),
            P("fs", "tp"),
            P("fs", "tp"),
            P("fs", "tp"),
            P("fs", "tp"),
            P("fs", "tp"),
            P("fs", "tp"),
            P("fs", "tp"),
            P(None, "tp"),
            P(None, "tp"),
        ),
        check_vma=False,
    )
```

```python
import functools

import jax
import jax.numpy as jnp
from jax import lax
from jax.experimental import pallas as pl
from jax.experimental.pallas import tpu as pltpu
from jax.sharding import PartitionSpec as P

D = 2048
DA = 1024
RANK = 256
NZ, NX, NY = 8, 4, 4

beta_first = 0.9
beta_second = 0.95
adam_eps = 1e-08
mean_eps = 1e-06
learn_rate = 0.02
HALF = 768

MESH = pl.DeviceIdType.MESH
NEAR_FIRST = (1, 7, 2, 6, 3, 5, 4)


def moment_update(low_sum, first, second):
    first_new = beta_first * first + (1.0 - beta_first) * low_sum
    second_new = beta_second * second + (1.0 - beta_second) * low_sum * low_sum
    normed = first_new / (jnp.sqrt(second_new) + adam_eps)
    return (first_new, second_new, normed)


def coded(v):
    square = v * v
    fourth = jnp.maximum(square * square, 1e-36)
    return jnp.where(v < 0, -fourth, fourth).astype(jnp.bfloat16)


def decoded(c):
    c = c.astype(jnp.float32)
    root = c * lax.rsqrt(jnp.abs(c))
    return root * lax.rsqrt(jnp.abs(root))


def comm_kernel(
    inputs, query_cot, attended, output_cot, proj_q, proj_o, w_q, w_o,
    first_q, second_q, first_o, second_o,
    pf_out, half_out, low_out, total_out, wg_q, wg_o,
    pf, half, low,
    x_in, c_q, x_at, c_o, fst, snd, old_q, old_o, code_q, code_o,
    lb_o, lb_q, cb_o, cb_q, by_o, by_q, bx_o, bx_q, sz, bz, ty, by2, qz, qx, qy, qt,
    loc, sent, a_z, a_x, a_c, w_x, w_z, w_d, w_y, b_y, b_x, b_z, b_2, b_l,
    e_z, e_x, e_y, q_z, q_x, q_y,
):
    f = lax.axis_index("fs")
    y = lax.axis_index("rep")
    t = lax.axis_index("tp")
    z = f // NX
    x = f % NX
    p = y % 2
    o = 1 - p

    def at_z(d):
        return {"fs": ((z + d) % NZ) * NX + x}

    def at_zt(d):
        return {"fs": ((z + d) % NZ) * NX + x, "tp": 1 - t}

    def at_x(e):
        return {"fs": z * NX + (x + e) % NX}

    def at_y(s):
        return {"rep": (y + s) % NY}

    other_core = {"tp": 1 - t}

    def remote(src, dst, ssem, rsem, dev):
        return pltpu.make_async_remote_copy(
            src_ref=src, dst_ref=dst, send_sem=ssem, recv_sem=rsem,
            device_id=dev, device_id_type=MESH,
        )

    def send(src, dst, kind, rsem, dev):
        remote(src, dst, sent.at[kind], rsem, dev).start()

    def arrived(dst, rsem):
        remote(dst, dst, rsem, rsem, other_core).wait_recv()

    loads = [
        pltpu.make_async_copy(proj_q.at[t], pf.at[f, t, pl.ds(0, 32)], loc.at[0]),
        pltpu.make_async_copy(proj_o.at[t], pf.at[f, t, pl.ds(32, 16)], loc.at[1]),
        pltpu.make_async_copy(w_q.at[p], old_q, loc.at[12]),
        pltpu.make_async_copy(w_o.at[p], old_o, loc.at[13]),
        pltpu.make_async_copy(inputs, x_in, loc.at[2]),
        pltpu.make_async_copy(attended, x_at, loc.at[3]),
        pltpu.make_async_copy(query_cot, c_q, loc.at[4]),
        pltpu.make_async_copy(output_cot, c_o, loc.at[5]),
        pltpu.make_async_copy(first_o.at[:, pl.ds(0, 512)], fst.at[0, :, pl.ds(0, 512)], loc.at[6]),
        pltpu.make_async_copy(first_o.at[:, pl.ds(512, 512)], fst.at[1, :, pl.ds(0, 512)], loc.at[7]),
        pltpu.make_async_copy(first_q.at[:, pl.ds(0, 256)], fst.at[0, :, pl.ds(512, 256)], loc.at[8]),
        pltpu.make_async_copy(first_q.at[:, pl.ds(256, 256)], fst.at[1, :, pl.ds(512, 256)], loc.at[9]),
        pltpu.make_async_copy(second_o.at[:, pl.ds(0, 512)], snd.at[0, :, pl.ds(0, 512)], loc.at[10]),
        pltpu.make_async_copy(second_o.at[:, pl.ds(512, 512)], snd.at[1, :, pl.ds(0, 512)], loc.at[11]),
        pltpu.make_async_copy(second_q.at[:, pl.ds(0, 256)], snd.at[0, :, pl.ds(512, 256)], loc.at[14]),
        pltpu.make_async_copy(second_q.at[:, pl.ds(256, 256)], snd.at[1, :, pl.ds(512, 256)], loc.at[15]),
    ]
    for c in loads:
        c.start()

    barrier = pltpu.get_barrier_semaphore()
    peers = [at_z(d) for d in range(1, NZ)] + [at_zt(d) for d in range(1, NZ)]
    peers += [at_x(e) for e in range(1, NX)]
    peers += [at_y(s) for s in range(1, NY)] + [other_core]
    for dev in peers:
        pl.semaphore_signal(barrier, inc=1, device_id=dev, device_id_type=MESH)
    for c in loads[:4]:
        c.wait()
    code_q[...] = coded(old_q[...])
    code_o[...] = coded(old_o[...])
    own_q = pltpu.make_async_copy(code_q, wg_q.at[f, p], loc.at[12])
    own_o = pltpu.make_async_copy(code_o, wg_o.at[f, p], loc.at[13])
    own_q.start()
    own_o.start()
    pl.semaphore_wait(barrier, len(peers))

    factor_rows = (pl.ds(32, 16), pl.ds(0, 32))
    for k, rows in enumerate(factor_rows):
        for d in NEAR_FIRST:
            own = pf.at[f, t, rows]
            send(own, own, 0, a_z.at[k, d], at_z(d))

    def factors_x(k, d):
        part = pf.at[((z + NZ - d) % NZ) * NX + x, t, factor_rows[k]]
        if d:
            arrived(part, a_z.at[k, d])
        for e in (2, 1, 3):
            send(part, part, 0, a_x.at[k, d], at_x(e))

    def rows_at(d):
        return ((z + NZ - d) % NZ) * NX

    def output_x(d):
        g = rows_at(d) + x
        if d:
            arrived(wg_o.at[g, p], w_d.at[d])
        src = wg_o.at[g, p] if d else code_o
        for e in (2, 1, 3):
            send(src, wg_o.at[g, p], 4, w_x.at[1 + d], at_x(e))

    def weights_y(k, d):
        ref = (wg_q, wg_o)[k]
        for side in range(2):
            two = ref.at[pl.ds(rows_at(d) + 2 * side, 2), p]
            send(two, two, 3 + 2 * k, w_y.at[k], at_y(1 if side == 0 else NY - 1))

    def output_y(d):
        arrived(wg_o.at[pl.ds(0, 3), p], w_x.at[1 + d])
        weights_y(1, d)

    def query_z(s):
        if s == 0:
            arrived(wg_q.at[pl.ds(0, 3), p], w_x.at[0])
            part = wg_q.at[pl.ds(rows_at(0), NX), p]
            send(part, part, 2, w_z.at[1, 0], at_z(1))
            send(part, part, 2, w_z.at[1, 1], at_z(NZ - 1))
            return
        if s == NZ // 2:
            for way in range(2):
                arrived(wg_q.at[pl.ds(rows_at(s) + 2 * way, 2), p], w_z.at[s, way])
            return
        for way, sign in ((0, 1), (1, -1)):
            part = wg_q.at[pl.ds(rows_at(sign * s), NX), p]
            arrived(part, w_z.at[s, way])
            if s == NZ // 2 - 1:
                part = wg_q.at[pl.ds(rows_at(sign * s) + 2 * way, 2), p]
            send(part, part, 2, w_z.at[s + 1, way], at_z(sign % NZ))

    def query_y(s):
        for d in ((s, NZ - s) if s % (NZ // 2) else (s,)):
            weights_y(0, d)

    for d in NEAR_FIRST:
        send(code_o, wg_o.at[f, p], 4, w_d.at[d], at_z(d))
    factors_x(0, 0)
    factors_x(1, 0)
    for e in (2, 1, 3):
        send(code_q, wg_q.at[f, p], 2, w_x.at[0], at_x(e))
    for k in range(2):
        for d in NEAR_FIRST:
            factors_x(k, d)

    own_q.wait()
    own_o.wait()
    query_z(0)
    query_y(0)

    def factors_core(k):
        rows = factor_rows[k]
        for d in (0,) + NEAR_FIRST:
            arrived(pf.at[pl.ds(0, 3), t, rows], a_x.at[k, d])
            part = pf.at[pl.ds(rows_at(d), NX), t, rows]
            send(part, part, 1, a_c.at[k], other_core)
        arrived(pf.at[:, 1 - t, rows], a_c.at[k])

    def partial_low(tokens, whole, cot, depth):
        reduced = jnp.dot(
            tokens[...], whole.reshape(depth, RANK), preferred_element_type=jnp.float32
        )
        high = reduced.astype(jnp.bfloat16)
        rest = (reduced - high.astype(jnp.float32)).astype(jnp.bfloat16)
        both = jnp.concatenate([high, rest], axis=0)
        return lax.dot_general(
            both, jnp.concatenate([cot, cot], axis=0),
            (((0,), (0,)), ((), ())), preferred_element_type=jnp.float32,
        )

    def put(lb, block):
        width = block.shape[1] // 2
        for par in range(2):
            for zz in range(NZ):
                for xx in range(NX):
                    r = (zz * NX + xx) * 8
                    lb[par, xx, zz] = block[r : r + 8, par * width : (par + 1) * width]

    chunks = (
        (2, 0, 8, 1), (3, 0, 8, NY - 1), (1, 0, 4, 1), (1, 4, 4, NY - 1), (0, 0, 4, 1), (0, 4, 4, NY - 1),
    )

    def sums_y(k, lb, cb, by):
        for n, (e, lo, rows, step) in enumerate(chunks):
            part = (x + e) % NX, pl.ds(lo, rows)
            cb[part] = coded(lb[(o,) + part])
            send(cb.at[part], by.at[part], 6 + k, b_y.at[k, n], at_y(step))

    def sums_x(k, lb, cb, by, bx):
        for n, (e, lo, rows, step) in enumerate(chunks):
            j = (x + e) % NX
            part = j, pl.ds(lo, rows)
            arrived(by.at[part], b_y.at[k, n])
            lb[(p,) + part] = lb[(p,) + part] + decoded(by[part])
            if e and lo + rows == NZ:
                cb[NX + e - 1] = coded(lb[p, j])
                send(cb.at[NX + e - 1], bx.at[e - 1], 16 + k, b_x.at[k], at_x(e))

    factors_core(0)
    loads[5].wait()
    loads[7].wait()
    put(lb_o, partial_low(x_at, pf[:, :, 32:, :], c_o[...], DA))
    sums_y(0, lb_o, cb_o, by_o)
    output_x(0)
    output_x(1)
    output_x(7)
    factors_core(1)
    outs = [pltpu.make_async_copy(pf, pf_out, loc.at[0])]
    outs[0].start()
    loads[4].wait()
    loads[6].wait()
    put(lb_q, partial_low(x_in, pf[:, :, :32, :], c_q[...], D))
    sums_y(1, lb_q, cb_q, by_q)
    query_z(1)
    query_y(1)
    output_y(0)

    sums_x(0, lb_o, cb_o, by_o, bx_o)
    sums_x(1, lb_q, cb_q, by_q, bx_q)
    for d in (2, 6, 3, 5, 4):
        output_x(d)
    output_y(1)
    output_y(7)
    query_z(2)
    query_y(2)
    for k, (lb, bx) in enumerate(((lb_o, bx_o), (lb_q, bx_q))):
        arrived(bx, b_x.at[k])
        part = (lb[p, x] + decoded(bx[0])) + (decoded(bx[1]) + decoded(bx[2]))
        lb[o, 0] = part
        sz[:, :, pl.ds(512 * k, part.shape[2])] = coded(part)
    for d in (4, 3, 5, 2, 6, 1, 7):
        send(sz.at[(z + d) % NZ], bz.at[d - 1], 8, b_z.at[0], at_z(d))
    output_y(2)
    query_z(3)
    arrived(bz, b_z.at[0])
    mine = jnp.concatenate([lb_o[o, 0, z], lb_q[o, 0, z]], axis=1)
    for d in range(7):
        mine = mine + decoded(bz[d])
    ty[...] = mine
    send(ty, by2, 9, b_2.at[0], at_y(2))
    query_y(3)
    output_y(6)
    output_y(3)
    query_z(4)
    for c in loads[8:16]:
        c.wait()
    arrived(by2, b_2.at[0])

    low_sum = mine + by2[...]
    low[p] = low_sum
    _, _, normed = moment_update(low_sum, fst[p], snd[p])
    half[p, f] = normed.astype(jnp.bfloat16)
    square = normed * normed
    total = square[:, 0:128]
    for k in range(1, 6):
        total = total + square[:, k * 128 : (k + 1) * 128]
    qz[z * 2 + t] = jnp.sum(total, axis=0, keepdims=True)

    def piece(g, n, par):
        return half.at[par, pl.ds(g, n)]

    for d in NEAR_FIRST:
        send(piece(f, 1, p), piece(f, 1, p), 11, e_z.at[d], at_z(d))
    for d in range(NZ):
        for core, dev in ((0, at_z(d)), (1, at_zt(d) if d else other_core)):
            if d or core:
                row = qz.at[z * 2 + t]
                send(row, row, 13, q_z.at[0], dev)
    send(low.at[p], low.at[p], 10, b_l.at[0], at_y(1))
    query_y(4)
    output_y(5)
    output_y(4)
    for d in (0,) + NEAR_FIRST:
        g = ((z + NZ - d) % NZ) * NX + x
        if d:
            arrived(piece(g, 1, p), e_z.at[d])
        for e in (2, 1, 3):
            send(piece(g, 1, p), piece(g, 1, p), 11, e_x.at[d], at_x(e))
    arrived(qz.at[pl.ds(0, 2 * NZ - 1)], q_z.at[0])
    total = qz[0]
    for k in range(1, 2 * NZ):
        total = total + qz[k]
    qx[x] = total
    for e in (2, 1, 3):
        send(qx.at[x], qx.at[x], 14, q_x.at[0], at_x(e))
    for d in (0,) + NEAR_FIRST:
        row = rows_at(d)
        arrived(piece(0, 3, p), e_x.at[d])
        for side in range(2):
            two = piece(row + 2 * side, 2, p)
            send(two, two, 12, e_y.at[0], at_y(1 if side == 0 else NY - 1))
    arrived(qx.at[pl.ds(0, 3)], q_x.at[0])
    qy[p] = (qx[0] + qx[1]) + (qx[2] + qx[3])
    send(qy.at[p], qy.at[p], 15, q_y.at[0], at_y(1))
    arrived(low.at[o], b_l.at[0])
    arrived(piece(0, 32, o), e_y.at[0])
    arrived(qy.at[o], q_y.at[0])
    qt[...] = qy[0] + qy[1]
    outs += [
        pltpu.make_async_copy(half, half_out, loc.at[2]),
        pltpu.make_async_copy(low, low_out, loc.at[3]),
        pltpu.make_async_copy(qt, total_out, loc.at[4]),
    ]
    for c in outs[1:]:
        c.start()
    arrived(wg_q.at[:, o], w_y.at[0])
    arrived(wg_o.at[:, o], w_y.at[1])
    for c in outs:
        c.wait()
    for kind, ref in enumerate((
        pf.at[pl.ds(0, 31), 0], pf.at[:, 0],
        wg_q.at[pl.ds(0, 31), 0], wg_q.at[:, 0], wg_o.at[pl.ds(0, 31), 0], wg_o.at[:, 0],
        by_o, by_q, bz, by2, low.at[0], piece(0, 31, 0), piece(0, 32, 0),
        qz.at[pl.ds(0, 2 * NZ - 1)], qx.at[pl.ds(0, 3)], qy.at[0],
        bx_o, bx_q,
    )):
        remote(ref, ref, sent.at[kind], sent.at[kind], other_core).wait_send()


def gathered(inputs, query_cot, attended, output_cot, proj_q, proj_o, w_q, w_o,
             first_q, second_q, first_o, second_o):
    f32, bf16 = jnp.float32, jnp.bfloat16
    anywhere = pl.BlockSpec(memory_space=pl.ANY)
    dma = pltpu.SemaphoreType.DMA
    shared = (
        ((32, 2, 48, RANK), bf16),
        ((2, 32, 8, HALF), bf16),
        ((2, 8, HALF), f32),
    )
    return pl.pallas_call(
        comm_kernel,
        out_shape=tuple(jax.ShapeDtypeStruct(*s) for s in shared) + (
            jax.ShapeDtypeStruct((1, 128), f32),
            jax.ShapeDtypeStruct((32, 2, 32, 512), bf16),
            jax.ShapeDtypeStruct((32, 2, 16, 1024), bf16),
        ),
        in_specs=[anywhere] * 12,
        out_specs=(anywhere,) * 6,
        scratch_shapes=[pltpu.VMEM(*s) for s in shared] + [
            pltpu.VMEM((128, D), bf16),
            pltpu.VMEM((128, 512), bf16),
            pltpu.VMEM((128, DA), bf16),
            pltpu.VMEM((128, 1024), bf16),
            pltpu.VMEM((2, 8, HALF), f32),
            pltpu.VMEM((2, 8, HALF), f32),
            pltpu.VMEM((32, 512), f32),
            pltpu.VMEM((16, 1024), f32),
            pltpu.VMEM((32, 512), bf16),
            pltpu.VMEM((16, 1024), bf16),
            pltpu.VMEM((2, NX, NZ, 8, 512), f32),
            pltpu.VMEM((2, NX, NZ, 8, 256), f32),
            pltpu.VMEM((7, NZ, 8, 512), bf16),
            pltpu.VMEM((7, NZ, 8, 256), bf16),
            pltpu.VMEM((NX, NZ, 8, 512), bf16),
            pltpu.VMEM((NX, NZ, 8, 256), bf16),
            pltpu.VMEM((3, NZ, 8, 512), bf16),
            pltpu.VMEM((3, NZ, 8, 256), bf16),
            pltpu.VMEM((NZ, 8, HALF), bf16),
            pltpu.VMEM((7, 8, HALF), bf16),
            pltpu.VMEM((8, HALF), f32),
            pltpu.VMEM((8, HALF), f32),
            pltpu.VMEM((2 * NZ, 1, 128), f32),
            pltpu.VMEM((NX, 1, 128), f32),
            pltpu.VMEM((2, 1, 128), f32),
            pltpu.VMEM((1, 128), f32),
            dma((16,)), dma((18,)), dma((2, 8)), dma((2, 8)), dma((2,)), dma((9,)), dma((5, 2)), dma((8,)), dma((2,)),
            dma((2, 6)), dma((2,)), dma((1,)), dma((1,)), dma((1,)),
            dma((8,)), dma((8,)), dma((1,)), dma((1,)), dma((1,)), dma((1,)),
        ],
        compiler_params=pltpu.CompilerParams(collective_id=0, has_side_effects=True),
    )(
        inputs, query_cot, attended, output_cot,
        proj_q.reshape(2, 32, RANK), proj_o.reshape(2, 16, RANK),
        w_q.reshape(2, 32, 512), w_o.reshape(2, 16, 1024),
        first_q, second_q, first_o, second_o,
    )


CHUNKS = 4


def final_kernel(
    pf_in, wq_in, wo_in, half_in, low_in, total_in, proj_q_in, proj_o_in, weight_q_in, weight_o_in,
    first_q_in, second_q_in, first_o_in, second_o_in,
    new_q_out, new_o_out, step_q_out, step_o_out, nf_q_out, ns_q_out, nf_o_out, ns_o_out,
    copy_q_out, copy_o_out,
    pf, wq, wo, half, rows, small, new, copy_q, copy_o, chunk_sems, small_sems, new_sems, out_sems,
):
    low, total, proj_q, proj_o, weight_q, weight_o, first_q, second_q, first_o, second_o = small
    new_q, new_o, step_q, step_o, nf_q, ns_q, nf_o, ns_o = new
    shards = NZ * NX // CHUNKS

    def chunk_loads(i):
        part = pl.ds(i * shards, shards)
        return [
            pltpu.make_async_copy(src.at[part], dst.at[part], chunk_sems.at[k, i])
            for k, (src, dst) in enumerate(((pf_in, pf), (wq_in, wq), (wo_in, wo)))
        ]

    small_loads = [
        pltpu.make_async_copy(src, dst, small_sems.at[k])
        for k, (src, dst) in enumerate(zip(
            (low_in, total_in, proj_q_in, proj_o_in, weight_q_in, weight_o_in,
             first_q_in, second_q_in, first_o_in, second_o_in), small
        ))
    ]
    half_load = pltpu.make_async_copy(half_in, half, small_sems.at[len(small)])
    half_load.start()
    small_loads[1].start()
    for i in range(CHUNKS):
        for c in chunk_loads(i):
            c.start()
    for k, c in enumerate(small_loads):
        if k != 1:
            c.start()

    half_load.wait()
    small_loads[1].wait()
    mean = jnp.sum(total[...], axis=1, keepdims=True) / (RANK * (DA + D))
    scale = lax.rsqrt(mean + mean_eps)
    rate = learn_rate * scale
    for h in range(2):
        rows[:, HALF * h : HALF * (h + 1)] = half[h].reshape(RANK, HALF)

    def product(factor, h, lo, width):
        start = HALF * h + lo
        return jnp.dot(factor, rows[:, start : start + width], preferred_element_type=jnp.float32)

    rows_q, rows_o = 64 * shards, 32 * shards

    def out_copies(i):
        part_q, part_o = pl.ds(i * rows_q, rows_q), pl.ds(i * rows_o, rows_o)
        return (
            pltpu.make_async_copy(copy_q.at[part_q], copy_q_out.at[part_q], out_sems.at[0, i]),
            pltpu.make_async_copy(copy_o.at[part_o], copy_o_out.at[part_o], out_sems.at[1, i]),
        )

    @pl.loop(0, CHUNKS)
    def _(i):
        for c in chunk_loads(i):
            c.wait()
        part = pl.ds(i * shards, shards)
        part_q, part_o = pl.ds(i * rows_q, rows_q), pl.ds(i * rows_o, rows_o)
        factor_o = pf[part, :, 32:, :].reshape(rows_o, RANK)
        factor_q = pf[part, :, :32, :].reshape(rows_q, RANK)
        for h in range(2):
            at_o, at_q = pl.ds(512 * h, 512), pl.ds(256 * h, 256)
            old_o = decoded(wo[part, :, :, at_o].reshape(rows_o, 512))
            copy_o[part_o, at_o] = (old_o - rate * product(factor_o, h, 0, 512)).astype(jnp.bfloat16)
            old_q = decoded(wq[part, :, :, at_q].reshape(rows_q, 256))
            copy_q[part_q, at_q] = (old_q - rate * product(factor_q, h, 512, 256)).astype(jnp.bfloat16)
        for c in out_copies(i):
            c.start()

    for k, c in enumerate(small_loads):
        if k != 1:
            c.wait()
    for h in range(2):
        at_o, at_q = pl.ds(512 * h, 512), pl.ds(256 * h, 256)
        mine_o = scale * product(proj_o[...], h, 0, 512)
        step_o[:, at_o] = mine_o
        new_o[:, at_o] = weight_o[:, at_o] - learn_rate * mine_o
        mine_q = scale * product(proj_q[...], h, 512, 256)
        step_q[:, at_q] = mine_q
        new_q[:, at_q] = weight_q[:, at_q] - learn_rate * mine_q
        nf_o[:, at_o], ns_o[:, at_o], _ = moment_update(
            low[h, :, :512], first_o[:, at_o], second_o[:, at_o]
        )
        nf_q[:, at_q], ns_q[:, at_q], _ = moment_update(
            low[h, :, 512:], first_q[:, at_q], second_q[:, at_q]
        )
    new_copies = [
        pltpu.make_async_copy(src, dst, new_sems.at[k])
        for k, (src, dst) in enumerate(zip(new, (
            new_q_out, new_o_out, step_q_out, step_o_out, nf_q_out, ns_q_out, nf_o_out, ns_o_out
        )))
    ]
    for c in new_copies:
        c.start()
    for i in range(CHUNKS):
        for c in out_copies(i):
            c.wait()
    for c in new_copies:
        c.wait()


def finished(pf, wq, wo, half, low, total, proj_q, proj_o, weight_q, weight_o,
             first_q, second_q, first_o, second_o):
    f32, bf16 = jnp.float32, jnp.bfloat16
    anywhere = pl.BlockSpec(memory_space=pl.ANY)
    dma = pltpu.SemaphoreType.DMA
    small = (low, total, proj_q, proj_o, weight_q, weight_o, first_q, second_q, first_o, second_o)
    outs = (
        ((64, 512), f32), ((32, 1024), f32), ((64, 512), f32), ((32, 1024), f32),
        ((8, 512), f32), ((8, 512), f32), ((8, 1024), f32), ((8, 1024), f32),
        ((D, 512), bf16), ((DA, 1024), bf16),
    )
    return pl.pallas_call(
        final_kernel,
        out_shape=tuple(jax.ShapeDtypeStruct(*s) for s in outs),
        in_specs=[anywhere] * 14,
        out_specs=(anywhere,) * 10,
        scratch_shapes=[
            *(pltpu.VMEM(a.shape, a.dtype) for a in (pf, wq, wo, half)),
            pltpu.VMEM((RANK, 2 * HALF), bf16),
            tuple(pltpu.VMEM(a.shape, a.dtype) for a in small),
            tuple(pltpu.VMEM(*s) for s in outs[:8]),
            *(pltpu.VMEM(*s) for s in outs[8:]),
            dma((3, CHUNKS)), dma((len(small) + 1,)), dma((8,)), dma((2, CHUNKS)),
        ],
        cost_estimate=pl.CostEstimate(flops=2_200_000_000, bytes_accessed=12_000_000, transcendentals=0),
    )(pf, wq, wo, half, *small)


def local(
    inputs, query_cot, attended, output_cot, proj_query, proj_output,
    weight_query, weight_output, first_query, second_query, first_output, second_output,
):
    pf, half, low, total, wg_q, wg_o = gathered(
        inputs, query_cot, attended, output_cot, proj_query, proj_output,
        weight_query, weight_output, first_query, second_query, first_output, second_output,
    )
    return finished(
        pf, wg_q, wg_o, half, low, total, proj_query, proj_output, weight_query, weight_output,
        first_query, second_query, first_output, second_output,
    )


def solution(mesh):
    return jax.shard_map(
        local,
        mesh=mesh,
        in_specs=(
            P(("fs", "rep"), None),
            P(("fs", "rep"), "tp"),
            P(("fs", "rep"), None),
            P(("fs", "rep"), "tp"),
            P("fs", None),
            P("fs", None),
            P("fs", "tp"),
            P("fs", "tp"),
            P("fs", "tp"),
            P("fs", "tp"),
            P("fs", "tp"),
            P("fs", "tp"),
        ),
        out_specs=(
            P("fs", "tp"),
            P("fs", "tp"),
            P("fs", "tp"),
            P("fs", "tp"),
            P("fs", "tp"),
            P("fs", "tp"),
            P("fs", "tp"),
            P("fs", "tp"),
            P(None, "tp"),
            P(None, "tp"),
        ),
        check_vma=False,
    )
```

```python
import functools

import jax
import jax.numpy as jnp
from jax import lax
from jax.experimental import pallas as pl
from jax.experimental.pallas import tpu as pltpu
from jax.sharding import PartitionSpec as P

D = 2048
DA = 1024
RANK = 256
NZ, NX, NY = 8, 4, 4

beta_first = 0.9
beta_second = 0.95
adam_eps = 1e-08
mean_eps = 1e-06
learn_rate = 0.02
HALF = 768

MESH = pl.DeviceIdType.MESH
NEAR_FIRST = (1, 7, 2, 6, 3, 5, 4)


def moment_update(low_sum, first, second):
    first_new = beta_first * first + (1.0 - beta_first) * low_sum
    second_new = beta_second * second + (1.0 - beta_second) * low_sum * low_sum
    normed = first_new / (jnp.sqrt(second_new) + adam_eps)
    return (first_new, second_new, normed)


def coded(v):
    square = v * v
    fourth = jnp.maximum(square * square, 1e-36)
    return jnp.where(v < 0, -fourth, fourth).astype(jnp.bfloat16)


def decoded(c):
    c = c.astype(jnp.float32)
    root = c * lax.rsqrt(jnp.abs(c))
    return root * lax.rsqrt(jnp.abs(root))


def comm_kernel(
    inputs, query_cot, attended, output_cot, proj_q, proj_o, w_q, w_o,
    first_q, second_q, first_o, second_o,
    pf_out, half_out, low_out, total_out, wg_q, wg_o,
    pf, half, low,
    x_in, c_q, x_at, c_o, fst, snd, old_q, old_o, code_q, code_o,
    lb_o, lb_q, cb_o, cb_q, by_o, by_q, bx_o, bx_q, sz, bz, ty, by2, qz, qx, qy,
    loc, sent, a_z, a_x, a_c, w_x, w_z, w_d, w_y, b_y, b_x, b_z, b_2, b_l,
    e_z, e_x, e_y, q_z, q_x, q_y,
):
    f = lax.axis_index("fs")
    y = lax.axis_index("rep")
    t = lax.axis_index("tp")
    z = f // NX
    x = f % NX
    p = y % 2
    o = 1 - p

    def at_z(d):
        return {"fs": ((z + d) % NZ) * NX + x}

    def at_zt(d):
        return {"fs": ((z + d) % NZ) * NX + x, "tp": 1 - t}

    def at_x(e):
        return {"fs": z * NX + (x + e) % NX}

    def at_y(s):
        return {"rep": (y + s) % NY}

    other_core = {"tp": 1 - t}

    def remote(src, dst, ssem, rsem, dev):
        return pltpu.make_async_remote_copy(
            src_ref=src, dst_ref=dst, send_sem=ssem, recv_sem=rsem,
            device_id=dev, device_id_type=MESH,
        )

    def send(src, dst, kind, rsem, dev):
        remote(src, dst, sent.at[kind], rsem, dev).start()

    def arrived(dst, rsem):
        remote(dst, dst, rsem, rsem, other_core).wait_recv()

    loads = [
        pltpu.make_async_copy(proj_q.at[t], pf.at[f, t, pl.ds(0, 32)], loc.at[0]),
        pltpu.make_async_copy(proj_o.at[t], pf.at[f, t, pl.ds(32, 16)], loc.at[1]),
        pltpu.make_async_copy(w_q.at[p], old_q, loc.at[12]),
        pltpu.make_async_copy(w_o.at[p], old_o, loc.at[13]),
        pltpu.make_async_copy(inputs, x_in, loc.at[2]),
        pltpu.make_async_copy(attended, x_at, loc.at[3]),
        pltpu.make_async_copy(query_cot, c_q, loc.at[4]),
        pltpu.make_async_copy(output_cot, c_o, loc.at[5]),
        pltpu.make_async_copy(first_o.at[:, pl.ds(0, 512)], fst.at[0, :, pl.ds(0, 512)], loc.at[6]),
        pltpu.make_async_copy(first_o.at[:, pl.ds(512, 512)], fst.at[1, :, pl.ds(0, 512)], loc.at[7]),
        pltpu.make_async_copy(first_q.at[:, pl.ds(0, 256)], fst.at[0, :, pl.ds(512, 256)], loc.at[8]),
        pltpu.make_async_copy(first_q.at[:, pl.ds(256, 256)], fst.at[1, :, pl.ds(512, 256)], loc.at[9]),
        pltpu.make_async_copy(second_o.at[:, pl.ds(0, 512)], snd.at[0, :, pl.ds(0, 512)], loc.at[10]),
        pltpu.make_async_copy(second_o.at[:, pl.ds(512, 512)], snd.at[1, :, pl.ds(0, 512)], loc.at[11]),
        pltpu.make_async_copy(second_q.at[:, pl.ds(0, 256)], snd.at[0, :, pl.ds(512, 256)], loc.at[14]),
        pltpu.make_async_copy(second_q.at[:, pl.ds(256, 256)], snd.at[1, :, pl.ds(512, 256)], loc.at[15]),
    ]
    for c in loads:
        c.start()

    barrier = pltpu.get_barrier_semaphore()
    peers = [at_z(d) for d in range(1, NZ)] + [at_zt(d) for d in range(1, NZ)]
    peers += [at_x(e) for e in range(1, NX)]
    peers += [at_y(s) for s in range(1, NY)] + [other_core]
    for dev in peers:
        pl.semaphore_signal(barrier, inc=1, device_id=dev, device_id_type=MESH)
    for c in loads[:4]:
        c.wait()
    code_q[...] = coded(old_q[...])
    code_o[...] = coded(old_o[...])
    own_q = pltpu.make_async_copy(code_q, wg_q.at[f, p], loc.at[12])
    own_o = pltpu.make_async_copy(code_o, wg_o.at[f, p], loc.at[13])
    own_q.start()
    own_o.start()
    pl.semaphore_wait(barrier, len(peers))

    factor_rows = (pl.ds(32, 16), pl.ds(0, 32))
    for k, rows in enumerate(factor_rows):
        for d in NEAR_FIRST:
            own = pf.at[f, t, rows]
            send(own, own, 0, a_z.at[k, d], at_z(d))

    def factors_x(k, d):
        part = pf.at[((z + NZ - d) % NZ) * NX + x, t, factor_rows[k]]
        if d:
            arrived(part, a_z.at[k, d])
        for e in (2, 1, 3):
            send(part, part, 0, a_x.at[k, d], at_x(e))

    def rows_at(d):
        return ((z + NZ - d) % NZ) * NX

    def output_x(d):
        g = rows_at(d) + x
        if d:
            arrived(wg_o.at[g, p], w_d.at[d])
        src = wg_o.at[g, p] if d else code_o
        for e in (2, 1, 3):
            send(src, wg_o.at[g, p], 4, w_x.at[1 + d], at_x(e))

    def weights_y(k, d):
        ref = (wg_q, wg_o)[k]
        for side in range(2):
            two = ref.at[pl.ds(rows_at(d) + 2 * side, 2), p]
            send(two, two, 3 + 2 * k, w_y.at[k], at_y(1 if side == 0 else NY - 1))

    def output_y(d):
        arrived(wg_o.at[pl.ds(0, 3), p], w_x.at[1 + d])
        weights_y(1, d)

    def query_z(s):
        if s == 0:
            arrived(wg_q.at[pl.ds(0, 3), p], w_x.at[0])
            part = wg_q.at[pl.ds(rows_at(0), NX), p]
            send(part, part, 2, w_z.at[1, 0], at_z(1))
            send(part, part, 2, w_z.at[1, 1], at_z(NZ - 1))
            return
        if s == NZ // 2:
            for way in range(2):
                arrived(wg_q.at[pl.ds(rows_at(s) + 2 * way, 2), p], w_z.at[s, way])
            return
        for way, sign in ((0, 1), (1, -1)):
            part = wg_q.at[pl.ds(rows_at(sign * s), NX), p]
            arrived(part, w_z.at[s, way])
            if s == NZ // 2 - 1:
                part = wg_q.at[pl.ds(rows_at(sign * s) + 2 * way, 2), p]
            send(part, part, 2, w_z.at[s + 1, way], at_z(sign % NZ))

    def query_y(s):
        for d in ((s, NZ - s) if s % (NZ // 2) else (s,)):
            weights_y(0, d)

    for d in NEAR_FIRST:
        send(code_o, wg_o.at[f, p], 4, w_d.at[d], at_z(d))
    factors_x(0, 0)
    factors_x(1, 0)
    for e in (2, 1, 3):
        send(code_q, wg_q.at[f, p], 2, w_x.at[0], at_x(e))
    for k in range(2):
        for d in NEAR_FIRST:
            factors_x(k, d)

    own_q.wait()
    own_o.wait()
    query_z(0)
    query_y(0)

    def factors_core(k):
        rows = factor_rows[k]
        for d in (0,) + NEAR_FIRST:
            arrived(pf.at[pl.ds(0, 3), t, rows], a_x.at[k, d])
            part = pf.at[pl.ds(rows_at(d), NX), t, rows]
            send(part, part, 1, a_c.at[k], other_core)
        arrived(pf.at[:, 1 - t, rows], a_c.at[k])

    def partial_low(tokens, whole, cot, depth):
        reduced = jnp.dot(
            tokens[...], whole.reshape(depth, RANK), preferred_element_type=jnp.float32
        )
        high = reduced.astype(jnp.bfloat16)
        rest = (reduced - high.astype(jnp.float32)).astype(jnp.bfloat16)
        both = jnp.concatenate([high, rest], axis=0)
        return lax.dot_general(
            both, jnp.concatenate([cot, cot], axis=0),
            (((0,), (0,)), ((), ())), preferred_element_type=jnp.float32,
        )

    def put(lb, block):
        width = block.shape[1] // 2
        for par in range(2):
            for zz in range(NZ):
                for xx in range(NX):
                    r = (zz * NX + xx) * 8
                    lb[par, xx, zz] = block[r : r + 8, par * width : (par + 1) * width]

    chunks = (
        (2, 0, 8, 1), (3, 0, 8, NY - 1), (1, 0, 4, 1), (1, 4, 4, NY - 1), (0, 0, 4, 1), (0, 4, 4, NY - 1),
    )

    def sums_y(k, lb, cb, by):
        for n, (e, lo, rows, step) in enumerate(chunks):
            part = (x + e) % NX, pl.ds(lo, rows)
            cb[part] = coded(lb[(o,) + part])
            send(cb.at[part], by.at[part], 6 + k, b_y.at[k, n], at_y(step))

    def sums_x(k, lb, cb, by, bx):
        for n, (e, lo, rows, step) in enumerate(chunks):
            j = (x + e) % NX
            part = j, pl.ds(lo, rows)
            arrived(by.at[part], b_y.at[k, n])
            lb[(p,) + part] = lb[(p,) + part] + decoded(by[part])
            if e and lo + rows == NZ:
                cb[NX + e - 1] = coded(lb[p, j])
                send(cb.at[NX + e - 1], bx.at[e - 1], 16 + k, b_x.at[k], at_x(e))

    factors_core(0)
    loads[5].wait()
    loads[7].wait()
    put(lb_o, partial_low(x_at, pf[:, :, 32:, :], c_o[...], DA))
    sums_y(0, lb_o, cb_o, by_o)
    output_x(0)
    output_x(1)
    output_x(7)
    factors_core(1)
    outs = [pltpu.make_async_copy(pf, pf_out, loc.at[0])]
    outs[0].start()
    loads[4].wait()
    loads[6].wait()
    put(lb_q, partial_low(x_in, pf[:, :, :32, :], c_q[...], D))
    sums_y(1, lb_q, cb_q, by_q)
    query_z(1)
    query_y(1)
    output_y(0)

    sums_x(0, lb_o, cb_o, by_o, bx_o)
    sums_x(1, lb_q, cb_q, by_q, bx_q)
    for d in (2, 6, 3, 5, 4):
        output_x(d)
    output_y(1)
    output_y(7)
    query_z(2)
    query_y(2)
    for k, (lb, bx) in enumerate(((lb_o, bx_o), (lb_q, bx_q))):
        arrived(bx, b_x.at[k])
        part = (lb[p, x] + decoded(bx[0])) + (decoded(bx[1]) + decoded(bx[2]))
        lb[o, 0] = part
        sz[:, :, pl.ds(512 * k, part.shape[2])] = coded(part)
    for d in (4, 3, 5, 2, 6, 1, 7):
        send(sz.at[(z + d) % NZ], bz.at[d - 1], 8, b_z.at[0], at_z(d))
    output_y(2)
    query_z(3)
    arrived(bz, b_z.at[0])
    mine = jnp.concatenate([lb_o[o, 0, z], lb_q[o, 0, z]], axis=1)
    for d in range(7):
        mine = mine + decoded(bz[d])
    ty[...] = mine
    send(ty, by2, 9, b_2.at[0], at_y(2))
    query_y(3)
    output_y(6)
    output_y(3)
    query_z(4)
    for c in loads[8:16]:
        c.wait()
    arrived(by2, b_2.at[0])

    low_sum = mine + by2[...]
    low[...] = low_sum
    _, _, normed = moment_update(low_sum, fst[p], snd[p])
    half[f] = normed.astype(jnp.bfloat16)
    square = normed * normed
    total = square[:, 0:128]
    for k in range(1, 6):
        total = total + square[:, k * 128 : (k + 1) * 128]
    qz[z * 2 + t] = jnp.sum(total, axis=0, keepdims=True)

    def piece(g, n):
        return half.at[pl.ds(g, n)]

    def half_piece(g):
        return half_out.at[p, pl.ds(g, 2)]

    for d in NEAR_FIRST:
        send(piece(f, 1), piece(f, 1), 11, e_z.at[d], at_z(d))
    for d in range(NZ):
        for core, dev in ((0, at_z(d)), (1, at_zt(d) if d else other_core)):
            if d or core:
                row = qz.at[z * 2 + t]
                send(row, row, 13, q_z.at[0], dev)
    send(low, low_out.at[p], 10, b_l.at[0], at_y(1))
    outs.append(pltpu.make_async_copy(low, low_out.at[p], loc.at[3]))
    outs[-1].start()
    query_y(4)
    output_y(5)
    output_y(4)
    for d in (0,) + NEAR_FIRST:
        g = ((z + NZ - d) % NZ) * NX + x
        if d:
            arrived(piece(g, 1), e_z.at[d])
        for e in (2, 1, 3):
            send(piece(g, 1), piece(g, 1), 11, e_x.at[d], at_x(e))
    arrived(qz.at[pl.ds(0, 2 * NZ - 1)], q_z.at[0])
    total = qz[0]
    for k in range(1, 2 * NZ):
        total = total + qz[k]
    qx[x] = total
    for e in (2, 1, 3):
        send(qx.at[x], qx.at[x], 14, q_x.at[0], at_x(e))
    for d in (0,) + NEAR_FIRST:
        row = rows_at(d)
        arrived(piece(0, 3), e_x.at[d])
        for side in range(2):
            two = piece(row + 2 * side, 2)
            send(two, half_piece(row + 2 * side), 12, e_y.at[0], at_y(1 if side == 0 else NY - 1))
    outs.append(pltpu.make_async_copy(half, half_out.at[p], loc.at[2]))
    outs[-1].start()
    arrived(qx.at[pl.ds(0, 3)], q_x.at[0])
    qy[...] = (qx[0] + qx[1]) + (qx[2] + qx[3])
    send(qy, total_out.at[p], 15, q_y.at[0], at_y(1))
    outs.append(pltpu.make_async_copy(qy, total_out.at[p], loc.at[4]))
    outs[-1].start()
    arrived(low_out.at[o], b_l.at[0])
    arrived(half_out.at[o], e_y.at[0])
    arrived(total_out.at[o], q_y.at[0])
    arrived(wg_q.at[:, o], w_y.at[0])
    arrived(wg_o.at[:, o], w_y.at[1])
    for c in outs:
        c.wait()
    for kind, ref in enumerate((
        pf.at[pl.ds(0, 31), 0], pf.at[:, 0],
        wg_q.at[pl.ds(0, 31), 0], wg_q.at[:, 0], wg_o.at[pl.ds(0, 31), 0], wg_o.at[:, 0],
        by_o, by_q, bz, by2, low, piece(0, 31), piece(0, 32),
        qz.at[pl.ds(0, 2 * NZ - 1)], qx.at[pl.ds(0, 3)], qy,
        bx_o, bx_q,
    )):
        remote(ref, ref, sent.at[kind], sent.at[kind], other_core).wait_send()


def gathered(inputs, query_cot, attended, output_cot, proj_q, proj_o, w_q, w_o,
             first_q, second_q, first_o, second_o):
    f32, bf16 = jnp.float32, jnp.bfloat16
    anywhere = pl.BlockSpec(memory_space=pl.ANY)
    dma = pltpu.SemaphoreType.DMA
    own_sides = (((32, 2, 48, RANK), bf16), ((32, 8, HALF), bf16), ((8, HALF), f32))
    both_sides = own_sides[:1] + tuple(((2,) + shape, kind) for shape, kind in own_sides[1:])
    return pl.pallas_call(
        comm_kernel,
        out_shape=tuple(jax.ShapeDtypeStruct(*s) for s in both_sides) + (
            jax.ShapeDtypeStruct((2, 1, 128), f32),
            jax.ShapeDtypeStruct((32, 2, 32, 512), bf16),
            jax.ShapeDtypeStruct((32, 2, 16, 1024), bf16),
        ),
        in_specs=[anywhere] * 12,
        out_specs=(anywhere,) * 6,
        scratch_shapes=[pltpu.VMEM(*s) for s in own_sides] + [
            pltpu.VMEM((128, D), bf16),
            pltpu.VMEM((128, 512), bf16),
            pltpu.VMEM((128, DA), bf16),
            pltpu.VMEM((128, 1024), bf16),
            pltpu.VMEM((2, 8, HALF), f32),
            pltpu.VMEM((2, 8, HALF), f32),
            pltpu.VMEM((32, 512), f32),
            pltpu.VMEM((16, 1024), f32),
            pltpu.VMEM((32, 512), bf16),
            pltpu.VMEM((16, 1024), bf16),
            pltpu.VMEM((2, NX, NZ, 8, 512), f32),
            pltpu.VMEM((2, NX, NZ, 8, 256), f32),
            pltpu.VMEM((7, NZ, 8, 512), bf16),
            pltpu.VMEM((7, NZ, 8, 256), bf16),
            pltpu.VMEM((NX, NZ, 8, 512), bf16),
            pltpu.VMEM((NX, NZ, 8, 256), bf16),
            pltpu.VMEM((3, NZ, 8, 512), bf16),
            pltpu.VMEM((3, NZ, 8, 256), bf16),
            pltpu.VMEM((NZ, 8, HALF), bf16),
            pltpu.VMEM((7, 8, HALF), bf16),
            pltpu.VMEM((8, HALF), f32),
            pltpu.VMEM((8, HALF), f32),
            pltpu.VMEM((2 * NZ, 1, 128), f32),
            pltpu.VMEM((NX, 1, 128), f32),
            pltpu.VMEM((1, 128), f32),
            dma((16,)), dma((18,)), dma((2, 8)), dma((2, 8)), dma((2,)), dma((9,)), dma((5, 2)), dma((8,)), dma((2,)),
            dma((2, 6)), dma((2,)), dma((1,)), dma((1,)), dma((1,)),
            dma((8,)), dma((8,)), dma((1,)), dma((1,)), dma((1,)), dma((1,)),
        ],
        compiler_params=pltpu.CompilerParams(collective_id=0, has_side_effects=True),
    )(
        inputs, query_cot, attended, output_cot,
        proj_q.reshape(2, 32, RANK), proj_o.reshape(2, 16, RANK),
        w_q.reshape(2, 32, 512), w_o.reshape(2, 16, 1024),
        first_q, second_q, first_o, second_o,
    )


CHUNKS = 4


def final_kernel(
    pf_in, wq_in, wo_in, half_in, low_in, total_in, proj_q_in, proj_o_in, weight_q_in, weight_o_in,
    first_q_in, second_q_in, first_o_in, second_o_in,
    new_q_out, new_o_out, step_q_out, step_o_out, nf_q_out, ns_q_out, nf_o_out, ns_o_out,
    copy_q_out, copy_o_out,
    pf, wq, wo, half, rows, small, new, copy_q, copy_o, chunk_sems, small_sems, new_sems, out_sems,
):
    low, total, proj_q, proj_o, weight_q, weight_o, first_q, second_q, first_o, second_o = small
    new_q, new_o, step_q, step_o, nf_q, ns_q, nf_o, ns_o = new
    shards = NZ * NX // CHUNKS

    def chunk_loads(i):
        part = pl.ds(i * shards, shards)
        return [
            pltpu.make_async_copy(src.at[part], dst.at[part], chunk_sems.at[k, i])
            for k, (src, dst) in enumerate(((pf_in, pf), (wq_in, wq), (wo_in, wo)))
        ]

    small_loads = [
        pltpu.make_async_copy(src, dst, small_sems.at[k])
        for k, (src, dst) in enumerate(zip(
            (low_in, total_in, proj_q_in, proj_o_in, weight_q_in, weight_o_in,
             first_q_in, second_q_in, first_o_in, second_o_in), small
        ))
    ]
    half_load = pltpu.make_async_copy(half_in, half, small_sems.at[len(small)])
    half_load.start()
    small_loads[1].start()
    for i in range(CHUNKS):
        for c in chunk_loads(i):
            c.start()
    for k, c in enumerate(small_loads):
        if k != 1:
            c.start()

    half_load.wait()
    small_loads[1].wait()
    mean = jnp.sum(total[0] + total[1], axis=1, keepdims=True) / (RANK * (DA + D))
    scale = lax.rsqrt(mean + mean_eps)
    rate = learn_rate * scale
    for h in range(2):
        rows[:, HALF * h : HALF * (h + 1)] = half[h].reshape(RANK, HALF)

    def product(factor, h, lo, width):
        start = HALF * h + lo
        return jnp.dot(factor, rows[:, start : start + width], preferred_element_type=jnp.float32)

    rows_q, rows_o = 64 * shards, 32 * shards

    def out_copies(i):
        part_q, part_o = pl.ds(i * rows_q, rows_q), pl.ds(i * rows_o, rows_o)
        return (
            pltpu.make_async_copy(copy_q.at[part_q], copy_q_out.at[part_q], out_sems.at[0, i]),
            pltpu.make_async_copy(copy_o.at[part_o], copy_o_out.at[part_o], out_sems.at[1, i]),
        )

    @pl.loop(0, CHUNKS)
    def _(i):
        for c in chunk_loads(i):
            c.wait()
        part = pl.ds(i * shards, shards)
        part_q, part_o = pl.ds(i * rows_q, rows_q), pl.ds(i * rows_o, rows_o)
        factor_o = pf[part, :, 32:, :].reshape(rows_o, RANK)
        factor_q = pf[part, :, :32, :].reshape(rows_q, RANK)
        for h in range(2):
            at_o, at_q = pl.ds(512 * h, 512), pl.ds(256 * h, 256)
            old_o = decoded(wo[part, :, :, at_o].reshape(rows_o, 512))
            copy_o[part_o, at_o] = (old_o - rate * product(factor_o, h, 0, 512)).astype(jnp.bfloat16)
            old_q = decoded(wq[part, :, :, at_q].reshape(rows_q, 256))
            copy_q[part_q, at_q] = (old_q - rate * product(factor_q, h, 512, 256)).astype(jnp.bfloat16)
        for c in out_copies(i):
            c.start()

    for k, c in enumerate(small_loads):
        if k != 1:
            c.wait()
    for h in range(2):
        at_o, at_q = pl.ds(512 * h, 512), pl.ds(256 * h, 256)
        mine_o = scale * product(proj_o[...], h, 0, 512)
        step_o[:, at_o] = mine_o
        new_o[:, at_o] = weight_o[:, at_o] - learn_rate * mine_o
        mine_q = scale * product(proj_q[...], h, 512, 256)
        step_q[:, at_q] = mine_q
        new_q[:, at_q] = weight_q[:, at_q] - learn_rate * mine_q
        nf_o[:, at_o], ns_o[:, at_o], _ = moment_update(
            low[h, :, :512], first_o[:, at_o], second_o[:, at_o]
        )
        nf_q[:, at_q], ns_q[:, at_q], _ = moment_update(
            low[h, :, 512:], first_q[:, at_q], second_q[:, at_q]
        )
    new_copies = [
        pltpu.make_async_copy(src, dst, new_sems.at[k])
        for k, (src, dst) in enumerate(zip(new, (
            new_q_out, new_o_out, step_q_out, step_o_out, nf_q_out, ns_q_out, nf_o_out, ns_o_out
        )))
    ]
    for c in new_copies:
        c.start()
    for i in range(CHUNKS):
        for c in out_copies(i):
            c.wait()
    for c in new_copies:
        c.wait()


def finished(pf, wq, wo, half, low, total, proj_q, proj_o, weight_q, weight_o,
             first_q, second_q, first_o, second_o):
    f32, bf16 = jnp.float32, jnp.bfloat16
    anywhere = pl.BlockSpec(memory_space=pl.ANY)
    dma = pltpu.SemaphoreType.DMA
    small = (low, total, proj_q, proj_o, weight_q, weight_o, first_q, second_q, first_o, second_o)
    outs = (
        ((64, 512), f32), ((32, 1024), f32), ((64, 512), f32), ((32, 1024), f32),
        ((8, 512), f32), ((8, 512), f32), ((8, 1024), f32), ((8, 1024), f32),
        ((D, 512), bf16), ((DA, 1024), bf16),
    )
    return pl.pallas_call(
        final_kernel,
        out_shape=tuple(jax.ShapeDtypeStruct(*s) for s in outs),
        in_specs=[anywhere] * 14,
        out_specs=(anywhere,) * 10,
        scratch_shapes=[
            *(pltpu.VMEM(a.shape, a.dtype) for a in (pf, wq, wo, half)),
            pltpu.VMEM((RANK, 2 * HALF), bf16),
            tuple(pltpu.VMEM(a.shape, a.dtype) for a in small),
            tuple(pltpu.VMEM(*s) for s in outs[:8]),
            *(pltpu.VMEM(*s) for s in outs[8:]),
            dma((3, CHUNKS)), dma((len(small) + 1,)), dma((8,)), dma((2, CHUNKS)),
        ],
        cost_estimate=pl.CostEstimate(flops=2_200_000_000, bytes_accessed=12_000_000, transcendentals=0),
    )(pf, wq, wo, half, *small)


def local(
    inputs, query_cot, attended, output_cot, proj_query, proj_output,
    weight_query, weight_output, first_query, second_query, first_output, second_output,
):
    pf, half, low, total, wg_q, wg_o = gathered(
        inputs, query_cot, attended, output_cot, proj_query, proj_output,
        weight_query, weight_output, first_query, second_query, first_output, second_output,
    )
    return finished(
        pf, wg_q, wg_o, half, low, total, proj_query, proj_output, weight_query, weight_output,
        first_query, second_query, first_output, second_output,
    )


def solution(mesh):
    return jax.shard_map(
        local,
        mesh=mesh,
        in_specs=(
            P(("fs", "rep"), None),
            P(("fs", "rep"), "tp"),
            P(("fs", "rep"), None),
            P(("fs", "rep"), "tp"),
            P("fs", None),
            P("fs", None),
            P("fs", "tp"),
            P("fs", "tp"),
            P("fs", "tp"),
            P("fs", "tp"),
            P("fs", "tp"),
            P("fs", "tp"),
        ),
        out_specs=(
            P("fs", "tp"),
            P("fs", "tp"),
            P("fs", "tp"),
            P("fs", "tp"),
            P("fs", "tp"),
            P("fs", "tp"),
            P("fs", "tp"),
            P("fs", "tp"),
            P(None, "tp"),
            P(None, "tp"),
        ),
        check_vma=False,
    )
```

```python
import functools

import jax
import jax.numpy as jnp
from jax import lax
from jax.experimental import pallas as pl
from jax.experimental.pallas import tpu as pltpu
from jax.sharding import PartitionSpec as P

D = 2048
DA = 1024
RANK = 256
NZ, NX, NY = 8, 4, 4

beta_first = 0.9
beta_second = 0.95
adam_eps = 1e-08
mean_eps = 1e-06
learn_rate = 0.02
HALF = 768

MESH = pl.DeviceIdType.MESH
NEAR_FIRST = (1, 7, 2, 6, 3, 5, 4)


def moment_update(low_sum, first, second):
    first_new = beta_first * first + (1.0 - beta_first) * low_sum
    second_new = beta_second * second + (1.0 - beta_second) * low_sum * low_sum
    normed = first_new / (jnp.sqrt(second_new) + adam_eps)
    return (first_new, second_new, normed)


def coded(v):
    square = v * v
    fourth = jnp.maximum(square * square, 1e-36)
    return jnp.where(v < 0, -fourth, fourth).astype(jnp.bfloat16)


def decoded(c):
    c = c.astype(jnp.float32)
    root = c * lax.rsqrt(jnp.abs(c))
    return root * lax.rsqrt(jnp.abs(root))


def comm_kernel(
    inputs, query_cot, attended, output_cot, proj_q, proj_o, w_q, w_o,
    first_q, second_q, first_o, second_o,
    pf_out, half_out, low_out, total_out, wg_q, wg_o,
    pf, half, low,
    x_in, c_q, x_at, c_o, fst, snd, old_q, old_o, code_q, code_o,
    lb_o, lb_q, cb_o, cb_q, by_o, by_q, bx_o, bx_q, sz, bz, ty, by2, qz, qx, qy,
    loc, sent, a_z, a_x, a_c, w_x, w_z, w_d, w_y, b_y, b_x, b_z, b_2, b_l,
    e_z, e_x, e_y, q_z, q_x, q_y,
):
    f = lax.axis_index("fs")
    y = lax.axis_index("rep")
    t = lax.axis_index("tp")
    z = f // NX
    x = f % NX
    p = y % 2
    o = 1 - p

    def at_z(d):
        return {"fs": ((z + d) % NZ) * NX + x}

    def at_zt(d):
        return {"fs": ((z + d) % NZ) * NX + x, "tp": 1 - t}

    def at_x(e):
        return {"fs": z * NX + (x + e) % NX}

    def at_y(s):
        return {"rep": (y + s) % NY}

    other_core = {"tp": 1 - t}

    def remote(src, dst, ssem, rsem, dev):
        return pltpu.make_async_remote_copy(
            src_ref=src, dst_ref=dst, send_sem=ssem, recv_sem=rsem,
            device_id=dev, device_id_type=MESH,
        )

    def send(src, dst, kind, rsem, dev):
        remote(src, dst, sent.at[kind], rsem, dev).start()

    def arrived(dst, rsem):
        remote(dst, dst, rsem, rsem, other_core).wait_recv()

    loads = [
        pltpu.make_async_copy(proj_q.at[t], pf.at[f, t, pl.ds(0, 32)], loc.at[0]),
        pltpu.make_async_copy(proj_o.at[t], pf.at[f, t, pl.ds(32, 16)], loc.at[1]),
        pltpu.make_async_copy(w_q.at[p], old_q, loc.at[12]),
        pltpu.make_async_copy(w_o.at[p], old_o, loc.at[13]),
        pltpu.make_async_copy(inputs, x_in, loc.at[2]),
        pltpu.make_async_copy(attended, x_at, loc.at[3]),
        pltpu.make_async_copy(query_cot, c_q, loc.at[4]),
        pltpu.make_async_copy(output_cot, c_o, loc.at[5]),
        pltpu.make_async_copy(first_o.at[:, pl.ds(0, 512)], fst.at[0, :, pl.ds(0, 512)], loc.at[6]),
        pltpu.make_async_copy(first_o.at[:, pl.ds(512, 512)], fst.at[1, :, pl.ds(0, 512)], loc.at[7]),
        pltpu.make_async_copy(first_q.at[:, pl.ds(0, 256)], fst.at[0, :, pl.ds(512, 256)], loc.at[8]),
        pltpu.make_async_copy(first_q.at[:, pl.ds(256, 256)], fst.at[1, :, pl.ds(512, 256)], loc.at[9]),
        pltpu.make_async_copy(second_o.at[:, pl.ds(0, 512)], snd.at[0, :, pl.ds(0, 512)], loc.at[10]),
        pltpu.make_async_copy(second_o.at[:, pl.ds(512, 512)], snd.at[1, :, pl.ds(0, 512)], loc.at[11]),
        pltpu.make_async_copy(second_q.at[:, pl.ds(0, 256)], snd.at[0, :, pl.ds(512, 256)], loc.at[14]),
        pltpu.make_async_copy(second_q.at[:, pl.ds(256, 256)], snd.at[1, :, pl.ds(512, 256)], loc.at[15]),
    ]
    for c in loads:
        c.start()

    barrier = pltpu.get_barrier_semaphore()
    peers = [at_z(d) for d in range(1, NZ)] + [at_zt(d) for d in range(1, NZ)]
    peers += [at_x(e) for e in range(1, NX)]
    peers += [at_y(s) for s in range(1, NY)] + [other_core]
    for dev in peers:
        pl.semaphore_signal(barrier, inc=1, device_id=dev, device_id_type=MESH)
    for c in loads[:4]:
        c.wait()
    code_q[...] = coded(old_q[...])
    code_o[...] = coded(old_o[...])
    own_q = pltpu.make_async_copy(code_q, wg_q.at[f, p], loc.at[12])
    own_o = pltpu.make_async_copy(code_o, wg_o.at[f, p], loc.at[13])
    own_q.start()
    own_o.start()
    pl.semaphore_wait(barrier, len(peers))

    factor_rows = (pl.ds(32, 16), pl.ds(0, 32))
    for k, rows in enumerate(factor_rows):
        for d in NEAR_FIRST:
            own = pf.at[f, t, rows]
            send(own, own, 0, a_z.at[k, d], at_z(d))

    def factors_x(k, d):
        part = pf.at[((z + NZ - d) % NZ) * NX + x, t, factor_rows[k]]
        if d:
            arrived(part, a_z.at[k, d])
        for e in (2, 1, 3):
            send(part, part, 0, a_x.at[k, d], at_x(e))

    def rows_at(d):
        return ((z + NZ - d) % NZ) * NX

    def output_x(d):
        g = rows_at(d) + x
        if d:
            arrived(wg_o.at[g, p], w_d.at[d])
        src = wg_o.at[g, p] if d else code_o
        for e in (2, 1, 3):
            send(src, wg_o.at[g, p], 4, w_x.at[1 + d], at_x(e))

    def weights_y(k, d):
        ref = (wg_q, wg_o)[k]
        for side in range(2):
            two = ref.at[pl.ds(rows_at(d) + 2 * side, 2), p]
            send(two, two, 3 + 2 * k, w_y.at[k], at_y(1 if side == 0 else NY - 1))

    def output_y(d):
        arrived(wg_o.at[pl.ds(0, 3), p], w_x.at[1 + d])
        weights_y(1, d)

    def query_z(s):
        if s == 0:
            arrived(wg_q.at[pl.ds(0, 3), p], w_x.at[0])
            part = wg_q.at[pl.ds(rows_at(0), NX), p]
            send(part, part, 2, w_z.at[1, 0], at_z(1))
            send(part, part, 2, w_z.at[1, 1], at_z(NZ - 1))
            return
        if s == NZ // 2:
            for way in range(2):
                arrived(wg_q.at[pl.ds(rows_at(s) + 2 * way, 2), p], w_z.at[s, way])
            return
        for way, sign in ((0, 1), (1, -1)):
            part = wg_q.at[pl.ds(rows_at(sign * s), NX), p]
            arrived(part, w_z.at[s, way])
            if s == NZ // 2 - 1:
                part = wg_q.at[pl.ds(rows_at(sign * s) + 2 * way, 2), p]
            send(part, part, 2, w_z.at[s + 1, way], at_z(sign % NZ))

    def query_y(s):
        for d in ((s, NZ - s) if s % (NZ // 2) else (s,)):
            weights_y(0, d)

    for d in NEAR_FIRST:
        send(code_o, wg_o.at[f, p], 4, w_d.at[d], at_z(d))
    factors_x(0, 0)
    factors_x(1, 0)
    for e in (2, 1, 3):
        send(code_q, wg_q.at[f, p], 2, w_x.at[0], at_x(e))
    for k in range(2):
        for d in NEAR_FIRST:
            factors_x(k, d)

    own_q.wait()
    own_o.wait()
    query_z(0)
    query_y(0)

    def factors_core(k):
        rows = factor_rows[k]
        for d in (0,) + NEAR_FIRST:
            arrived(pf.at[pl.ds(0, 3), t, rows], a_x.at[k, d])
            part = pf.at[pl.ds(rows_at(d), NX), t, rows]
            send(part, part, 1, a_c.at[k], other_core)
        arrived(pf.at[:, 1 - t, rows], a_c.at[k])

    def partial_low(tokens, whole, cot, depth):
        reduced = jnp.dot(
            tokens[...], whole.reshape(depth, RANK), preferred_element_type=jnp.float32
        )
        high = reduced.astype(jnp.bfloat16)
        rest = (reduced - high.astype(jnp.float32)).astype(jnp.bfloat16)
        both = jnp.concatenate([high, rest], axis=0)
        return lax.dot_general(
            both, jnp.concatenate([cot, cot], axis=0),
            (((0,), (0,)), ((), ())), preferred_element_type=jnp.float32,
        )

    def put(lb, block):
        width = block.shape[1] // 2
        for par in range(2):
            for zz in range(NZ):
                for xx in range(NX):
                    r = (zz * NX + xx) * 8
                    lb[par, xx, zz] = block[r : r + 8, par * width : (par + 1) * width]

    chunks = (
        (2, 0, 8, 1), (3, 0, 8, NY - 1), (1, 0, 4, 1), (1, 4, 4, NY - 1), (0, 0, 4, 1), (0, 4, 4, NY - 1),
    )

    def sums_y(k, lb, cb, by):
        for n, (e, lo, rows, step) in enumerate(chunks):
            part = (x + e) % NX, pl.ds(lo, rows)
            cb[part] = coded(lb[(o,) + part])
            send(cb.at[part], by.at[part], 6 + k, b_y.at[k, n], at_y(step))

    def sums_x(k, lb, cb, by, bx):
        for n, (e, lo, rows, step) in enumerate(chunks):
            j = (x + e) % NX
            part = j, pl.ds(lo, rows)
            arrived(by.at[part], b_y.at[k, n])
            lb[(p,) + part] = lb[(p,) + part] + decoded(by[part])
            if e and lo + rows == NZ:
                cb[NX + e - 1] = coded(lb[p, j])
                send(cb.at[NX + e - 1], bx.at[e - 1], 16 + k, b_x.at[k], at_x(e))

    factors_core(0)
    loads[5].wait()
    loads[7].wait()
    put(lb_o, partial_low(x_at, pf[:, :, 32:, :], c_o[...], DA))
    sums_y(0, lb_o, cb_o, by_o)
    output_x(0)
    output_x(1)
    output_x(7)
    factors_core(1)
    outs = [pltpu.make_async_copy(pf, pf_out, loc.at[0])]
    outs[0].start()
    loads[4].wait()
    loads[6].wait()
    put(lb_q, partial_low(x_in, pf[:, :, :32, :], c_q[...], D))
    sums_y(1, lb_q, cb_q, by_q)
    query_z(1)
    query_y(1)
    output_y(0)

    sums_x(0, lb_o, cb_o, by_o, bx_o)
    sums_x(1, lb_q, cb_q, by_q, bx_q)
    for d in (2, 6, 3, 5, 4):
        output_x(d)
    output_y(1)
    output_y(7)
    query_z(2)
    query_y(2)
    for k, (lb, bx) in enumerate(((lb_o, bx_o), (lb_q, bx_q))):
        arrived(bx, b_x.at[k])
        part = (lb[p, x] + decoded(bx[0])) + (decoded(bx[1]) + decoded(bx[2]))
        lb[o, 0] = part
        sz[:, :, pl.ds(512 * k, part.shape[2])] = coded(part)
    for d in (4, 3, 5, 2, 6, 1, 7):
        send(sz.at[(z + d) % NZ], bz.at[d - 1], 8, b_z.at[0], at_z(d))
    output_y(2)
    query_z(3)
    output_y(6)
    arrived(bz, b_z.at[0])
    mine = jnp.concatenate([lb_o[o, 0, z], lb_q[o, 0, z]], axis=1)
    for d in range(7):
        mine = mine + decoded(bz[d])
    ty[...] = mine
    send(ty, by2, 9, b_2.at[0], at_y(2))
    query_y(3)
    output_y(3)
    query_z(4)
    for c in loads[8:16]:
        c.wait()
    arrived(by2, b_2.at[0])

    low_sum = mine + by2[...]
    low[...] = low_sum
    _, _, normed = moment_update(low_sum, fst[p], snd[p])
    half[f] = normed.astype(jnp.bfloat16)
    square = normed * normed
    total = square[:, 0:128]
    for k in range(1, 6):
        total = total + square[:, k * 128 : (k + 1) * 128]
    qz[z * 2 + t] = jnp.sum(total, axis=0, keepdims=True)

    def piece(g, n):
        return half.at[pl.ds(g, n)]

    def half_piece(g):
        return half_out.at[p, pl.ds(g, 2)]

    for d in (4, 3, 5, 2, 6, 1, 7):
        send(piece(f, 1), piece(f, 1), 11, e_z.at[d], at_z(d))
    for d in range(NZ):
        for core, dev in ((0, at_z(d)), (1, at_zt(d) if d else other_core)):
            if d or core:
                row = qz.at[z * 2 + t]
                send(row, row, 13, q_z.at[0], dev)
    send(low, low_out.at[p], 10, b_l.at[0], at_y(1))
    outs.append(pltpu.make_async_copy(low, low_out.at[p], loc.at[3]))
    outs[-1].start()
    query_y(4)
    output_y(5)
    output_y(4)
    for d in (0,) + NEAR_FIRST:
        g = ((z + NZ - d) % NZ) * NX + x
        if d:
            arrived(piece(g, 1), e_z.at[d])
        for e in (2, 1, 3):
            send(piece(g, 1), piece(g, 1), 11, e_x.at[d], at_x(e))
    arrived(qz.at[pl.ds(0, 2 * NZ - 1)], q_z.at[0])
    total = qz[0]
    for k in range(1, 2 * NZ):
        total = total + qz[k]
    qx[x] = total
    for e in (2, 1, 3):
        send(qx.at[x], qx.at[x], 14, q_x.at[0], at_x(e))
    for d in (0,) + NEAR_FIRST:
        row = rows_at(d)
        arrived(piece(0, 3), e_x.at[d])
        for side in range(2):
            two = piece(row + 2 * side, 2)
            send(two, half_piece(row + 2 * side), 12, e_y.at[0], at_y(1 if side == 0 else NY - 1))
    outs.append(pltpu.make_async_copy(half, half_out.at[p], loc.at[2]))
    outs[-1].start()
    arrived(qx.at[pl.ds(0, 3)], q_x.at[0])
    qy[...] = (qx[0] + qx[1]) + (qx[2] + qx[3])
    send(qy, total_out.at[p], 15, q_y.at[0], at_y(1))
    outs.append(pltpu.make_async_copy(qy, total_out.at[p], loc.at[4]))
    outs[-1].start()
    arrived(low_out.at[o], b_l.at[0])
    arrived(half_out.at[o], e_y.at[0])
    arrived(total_out.at[o], q_y.at[0])
    arrived(wg_q.at[:, o], w_y.at[0])
    arrived(wg_o.at[:, o], w_y.at[1])
    for c in outs:
        c.wait()
    for kind, ref in enumerate((
        pf.at[pl.ds(0, 31), 0], pf.at[:, 0],
        wg_q.at[pl.ds(0, 31), 0], wg_q.at[:, 0], wg_o.at[pl.ds(0, 31), 0], wg_o.at[:, 0],
        by_o, by_q, bz, by2, low, piece(0, 31), piece(0, 32),
        qz.at[pl.ds(0, 2 * NZ - 1)], qx.at[pl.ds(0, 3)], qy,
        bx_o, bx_q,
    )):
        remote(ref, ref, sent.at[kind], sent.at[kind], other_core).wait_send()


def gathered(inputs, query_cot, attended, output_cot, proj_q, proj_o, w_q, w_o,
             first_q, second_q, first_o, second_o):
    f32, bf16 = jnp.float32, jnp.bfloat16
    anywhere = pl.BlockSpec(memory_space=pl.ANY)
    dma = pltpu.SemaphoreType.DMA
    own_sides = (((32, 2, 48, RANK), bf16), ((32, 8, HALF), bf16), ((8, HALF), f32))
    both_sides = own_sides[:1] + tuple(((2,) + shape, kind) for shape, kind in own_sides[1:])
    return pl.pallas_call(
        comm_kernel,
        out_shape=tuple(jax.ShapeDtypeStruct(*s) for s in both_sides) + (
            jax.ShapeDtypeStruct((2, 1, 128), f32),
            jax.ShapeDtypeStruct((32, 2, 32, 512), bf16),
            jax.ShapeDtypeStruct((32, 2, 16, 1024), bf16),
        ),
        in_specs=[anywhere] * 12,
        out_specs=(anywhere,) * 6,
        scratch_shapes=[pltpu.VMEM(*s) for s in own_sides] + [
            pltpu.VMEM((128, D), bf16),
            pltpu.VMEM((128, 512), bf16),
            pltpu.VMEM((128, DA), bf16),
            pltpu.VMEM((128, 1024), bf16),
            pltpu.VMEM((2, 8, HALF), f32),
            pltpu.VMEM((2, 8, HALF), f32),
            pltpu.VMEM((32, 512), f32),
            pltpu.VMEM((16, 1024), f32),
            pltpu.VMEM((32, 512), bf16),
            pltpu.VMEM((16, 1024), bf16),
            pltpu.VMEM((2, NX, NZ, 8, 512), f32),
            pltpu.VMEM((2, NX, NZ, 8, 256), f32),
            pltpu.VMEM((7, NZ, 8, 512), bf16),
            pltpu.VMEM((7, NZ, 8, 256), bf16),
            pltpu.VMEM((NX, NZ, 8, 512), bf16),
            pltpu.VMEM((NX, NZ, 8, 256), bf16),
            pltpu.VMEM((3, NZ, 8, 512), bf16),
            pltpu.VMEM((3, NZ, 8, 256), bf16),
            pltpu.VMEM((NZ, 8, HALF), bf16),
            pltpu.VMEM((7, 8, HALF), bf16),
            pltpu.VMEM((8, HALF), f32),
            pltpu.VMEM((8, HALF), f32),
            pltpu.VMEM((2 * NZ, 1, 128), f32),
            pltpu.VMEM((NX, 1, 128), f32),
            pltpu.VMEM((1, 128), f32),
            dma((16,)), dma((18,)), dma((2, 8)), dma((2, 8)), dma((2,)), dma((9,)), dma((5, 2)), dma((8,)), dma((2,)),
            dma((2, 6)), dma((2,)), dma((1,)), dma((1,)), dma((1,)),
            dma((8,)), dma((8,)), dma((1,)), dma((1,)), dma((1,)), dma((1,)),
        ],
        compiler_params=pltpu.CompilerParams(collective_id=0, has_side_effects=True),
    )(
        inputs, query_cot, attended, output_cot,
        proj_q.reshape(2, 32, RANK), proj_o.reshape(2, 16, RANK),
        w_q.reshape(2, 32, 512), w_o.reshape(2, 16, 1024),
        first_q, second_q, first_o, second_o,
    )


CHUNKS = 4


def final_kernel(
    pf_in, wq_in, wo_in, half_in, low_in, total_in, proj_q_in, proj_o_in, weight_q_in, weight_o_in,
    first_q_in, second_q_in, first_o_in, second_o_in,
    new_q_out, new_o_out, step_q_out, step_o_out, nf_q_out, ns_q_out, nf_o_out, ns_o_out,
    copy_q_out, copy_o_out,
    pf, wq, wo, half, rows, small, new, copy_q, copy_o, chunk_sems, small_sems, new_sems, out_sems,
):
    low, total, proj_q, proj_o, weight_q, weight_o, first_q, second_q, first_o, second_o = small
    new_q, new_o, step_q, step_o, nf_q, ns_q, nf_o, ns_o = new
    shards = NZ * NX // CHUNKS

    def chunk_loads(i):
        part = pl.ds(i * shards, shards)
        return [
            pltpu.make_async_copy(src.at[part], dst.at[part], chunk_sems.at[k, i])
            for k, (src, dst) in enumerate(((pf_in, pf), (wq_in, wq), (wo_in, wo)))
        ]

    small_loads = [
        pltpu.make_async_copy(src, dst, small_sems.at[k])
        for k, (src, dst) in enumerate(zip(
            (low_in, total_in, proj_q_in, proj_o_in, weight_q_in, weight_o_in,
             first_q_in, second_q_in, first_o_in, second_o_in), small
        ))
    ]
    half_load = pltpu.make_async_copy(half_in, half, small_sems.at[len(small)])
    half_load.start()
    small_loads[1].start()
    for i in range(CHUNKS):
        for c in chunk_loads(i):
            c.start()
    for k, c in enumerate(small_loads):
        if k != 1:
            c.start()

    half_load.wait()
    small_loads[1].wait()
    mean = jnp.sum(total[0] + total[1], axis=1, keepdims=True) / (RANK * (DA + D))
    scale = lax.rsqrt(mean + mean_eps)
    rate = learn_rate * scale
    for h in range(2):
        rows[:, HALF * h : HALF * (h + 1)] = half[h].reshape(RANK, HALF)

    def product(factor, h, lo, width):
        start = HALF * h + lo
        return jnp.dot(factor, rows[:, start : start + width], preferred_element_type=jnp.float32)

    rows_q, rows_o = 64 * shards, 32 * shards

    def out_copies(i):
        part_q, part_o = pl.ds(i * rows_q, rows_q), pl.ds(i * rows_o, rows_o)
        return (
            pltpu.make_async_copy(copy_q.at[part_q], copy_q_out.at[part_q], out_sems.at[0, i]),
            pltpu.make_async_copy(copy_o.at[part_o], copy_o_out.at[part_o], out_sems.at[1, i]),
        )

    @pl.loop(0, CHUNKS)
    def _(i):
        for c in chunk_loads(i):
            c.wait()
        part = pl.ds(i * shards, shards)
        part_q, part_o = pl.ds(i * rows_q, rows_q), pl.ds(i * rows_o, rows_o)
        factor_o = pf[part, :, 32:, :].reshape(rows_o, RANK)
        factor_q = pf[part, :, :32, :].reshape(rows_q, RANK)
        for h in range(2):
            at_o, at_q = pl.ds(512 * h, 512), pl.ds(256 * h, 256)
            old_o = decoded(wo[part, :, :, at_o].reshape(rows_o, 512))
            copy_o[part_o, at_o] = (old_o - rate * product(factor_o, h, 0, 512)).astype(jnp.bfloat16)
            old_q = decoded(wq[part, :, :, at_q].reshape(rows_q, 256))
            copy_q[part_q, at_q] = (old_q - rate * product(factor_q, h, 512, 256)).astype(jnp.bfloat16)
        for c in out_copies(i):
            c.start()

    for k, c in enumerate(small_loads):
        if k != 1:
            c.wait()
    for h in range(2):
        at_o, at_q = pl.ds(512 * h, 512), pl.ds(256 * h, 256)
        mine_o = scale * product(proj_o[...], h, 0, 512)
        step_o[:, at_o] = mine_o
        new_o[:, at_o] = weight_o[:, at_o] - learn_rate * mine_o
        mine_q = scale * product(proj_q[...], h, 512, 256)
        step_q[:, at_q] = mine_q
        new_q[:, at_q] = weight_q[:, at_q] - learn_rate * mine_q
        nf_o[:, at_o], ns_o[:, at_o], _ = moment_update(
            low[h, :, :512], first_o[:, at_o], second_o[:, at_o]
        )
        nf_q[:, at_q], ns_q[:, at_q], _ = moment_update(
            low[h, :, 512:], first_q[:, at_q], second_q[:, at_q]
        )
    new_copies = [
        pltpu.make_async_copy(src, dst, new_sems.at[k])
        for k, (src, dst) in enumerate(zip(new, (
            new_q_out, new_o_out, step_q_out, step_o_out, nf_q_out, ns_q_out, nf_o_out, ns_o_out
        )))
    ]
    for c in new_copies:
        c.start()
    for i in range(CHUNKS):
        for c in out_copies(i):
            c.wait()
    for c in new_copies:
        c.wait()


def finished(pf, wq, wo, half, low, total, proj_q, proj_o, weight_q, weight_o,
             first_q, second_q, first_o, second_o):
    f32, bf16 = jnp.float32, jnp.bfloat16
    anywhere = pl.BlockSpec(memory_space=pl.ANY)
    dma = pltpu.SemaphoreType.DMA
    small = (low, total, proj_q, proj_o, weight_q, weight_o, first_q, second_q, first_o, second_o)
    outs = (
        ((64, 512), f32), ((32, 1024), f32), ((64, 512), f32), ((32, 1024), f32),
        ((8, 512), f32), ((8, 512), f32), ((8, 1024), f32), ((8, 1024), f32),
        ((D, 512), bf16), ((DA, 1024), bf16),
    )
    return pl.pallas_call(
        final_kernel,
        out_shape=tuple(jax.ShapeDtypeStruct(*s) for s in outs),
        in_specs=[anywhere] * 14,
        out_specs=(anywhere,) * 10,
        scratch_shapes=[
            *(pltpu.VMEM(a.shape, a.dtype) for a in (pf, wq, wo, half)),
            pltpu.VMEM((RANK, 2 * HALF), bf16),
            tuple(pltpu.VMEM(a.shape, a.dtype) for a in small),
            tuple(pltpu.VMEM(*s) for s in outs[:8]),
            *(pltpu.VMEM(*s) for s in outs[8:]),
            dma((3, CHUNKS)), dma((len(small) + 1,)), dma((8,)), dma((2, CHUNKS)),
        ],
        cost_estimate=pl.CostEstimate(flops=2_200_000_000, bytes_accessed=12_000_000, transcendentals=0),
    )(pf, wq, wo, half, *small)


def local(
    inputs, query_cot, attended, output_cot, proj_query, proj_output,
    weight_query, weight_output, first_query, second_query, first_output, second_output,
):
    pf, half, low, total, wg_q, wg_o = gathered(
        inputs, query_cot, attended, output_cot, proj_query, proj_output,
        weight_query, weight_output, first_query, second_query, first_output, second_output,
    )
    return finished(
        pf, wg_q, wg_o, half, low, total, proj_query, proj_output, weight_query, weight_output,
        first_query, second_query, first_output, second_output,
    )


def solution(mesh):
    return jax.shard_map(
        local,
        mesh=mesh,
        in_specs=(
            P(("fs", "rep"), None),
            P(("fs", "rep"), "tp"),
            P(("fs", "rep"), None),
            P(("fs", "rep"), "tp"),
            P("fs", None),
            P("fs", None),
            P("fs", "tp"),
            P("fs", "tp"),
            P("fs", "tp"),
            P("fs", "tp"),
            P("fs", "tp"),
            P("fs", "tp"),
        ),
        out_specs=(
            P("fs", "tp"),
            P("fs", "tp"),
            P("fs", "tp"),
            P("fs", "tp"),
            P("fs", "tp"),
            P("fs", "tp"),
            P("fs", "tp"),
            P("fs", "tp"),
            P(None, "tp"),
            P(None, "tp"),
        ),
        check_vma=False,
    )
```
